128 devices in a mesh: ep: 128 (over z, y, x, core).
Axes of the slice: x: 4, y: 4, z: 4, core: 2. Of those that a mesh axis runs over, the one named last changes fastest.
Arguments:
- tokens: bfloat16 [512, 2048], P('ep'), may hold values from -6 to 6
- lengths: int32 [512], P('ep'), may hold values from 1 to 1023
- cache_keys: bfloat16 [512, 1024, 2, 128], P('ep')
- cache_values: bfloat16 [512, 1024, 2, 128], P('ep'), may hold values from -6 to 6
- query_w: bfloat16 [2048, 1024], replicated, may hold values from -0.125 to 0.125
- key_w: bfloat16 [2048, 256], replicated, may hold values from -0.125 to 0.125
- value_w: bfloat16 [2048, 256], replicated, may hold values from -0.125 to 0.125
- out_w: bfloat16 [1024, 2048], replicated, may hold values from -0.1875 to 0.1875
- mix_lambda: float32 [8], replicated, may hold values from 0.3 to 0.8
- head_gain: float32 [128], replicated, may hold values from 0.1 to 1.9
- attn_gain: float32 [2048], replicated, may hold values from 0.1 to 1.9
- ffn_gain: float32 [2048], replicated, may hold values from 0.1 to 1.9
- routes: int32 [512, 2], P('ep'), may hold values from 0 to 7, all different within a row; in each aligned block of 4 rows (0 to 3, 4 to 7, ...) at most 2 rows name the same one
- route_weights: float32 [512, 2], P('ep'), may hold values from 0.2 to 1
- exp_gate: bfloat16 [2048, 49152], P(None, 'ep'), may hold values from -0.125 to 0.125
- exp_up: bfloat16 [2048, 49152], P(None, 'ep'), may hold values from -0.125 to 0.125
- exp_down: bfloat16 [49152, 2048], P('ep'), may hold values from -0.078125 to 0.078125
- dense_gate: bfloat16 [128, 256, 352], P('ep'), may hold values from -0.125 to 0.125
- dense_up: bfloat16 [128, 256, 352], P('ep'), may hold values from -0.125 to 0.125
- dense_down: bfloat16 [128, 352, 256], P('ep'), may hold values from -0.078125 to 0.078125
- branch_gate: bfloat16 [2048], replicated, may hold values from -0.125 to 0.125
Outputs:
- output: bfloat16 [512, 2048], P('ep')
- new_keys: bfloat16 [512, 256], P('ep')
- new_values: bfloat16 [512, 256], P('ep')
The draws below stay inside these ranges and needn't reach their ends.
Inputs may be any that keep to these rules, and one draw needn't show every extreme that they name: `routes`: each row names 2 different experts; among the 4 rows of one device no expert is named by more than 2 rows, a bound that some block reaches.
All inputs are finite; a program needn't handle non-finite values.
Results may differ from the reference program's by a relative error of at most 0.015.
Values may be sent and summed in bfloat16 or wider, within the bound.
A program may use at most 128 MiB of HBM per device.

```python
import math
import jax
import jax.numpy as jnp
import numpy as np
from jax import lax

D = 2048
HEADS = 8
KV_HEADS = 2
HEAD_DIM = 128
CACHE = 1024
SEQ_DEV = 4
TOP_K = 2
SPLIT = 16
EXP_FF = 6144
DENSE_FF = 5632
EXPERTS = 8
BLOCKS = 8
CAP = 2
TOKENS = 512
N_EP = 128


def draw_cache_keys(key, part):
    shape = (TOKENS, CACHE, KV_HEADS, HEAD_DIM)
    base_key = jax.random.fold_in(jax.random.fold_in(key, 11), 0)
    values = jax.random.normal(base_key, shape, jnp.float32) * 1.75
    values = jnp.clip(values, -10.0, 10.0)
    return values.astype(jnp.bfloat16)


def plant(drawn, stream_key, least, high):
    longest = drawn.shape.index(max(drawn.shape))
    spots = []
    for shift in (0, 1):
        where = [jax.random.randint(jax.random.fold_in(stream_key, axis), (), 0, length) for axis, length in enumerate(drawn.shape)]
        where[longest] = (where[longest] + shift) % drawn.shape[longest]
        spots.append(tuple(where))
    return drawn.at[spots[0]].set(least).at[spots[1]].set(high)


def level_of(key, extent, cuts, low, top_value):
    level = 1.0
    for position, blocks in cuts:
        steps = jax.random.uniform(jax.random.fold_in(jax.random.fold_in(key, 6), position), (blocks,), jnp.float32, low / len(cuts), top_value / len(cuts))
        level = level * jnp.repeat(jnp.exp(steps), extent[position] // blocks).reshape((-1,) + (1,) * (len(extent) - 1 - position))
    return level


def deal_out(own_key, own, number, rows, number_of, top, most, lean):
    ranking = jax.random.permutation(own_key, number_of)
    packed, ordinary = load_shares(number_of, rows * top, most, lean, True), load_shares(number_of, rows * top, most, lean, False)
    places = jnp.arange(number_of)

    def named(sizes, offset_by):
        used = int((sizes > 0).sum())
        fixed = max(1, used // 4)
        passed = fixed + (places - fixed + offset_by * (used - fixed)) % max(1, number_of - fixed)
        return jnp.zeros((number_of,), jnp.int32).at[ranking[jnp.where(places < fixed, places, passed)]].set(jnp.asarray(sizes, jnp.int32))

    sizes = jnp.where(number % 4 == 0, named(packed, number // 4), named(ordinary, number - number // 4 - 1))
    mixed = jax.random.permutation(jax.random.fold_in(own, 3), number_of)
    source_of, receiver = mixed[0:number_of // 2 * 2:2], mixed[1:number_of // 2 * 2:2]
    slack = jnp.minimum(sizes[source_of] - 1, most - sizes[receiver]) // 2
    slack = jnp.where((source_of == ranking[0]) | (receiver == ranking[0]) | (sizes[receiver] == 0), 0, jnp.maximum(slack, 0))
    passed = jax.random.randint(jax.random.fold_in(own, 4), (number_of // 2,), 0, 1 << 20) % (slack + 1)
    sizes = sizes.at[source_of].add(-passed).at[receiver].add(passed)
    members = jnp.searchsorted(jnp.cumsum(sizes), jnp.arange(rows * top), side="right").astype(jnp.int32)
    listing = members.reshape(top, rows).T
    listing = listing[jax.random.permutation(jax.random.fold_in(own, 1), rows)]
    offset_by = jax.random.randint(jax.random.fold_in(own, 2), (rows, 1), 0, top)
    return jnp.take_along_axis(listing, (jnp.arange(top)[None, :] + offset_by) % top, axis=1)


def load_shares(count, total, limit, skew, full):
    loads = [(1 << 20) // math.isqrt(grade ** skew) + 1 for grade in range(1, count + 1)]
    largest = limit if full else min(limit, max(-(-total // count), total * loads[0] // sum(loads)))
    least = 1 if total - largest >= count - 1 else 0
    counts, spare = [largest] + [least] * (count - 1), total - largest - least * (count - 1)
    while spare > 0:
        free = [i for i in range(1, count) if counts[i] < largest] or [i for i in range(1, count) if counts[i] < limit]
        mass, left = sum([loads[i] for i in free]), spare
        for i in free:
            extra = min(limit - counts[i], max(1, left * loads[i] // mass), spare)
            counts[i] = counts[i] + extra
            spare = spare - extra
    return np.array(counts)


def centred(key, extent, spread, most, shards=(), kind=jnp.bfloat16):
    values = jax.random.normal(key, extent, jnp.float32) * spread
    if len(shards) > 0:
        values = level_of(key, extent, shards, -0.22, 0.18) * values
    return jnp.clip(values, min=-most, max=most).astype(kind)


def setup_inputs(seed: int = 0) -> dict:
    seeds = jax.random.split(jax.random.key(seed), 22)
    tokens = centred(seeds[0], (TOKENS, D), 1.0, 6.0, ((0, 128),))
    lengths = plant(jax.random.randint(seeds[1], (TOKENS,), 1, CACHE), jax.random.fold_in(seeds[1], 1), 1, CACHE - 1).astype(jnp.int32)
    cache_keys = draw_cache_keys(jax.random.fold_in(seeds[21], 71), 0)
    cache_values = centred(seeds[3], (TOKENS, CACHE, KV_HEADS, HEAD_DIM), 1.0, 6.0, ((0, 128),))
    query_w = centred(seeds[4], (D, HEADS * HEAD_DIM), D ** -0.5, 0.125)
    key_w = centred(seeds[5], (D, KV_HEADS * HEAD_DIM), D ** -0.5, 0.125)
    value_w = centred(seeds[6], (D, KV_HEADS * HEAD_DIM), D ** -0.5, 0.125)
    out_w = centred(seeds[7], (HEADS * HEAD_DIM, D), (HEADS * HEAD_DIM) ** -0.5, 0.1875)
    mix_lambda = jnp.clip(jax.random.uniform(seeds[8], (HEADS,), jnp.float32, 0.3, 0.8), 0.3, 0.8)
    head_gain = jnp.clip(1.0 + 0.18 * jax.random.normal(seeds[9], (HEAD_DIM,), jnp.float32), 0.1, 1.9)
    attn_gain = jnp.clip(1.0 + 0.18 * jax.random.normal(seeds[10], (D,), jnp.float32), 0.1, 1.9)
    ffn_gain = jnp.clip(1.0 + 0.18 * jax.random.normal(seeds[11], (D,), jnp.float32), 0.1, 1.9)
    routes_keys = jax.random.split(jax.random.fold_in(seeds[12], 1), TOKENS // SEQ_DEV)
    routes_turns = jax.random.permutation(jax.random.fold_in(seeds[12], 3), TOKENS // SEQ_DEV)
    routes = jax.vmap(lambda own, number: deal_out(jax.random.fold_in(seeds[12], 2), own, number, SEQ_DEV, EXPERTS, TOP_K, CAP, 1))(routes_keys, routes_turns).reshape((TOKENS, TOP_K))
    route_weights = jnp.clip(0.2 + 0.8 * jax.random.uniform(seeds[13], (TOKENS, TOP_K), jnp.float32) ** level_of(seeds[13], (TOKENS, TOP_K), ((0, 128),), -0.2, 0.2), 0.2, 1.0)
    exp_gate = centred(seeds[14], (D, EXPERTS * EXP_FF), D ** -0.5, 0.125, ((1, 128),))
    exp_up = centred(seeds[15], (D, EXPERTS * EXP_FF), D ** -0.5, 0.125, ((1, 128),))
    exp_down = centred(seeds[16], (EXPERTS * EXP_FF, D), EXP_FF ** -0.5, 0.078125, ((0, 128),))
    dense_gate = centred(seeds[17], (N_EP, D // BLOCKS, DENSE_FF // SPLIT), D ** -0.5, 0.125, ((0, 128),))
    dense_up = centred(seeds[18], (N_EP, D // BLOCKS, DENSE_FF // SPLIT), D ** -0.5, 0.125, ((0, 128),))
    dense_down = centred(seeds[19], (N_EP, DENSE_FF // SPLIT, D // BLOCKS), DENSE_FF ** -0.5, 0.078125, ((0, 128),))
    branch_gate = centred(seeds[20], (D,), D ** -0.5, 0.125)
    return {"tokens": tokens, "lengths": lengths, "cache_keys": cache_keys, "cache_values": cache_values, "query_w": query_w, "key_w": key_w, "value_w": value_w, "out_w": out_w, "mix_lambda": mix_lambda, "head_gain": head_gain, "attn_gain": attn_gain, "ffn_gain": ffn_gain, "routes": routes, "route_weights": route_weights, "exp_gate": exp_gate, "exp_up": exp_up, "exp_down": exp_down, "dense_gate": dense_gate, "dense_up": dense_up, "dense_down": dense_down, "branch_gate": branch_gate}


def rms_norm(values, gain, epsilon):
    scale = lax.rsqrt(lax.optimization_barrier(jnp.mean(values * values, axis=-1, keepdims=True)) + epsilon)
    return values * scale * gain.astype(jnp.float32)

def softmax_pair(scores, own_score, valid):
    masked = jnp.where(valid, scores, -jnp.inf)
    largest = jnp.maximum(lax.optimization_barrier(jnp.max(masked, axis=-1)), own_score)
    raised = jnp.where(valid, jnp.exp(scores - largest[..., None]), 0.0)
    own_raised = jnp.exp(own_score - largest)
    total = lax.optimization_barrier(jnp.sum(raised, axis=-1)) + own_raised
    return (raised / total[..., None], own_raised / total)

def attend_block(tokens, lengths, cache_keys, cache_values, query_w, key_w, value_w, out_w, mix_lambda, head_gain, attn_gain, ffn_gain):
    rows = tokens.shape[0]
    groups = HEADS // KV_HEADS
    half = HEAD_DIM // 2
    scale = (HEAD_DIM // 2) ** (-0.5)
    xfull = tokens.astype(jnp.float32)
    normed = rms_norm(xfull, attn_gain, 1e-06).astype(jnp.bfloat16)
    query = jnp.dot(normed, query_w, preferred_element_type=jnp.float32).astype(jnp.bfloat16)
    key_new = jnp.dot(normed, key_w, preferred_element_type=jnp.float32).astype(jnp.bfloat16)
    value_new = jnp.dot(normed, value_w, preferred_element_type=jnp.float32).astype(jnp.bfloat16)
    qfull = query.astype(jnp.float32).reshape(rows, KV_HEADS, groups, HEAD_DIM)
    knew = key_new.astype(jnp.float32).reshape(rows, KV_HEADS, HEAD_DIM)
    vnew = value_new.astype(jnp.float32).reshape(rows, KV_HEADS, HEAD_DIM)
    kcache = cache_keys.astype(jnp.float32)
    vcache = cache_values.astype(jnp.float32)
    valid = (jnp.arange(CACHE, dtype=jnp.int32)[None, :] < lengths[:, None])[:, None, None, :]
    first = jnp.einsum('sgqd,spgd->sgqp', qfull[..., :half], kcache[..., :half]) * scale
    first_own = jnp.einsum('sgqd,sgd->sgq', qfull[..., :half], knew[..., :half]) * scale
    second = jnp.einsum('sgqd,spgd->sgqp', qfull[..., half:], kcache[..., half:]) * scale
    second_own = jnp.einsum('sgqd,sgd->sgq', qfull[..., half:], knew[..., half:]) * scale
    prob_one, own_one = softmax_pair(first, first_own, valid)
    prob_two, own_two = softmax_pair(second, second_own, valid)
    lam = mix_lambda.astype(jnp.float32).reshape(KV_HEADS, groups)
    weights = (prob_one - lam[None, :, :, None] * prob_two).astype(jnp.bfloat16)
    own_weights = (own_one - lam[None] * own_two).astype(jnp.bfloat16)
    mixed = jnp.einsum('sgqp,spgd->sgqd', weights.astype(jnp.float32), vcache)
    mixed = mixed + own_weights.astype(jnp.float32)[..., None] * vnew[:, :, None, :]
    heads = rms_norm(mixed, head_gain, 1e-05).astype(jnp.bfloat16).reshape(rows, HEADS * HEAD_DIM)
    hidden_state = xfull + jnp.dot(heads, out_w, preferred_element_type=jnp.float32)
    ffn_in = rms_norm(hidden_state, ffn_gain, 1e-06).astype(jnp.bfloat16)
    return (hidden_state, ffn_in, key_new, value_new)

def reference(tokens, lengths, cache_keys, cache_values, query_w, key_w, value_w, out_w, mix_lambda, head_gain, attn_gain, ffn_gain, routes, route_weights, exp_gate, exp_up, exp_down, dense_gate, dense_up, dense_down, branch_gate):
    blocks = tokens.shape[0] // SEQ_DEV

    def one_block(pieces):
        return attend_block(pieces[0], pieces[1], pieces[2], pieces[3], query_w, key_w, value_w, out_w, mix_lambda, head_gain, attn_gain, ffn_gain)
    hidden_state, ffn_in, key_new, value_new = lax.map(one_block, (tokens.reshape(blocks, SEQ_DEV, D), lengths.reshape(blocks, SEQ_DEV), cache_keys.reshape(blocks, SEQ_DEV, CACHE, KV_HEADS, HEAD_DIM), cache_values.reshape(blocks, SEQ_DEV, CACHE, KV_HEADS, HEAD_DIM)))
    hidden_state = hidden_state.reshape(TOKENS, D)
    ffn_in = ffn_in.reshape(TOKENS, D)
    key_new = key_new.reshape(TOKENS, KV_HEADS * HEAD_DIM)
    value_new = value_new.reshape(TOKENS, KV_HEADS * HEAD_DIM)
    slots = N_EP * CAP

    def one_expert(total, expert):
        match = routes == expert
        hit = jnp.any(match, axis=-1)
        weight = lax.optimization_barrier(jnp.sum(jnp.where(match, route_weights.astype(jnp.float32), 0.0), axis=-1))
        rank = jnp.cumsum(hit.astype(jnp.int32)) - 1
        select = hit[None, :] & (rank[None, :] == jnp.arange(slots, dtype=jnp.int32)[:, None])
        chosen = jnp.dot(select.astype(jnp.bfloat16), ffn_in, preferred_element_type=jnp.float32).astype(jnp.bfloat16)
        start = (expert * EXP_FF).astype(jnp.int32)
        w_gate = lax.dynamic_slice_in_dim(exp_gate, start, EXP_FF, 1)
        w_up = lax.dynamic_slice_in_dim(exp_up, start, EXP_FF, 1)
        w_down = lax.dynamic_slice_in_dim(exp_down, start, EXP_FF, 0)
        gate_part = jnp.dot(chosen, w_gate, preferred_element_type=jnp.float32)
        up_part = jnp.dot(chosen, w_up, preferred_element_type=jnp.float32)
        act = (jax.nn.silu(gate_part) * up_part).astype(jnp.bfloat16)
        result = jnp.dot(act, w_down, preferred_element_type=jnp.float32)
        back = jnp.dot(select.astype(jnp.float32).T, result, precision=lax.Precision.HIGHEST)
        return (total + weight[:, None] * back, None)
    routed, unused = lax.scan(one_expert, jnp.zeros((TOKENS, D), jnp.float32), jnp.arange(EXPERTS, dtype=jnp.int32))
    row_span = D // BLOCKS
    col_span = DENSE_FF // SPLIT
    gate_full = dense_gate.reshape(BLOCKS, SPLIT, row_span, col_span).transpose(0, 2, 1, 3).reshape(D, DENSE_FF)
    up_full = dense_up.reshape(BLOCKS, SPLIT, row_span, col_span).transpose(0, 2, 1, 3).reshape(D, DENSE_FF)
    down_full = dense_down.reshape(BLOCKS, SPLIT, col_span, row_span).transpose(1, 2, 0, 3).reshape(DENSE_FF, D)
    gate_part = jnp.dot(ffn_in, gate_full, preferred_element_type=jnp.float32)
    up_part = jnp.dot(ffn_in, up_full, preferred_element_type=jnp.float32)
    dense_act = (jax.nn.silu(gate_part) * up_part).astype(jnp.bfloat16)
    dense = jnp.dot(dense_act, down_full, preferred_element_type=jnp.float32)
    gate = jax.nn.sigmoid(jnp.dot(ffn_in, branch_gate, preferred_element_type=jnp.float32))
    output = (hidden_state + routed + gate[:, None] * dense).astype(jnp.bfloat16)
    return (output, key_new, value_new)
```

```python
import functools

import jax
import jax.numpy as jnp
from jax import lax
from jax.experimental import pallas as pl
from jax.experimental.pallas import tpu as pltpu
from jax.sharding import PartitionSpec as P

HEADS = 8
KV_HEADS = 2
HEAD_DIM = 128
SEQ_DEV = 4
SPLIT = 16
EXPERTS = 8
D = 2048
SIDE = 128
WIDE = D + SIDE
HID = 384
PART = 48
CHUNKS = 4
COLS = D // CHUNKS
MESH = pl.DeviceIdType.MESH
NT = (((1,), (1,)), ((), ()))


def rms_norm(values, gain, epsilon):
    scale = lax.rsqrt(jnp.mean(values * values, axis=-1, keepdims=True) + epsilon)
    return values * scale * gain


def softmax_pair(scores, own_score, valid):
    masked = jnp.where(valid, scores, -jnp.inf)
    largest = jnp.maximum(jnp.max(masked, axis=-1), own_score)
    raised = jnp.where(valid, jnp.exp(scores - largest[..., None]), 0.0)
    own_raised = jnp.exp(own_score - largest)
    total = jnp.sum(raised, axis=-1) + own_raised
    return (raised / total[..., None], own_raised / total)


def remote(src, dst, send, recv, device):
    return pltpu.make_async_remote_copy(
        src_ref=src, dst_ref=dst, send_sem=send, recv_sem=recv,
        device_id=(device,), device_id_type=MESH,
    )


def rows16(block, count=16):
    return pl.ds(pl.multiple_of(block * 16, 16), count)


def ffn_kernel(
    x_ref, hid_ref, wg_hbm, wu_hbm, wd_hbm, dg_ref, du_ref, dd_ref,
    out_ref,
    wgu, wdx, wsend, wrecv, own4, pack, xown, xpart, act, acc, psend, drecv, csend, crecv,
    bsum, bsend, brecv, fa, aown, asend, arecv,
    wsem, rs_w, rr_w, as_s, as_r, bs_s, bs_r, cs_s, cs_r, ds_s, ds_r,
    d2s, d2r, c2s, c2r, b2s, b2r, a2s, a2r,
):
    me = lax.axis_index("ep")
    core = lax.rem(me, 2)
    x = lax.rem(lax.div(me, 2), 4)
    y = lax.rem(lax.div(me, 8), 4)
    z = lax.div(me, 32)
    other = 1 - core
    a, sa = x * other + y * core, 2 * other + 8 * core
    b, sb = y * other + z * core, 8 * other + 32 * core
    c, sc = z * other + x * core, 32 * other + 2 * core
    row_block = lax.div(me, SPLIT)
    partner = me + other - core

    def ring(coord, stride, d):
        new = lax.rem(coord + d, 4)
        return new, me + (new - coord) * stride

    def group(d):
        new = lax.rem(row_block + d, 8)
        return new, me + (new - row_block) * SPLIT

    loads = []
    for n in range(3):
        cols = pl.ds(128 * n, 128)
        loads.append(pltpu.make_async_copy(wg_hbm.at[:, cols], wgu.at[n, :, pl.ds(0, 128)], wsem.at[2 * n]))
        loads.append(pltpu.make_async_copy(wu_hbm.at[:, cols], wgu.at[n, :, pl.ds(128, 128)], wsem.at[2 * n + 1]))
    loads.append(pltpu.make_async_copy(wd_hbm, wdx.at[pl.ds(0, HID)], wsem.at[6]))
    for load in loads:
        load.start()

    barrier = pltpu.get_barrier_semaphore()
    for coord, stride in ((a, sa), (b, sb), (c, sc)):
        for d in (1, 2, 3):
            pl.semaphore_signal(barrier, inc=1, device_id=(ring(coord, stride, d)[1],), device_id_type=MESH)
    for d in range(1, 8):
        pl.semaphore_signal(barrier, inc=1, device_id=(group(d)[1],), device_id_type=MESH)
    pl.semaphore_signal(barrier, inc=1, device_id=(partner,), device_id_type=MESH)
    pl.semaphore_wait(barrier, 17)

    sends = []

    def start(*args):
        copy = remote(*args)
        copy.start()
        sends.append(copy)
        return copy

    arrive_a = [start(x_ref, own4.at[a], as_s.at[d], as_r.at[d], ring(a, sa, d + 1)[1]) for d in range(3)]
    own4[a] = x_ref[...]

    eye = (
        lax.broadcasted_iota(jnp.int32, (384, 352), 0) == lax.broadcasted_iota(jnp.int32, (384, 352), 1)
    ).astype(jnp.bfloat16)
    gate_t = lax.dot_general(eye, dg_ref[...], NT, preferred_element_type=jnp.float32).astype(jnp.bfloat16)
    up_t = lax.dot_general(eye, du_ref[...], NT, preferred_element_type=jnp.float32).astype(jnp.bfloat16)
    for r in range(8):
        wsend[r, 0:PART] = gate_t[PART * r : PART * (r + 1)]
        wsend[r, PART : 2 * PART] = up_t[PART * r : PART * (r + 1)]
        if r < 7:
            wsend[r, 2 * PART :] = dd_ref[PART * r : PART * (r + 1)]
        else:
            wsend[r, 2 * PART : 2 * PART + 16] = dd_ref[336:352]
            wsend[r, 2 * PART + 16 :] = jnp.zeros((32, 256), jnp.bfloat16)
    arrive_w = []
    for d in range(7):
        to, device = group(d + 1)
        arrive_w.append(start(wsend.at[to], wrecv.at[row_block], rs_w.at[d], rr_w.at[d], device))
    wrecv[row_block] = wsend[row_block]

    for copy in arrive_a:
        copy.wait_recv()
    for j in range(4):
        pack[4 * j : 4 * j + 4] = own4[j].astype(jnp.float32)
    mine = 4 * c + b
    xown[rows16(mine)] = pack[...].astype(jnp.bfloat16)

    arrive_b = [
        start(xown.at[rows16(mine)], xown.at[rows16(mine)], bs_s.at[d], bs_r.at[d], ring(b, sb, d + 1)[1])
        for d in range(3)
    ]
    arrive_c, arrive_d = {}, []

    def spread(db):
        block = 4 * c + lax.rem(b + 4 - db, 4)
        for dc in (1, 3, 2):
            arrive_c[db, dc] = start(
                xown.at[rows16(block)], xown.at[rows16(block)],
                cs_s.at[3 * db + dc - 1], cs_r.at[3 * db + dc - 1], ring(c, sc, dc)[1],
            )
        across(block)

    def across(block):
        k = len(arrive_d)
        arrive_d.append(start(xown.at[rows16(block)], xpart.at[rows16(block)], ds_s.at[k], ds_r.at[k], partner))

    spread(0)
    for db in (1, 3, 2):
        arrive_b[db - 1].wait_recv()
        spread(db)
    for db in (0, 1, 3, 2):
        for dc in (1, 3, 2):
            arrive_c[db, dc].wait_recv()
            across(4 * lax.rem(c + 4 - dc, 4) + lax.rem(b + 4 - db, 4))

    for load in loads:
        load.wait()
    for copy in arrive_w:
        copy.wait_recv()
    wdx[HID + PART :] = jnp.zeros((128 - PART, D), jnp.bfloat16)
    for r in range(8):
        wdx[HID : HID + PART, 256 * r : 256 * (r + 1)] = wrecv[r, 2 * PART :]

    lane = lax.broadcasted_iota(jnp.int32, (256, SIDE), 1)

    def hidden(rows, k):
        side = rows[:, D:].astype(jnp.float32)
        expert = lax.div(me, SPLIT)
        weight = jnp.sum(jnp.where((lane == expert) | (lane == expert + 8), side, 0.0), axis=1, keepdims=True)
        gate = jnp.sum(jnp.where((lane == 16) | (lane == 17), side, 0.0), axis=1, keepdims=True)
        for n in range(3):
            both = jnp.dot(rows[:, :D], wgu[n], preferred_element_type=jnp.float32)
            first, second = both[:, :128], both[:, 128:]
            act[k, :, 128 * n : 128 * (n + 1)] = (first * jax.nn.sigmoid(first) * second * weight).astype(jnp.bfloat16)
        both = jnp.zeros((256, 128), jnp.float32)
        for r in range(8):
            both += lax.dot_general(
                rows[:, 256 * r : 256 * (r + 1)], wrecv[r, 0:128], NT, preferred_element_type=jnp.float32
            )
        second = pltpu.roll(both, 128 - PART, 1)
        value = both * jax.nn.sigmoid(both) * second * gate
        act[k, :, HID:] = jnp.where(lane < PART, value, 0.0).astype(jnp.bfloat16)

    hidden(xown, 0)
    for copy in arrive_d:
        copy.wait_recv()
    hidden(xpart, 1)

    arrive_2 = []
    for n in range(CHUNKS):
        cols = slice(COLS * n, COLS * (n + 1))
        psend[n] = jnp.dot(act[1], wdx[:, cols], preferred_element_type=jnp.float32).astype(jnp.bfloat16)
        arrive_2.append(start(psend.at[n], drecv.at[n], d2s.at[n], d2r.at[n], partner))
        acc[n] = jnp.dot(act[0], wdx[:, cols], preferred_element_type=jnp.float32)

    def ahead(n, coord, stride, src, dst, send_sem, recv_sem, height):
        copies = []
        for d in (1, 3, 2):
            to, device = ring(coord, stride, d)
            k = 3 * n + d - 1
            copies.append(
                start(
                    src.at[n, pl.ds(pl.multiple_of(to * height, height), height)], dst.at[n, d - 1],
                    send_sem.at[k], recv_sem.at[k], device,
                )
            )
        return copies

    arrive_c2 = []
    for n in range(CHUNKS):
        arrive_2[n].wait_recv()
        total = acc[n] + drecv[n].astype(jnp.float32)
        acc[n] = total
        csend[n] = total.astype(jnp.bfloat16)
        arrive_c2.append(ahead(n, c, sc, csend, crecv, c2s, c2r, 64))
    arrive_b2 = []
    for n in range(CHUNKS):
        for copy in arrive_c2[n]:
            copy.wait_recv()
        total = acc[n, pl.ds(pl.multiple_of(64 * c, 64), 64)]
        for d in range(3):
            total = total + crecv[n, d].astype(jnp.float32)
        bsum[n] = total
        bsend[n] = total.astype(jnp.bfloat16)
        arrive_b2.append(ahead(n, b, sb, bsend, brecv, b2s, b2r, 16))
    arrive_a2 = []
    for n in range(CHUNKS):
        for copy in arrive_b2[n]:
            copy.wait_recv()
        total = bsum[n, rows16(b)]
        for d in range(3):
            total = total + brecv[n, d].astype(jnp.float32)
        fa[n] = total
        for j in range(4):
            piece = fa[n, 4 * j : 4 * j + 4]
            aown[n, j] = piece
            asend[n, j] = piece.astype(jnp.bfloat16)
        copies = []
        for d in (1, 3, 2):
            to, device = ring(a, sa, d)
            k = 3 * n + d - 1
            copies.append(start(asend.at[n, to], arecv.at[n, d - 1], a2s.at[k], a2r.at[k], device))
        arrive_a2.append(copies)
    for n in range(CHUNKS):
        cols = slice(COLS * n, COLS * (n + 1))
        for copy in arrive_a2[n]:
            copy.wait_recv()
        total = hid_ref[:, cols] + aown[n, a]
        for d in range(3):
            total = total + arecv[n, d].astype(jnp.float32)
        out_ref[:, cols] = total.astype(jnp.bfloat16)
    for copy in sends:
        copy.wait_send()


def ffn(x, hidden_state, wg, wu, wd, dg, du, dd):
    bf, f32 = jnp.bfloat16, jnp.float32
    dma = pltpu.SemaphoreType.DMA
    vmem = pl.BlockSpec(memory_space=pltpu.VMEM)
    anywhere = pl.BlockSpec(memory_space=pl.ANY)
    return pl.pallas_call(
        ffn_kernel,
        out_shape=jax.ShapeDtypeStruct((SEQ_DEV, D), bf),
        in_specs=[vmem, vmem, anywhere, anywhere, anywhere, vmem, vmem, vmem],
        out_specs=vmem,
        scratch_shapes=[
            pltpu.VMEM((3, D, 256), bf),
            pltpu.VMEM((512, D), bf),
            pltpu.VMEM((8, 3 * PART, 256), bf),
            pltpu.VMEM((8, 3 * PART, 256), bf),
            pltpu.VMEM((4, 4, WIDE), bf),
            pltpu.VMEM((16, WIDE), f32),
            pltpu.VMEM((256, WIDE), bf),
            pltpu.VMEM((256, WIDE), bf),
            pltpu.VMEM((2, 256, 512), bf),
            pltpu.VMEM((CHUNKS, 256, COLS), f32),
            pltpu.VMEM((CHUNKS, 256, COLS), bf),
            pltpu.VMEM((CHUNKS, 256, COLS), bf),
            pltpu.VMEM((CHUNKS, 256, COLS), bf),
            pltpu.VMEM((CHUNKS, 3, 64, COLS), bf),
            pltpu.VMEM((CHUNKS, 64, COLS), f32),
            pltpu.VMEM((CHUNKS, 64, COLS), bf),
            pltpu.VMEM((CHUNKS, 3, 16, COLS), bf),
            pltpu.VMEM((CHUNKS, 16, COLS), f32),
            pltpu.VMEM((CHUNKS, 4, 4, COLS), f32),
            pltpu.VMEM((CHUNKS, 4, 4, COLS), bf),
            pltpu.VMEM((CHUNKS, 3, 4, COLS), bf),
            dma((7,)), dma((7,)), dma((7,)), dma((3,)), dma((3,)), dma((3,)), dma((3,)),
            dma((12,)), dma((12,)), dma((16,)), dma((16,)),
            dma((CHUNKS,)), dma((CHUNKS,)),
            dma((3 * CHUNKS,)), dma((3 * CHUNKS,)), dma((3 * CHUNKS,)), dma((3 * CHUNKS,)),
            dma((3 * CHUNKS,)), dma((3 * CHUNKS,)),
        ],
        compiler_params=pltpu.CompilerParams(
            collective_id=0, has_side_effects=True, vmem_limit_bytes=48 * 1024 * 1024
        ),
    )(x, hidden_state, wg, wu, wd, dg, du, dd)


def per_device(
    tokens, lengths, cache_keys, cache_values, query_w, key_w, value_w, out_w, mix_lambda, head_gain,
    attn_gain, ffn_gain, routes, route_weights, exp_gate, exp_up, exp_down, dense_gate, dense_up,
    dense_down, branch_gate,
):
    rows = tokens.shape[0]
    groups = HEADS // KV_HEADS
    half = HEAD_DIM // 2
    scale = (HEAD_DIM // 2) ** (-0.5)
    cache_len = cache_keys.shape[1]
    f32 = jnp.float32
    xfull = tokens.astype(f32)
    normed = rms_norm(xfull, attn_gain, 1e-06).astype(jnp.bfloat16)
    query = jnp.dot(normed, query_w, preferred_element_type=f32).astype(jnp.bfloat16)
    key_new = jnp.dot(normed, key_w, preferred_element_type=f32).astype(jnp.bfloat16)
    value_new = jnp.dot(normed, value_w, preferred_element_type=f32).astype(jnp.bfloat16)
    qheads = query.reshape(rows, KV_HEADS, groups, HEAD_DIM)
    knew = key_new.reshape(rows, KV_HEADS, HEAD_DIM)
    vnew = value_new.reshape(rows, KV_HEADS, HEAD_DIM)
    valid = (jnp.arange(cache_len, dtype=jnp.int32)[None, :] < lengths[:, None])[:, None, None, :]
    pairs = []
    for part in (slice(0, half), slice(half, HEAD_DIM)):
        scores = jnp.einsum("sgqd,spgd->sgqp", qheads[..., part], cache_keys[..., part], preferred_element_type=f32)
        own = jnp.einsum("sgqd,sgd->sgq", qheads[..., part], knew[..., part], preferred_element_type=f32)
        pairs.append(softmax_pair(scores * scale, own * scale, valid))
    (prob_one, own_one), (prob_two, own_two) = pairs
    lam = mix_lambda.reshape(KV_HEADS, groups)
    weights = (prob_one - lam[None, :, :, None] * prob_two).astype(jnp.bfloat16)
    own_weights = (own_one - lam[None] * own_two).astype(jnp.bfloat16)
    mixed = jnp.einsum("sgqp,spgd->sgqd", weights, cache_values, preferred_element_type=f32)
    mixed = mixed + own_weights.astype(f32)[..., None] * vnew.astype(f32)[:, :, None, :]
    heads = rms_norm(mixed, head_gain, 1e-05).astype(jnp.bfloat16).reshape(rows, HEADS * HEAD_DIM)
    hidden_state = xfull + jnp.dot(heads, out_w, preferred_element_type=f32)
    ffn_in = rms_norm(hidden_state, ffn_gain, 1e-06).astype(jnp.bfloat16)
    gate = jax.nn.sigmoid(jnp.dot(ffn_in, branch_gate, preferred_element_type=f32))
    match = routes[:, :, None] == jnp.arange(EXPERTS, dtype=jnp.int32)
    weight = jnp.sum(jnp.where(match, route_weights[:, :, None], 0.0), axis=1)
    wide = jnp.concatenate([weight, weight, gate[:, None], gate[:, None]], axis=1)
    high = wide.astype(jnp.bfloat16)
    low = (wide - high.astype(f32)).astype(jnp.bfloat16)
    place = jnp.arange(18)
    side = jnp.where((place < 8) | (place == 16), high, low)
    x = jnp.concatenate([ffn_in, side, jnp.zeros((rows, SIDE - 18), jnp.bfloat16)], axis=1)
    output = ffn(
        x, hidden_state, exp_gate, exp_up, exp_down, dense_gate[0], dense_up[0], dense_down[0]
    )
    return (output, key_new, value_new)


def solution(mesh):
    placed = (
        P("ep", None), P("ep"), P("ep", None, None, None), P("ep", None, None, None),
        P(), P(), P(), P(), P(), P(), P(), P(),
        P("ep", None), P("ep", None), P(None, "ep"), P(None, "ep"), P("ep", None),
        P("ep", None, None), P("ep", None, None), P("ep", None, None), P(),
    )
    return jax.shard_map(
        per_device,
        mesh=mesh,
        in_specs=placed,
        out_specs=(P("ep", None), P("ep", None), P("ep", None)),
        check_vma=False,
    )
```

```python
import jax
import jax.numpy as jnp
from jax import lax
from jax.experimental import pallas as pl
from jax.experimental.pallas import tpu as pltpu
from jax.sharding import PartitionSpec as P

HEADS = 8
KV_HEADS = 2
HEAD_DIM = 128
SEQ_DEV = 4
CACHE = 1024
SPLIT = 16
D = 2048
SIDE = 128
WIDE = D + SIDE
HID = 384
PART = 48
CHUNKS = 4
VMEM_LIMIT = 67043328
COLS = D // CHUNKS
MESH = pl.DeviceIdType.MESH
NT = (((1,), (1,)), ((), ()))


def rms_norm(values, gain, epsilon):
    scale = lax.rsqrt(jnp.mean(values * values, axis=-1, keepdims=True) + epsilon)
    return values * scale * gain


def remote(src, dst, send, recv, device):
    return pltpu.make_async_remote_copy(
        src_ref=src, dst_ref=dst, send_sem=send, recv_sem=recv,
        device_id=(device,), device_id_type=MESH,
    )


def rows16(block, count=16):
    return pl.ds(pl.multiple_of(block * 16, 16), count)


def layer_kernel(
    len_ref, lam_ref, routes_ref, rweights_ref, tok_ref, again_ref, fgain_ref, hgain_ref, bgate_ref,
    keys_hbm, values_hbm, qw_hbm, kw_hbm, vw_hbm, ow_hbm,
    wg_hbm, wu_hbm, wd_hbm, dg_hbm, du_hbm, dd_hbm,
    out_ref, newk_ref, newv_ref,
    keys, values, qw, kvw, ow, dg_ref, du_ref, dd_ref, qf, qs, hf, hid_ref, x_ref,
    wgu, wdx, wsend, wrecv, own4, pack, xown, xpart, act, acc, psend, drecv, csend, crecv,
    bsum, bsend, brecv, fa, aown, asend, arecv,
    dsem, qsem, ksem, vsem, osem,
    wsem, rs_w, rr_w, as_s, as_r, bs_s, bs_r, cs_s, cs_r, ds_s, ds_r,
    d2s, d2r, c2s, c2r, b2s, b2r, a2s, a2r,
):
    me = lax.axis_index("ep")
    core = lax.rem(me, 2)
    x = lax.rem(lax.div(me, 2), 4)
    y = lax.rem(lax.div(me, 8), 4)
    z = lax.div(me, 32)
    other = 1 - core
    a, sa = x * other + y * core, 2 * other + 8 * core
    b, sb = y * other + z * core, 8 * other + 32 * core
    c, sc = z * other + x * core, 32 * other + 2 * core
    row_block = lax.div(me, SPLIT)
    partner = me + other - core

    def ring(coord, stride, d):
        new = lax.rem(coord + d, 4)
        return new, me + (new - coord) * stride

    def group(d):
        new = lax.rem(row_block + d, 8)
        return new, me + (new - row_block) * SPLIT

    bf, f32 = jnp.bfloat16, jnp.float32

    def fetch(src, dst, sem):
        copy = pltpu.make_async_copy(src, dst, sem)
        copy.start()
        return copy

    dense_in = [fetch(dg_hbm, dg_ref, dsem.at[0]), fetch(du_hbm, du_ref, dsem.at[1]), fetch(dd_hbm, dd_ref, dsem.at[2])]
    proj_in = []
    for n in range(4):
        cols = pl.ds(256 * n, 256)
        proj_in.append(fetch(qw_hbm.at[:, cols], qw.at[:, cols], qsem.at[n]))
    proj_in.append(fetch(kw_hbm, kvw.at[:, pl.ds(0, 256)], qsem.at[4]))
    proj_in.append(fetch(vw_hbm, kvw.at[:, pl.ds(256, 256)], qsem.at[5]))
    span = [pl.ds(2 * CACHE * s, 2 * CACHE) for s in range(SEQ_DEV)]
    keys_in = [fetch(keys_hbm.at[span[s]], keys.at[s], ksem.at[s]) for s in range(SEQ_DEV)]
    values_in = [fetch(values_hbm.at[span[s]], values.at[s], vsem.at[s]) for s in range(SEQ_DEV)]
    out_in = [
        fetch(ow_hbm.at[:, pl.ds(512 * n, 512)], ow.at[:, pl.ds(512 * n, 512)], osem.at[n]) for n in range(4)
    ]

    barrier = pltpu.get_barrier_semaphore()
    for coord, stride in ((a, sa), (b, sb), (c, sc)):
        for d in (1, 2, 3):
            pl.semaphore_signal(barrier, inc=1, device_id=(ring(coord, stride, d)[1],), device_id_type=MESH)
    for d in range(1, 8):
        pl.semaphore_signal(barrier, inc=1, device_id=(group(d)[1],), device_id_type=MESH)
    pl.semaphore_signal(barrier, inc=1, device_id=(partner,), device_id_type=MESH)

    sends = []

    def start(*args):
        copy = remote(*args)
        copy.start()
        sends.append(copy)
        return copy

    for copy in dense_in:
        copy.wait()
    for k, tile in enumerate((dg_ref, du_ref, dd_ref)):
        for r in range(7):
            wsend[r, PART * k : PART * (k + 1)] = tile[PART * r : PART * (r + 1)]
        wsend[7, PART * k : PART * k + 16] = tile[336:352]
        wsend[7, PART * k + 16 : PART * (k + 1)] = jnp.zeros((32, 256), bf)
    pl.semaphore_wait(barrier, 17)
    arrive_w = []
    for d in range(7):
        to, device = group(d + 1)
        arrive_w.append(start(wsend.at[to], wrecv.at[row_block], rs_w.at[d], rr_w.at[d], device))
    wrecv[row_block] = wsend[row_block]


    normed = rms_norm(tok_ref[...].astype(f32), again_ref[...], 1e-06).astype(bf)
    for n in range(4):
        proj_in[n].wait()
        cols = slice(256 * n, 256 * (n + 1))
        qf[:, cols] = jnp.dot(normed, qw[:, cols], preferred_element_type=f32).astype(bf).astype(f32)
    proj_in[4].wait()
    proj_in[5].wait()
    new = jnp.dot(normed, kvw[...], preferred_element_type=f32).astype(bf)
    newk_ref[...] = new[:, :256]
    newv_ref[...] = new[:, 256:]
    qf[:, HEADS * HEAD_DIM :] = new.astype(f32)
    for s in range(SEQ_DEV):
        for h in range(HEADS):
            qs[s, h : h + 1] = qf[s : s + 1, HEAD_DIM * h : HEAD_DIM * (h + 1)]

    loads = []
    for n in range(3):
        cols = pl.ds(128 * n, 128)
        loads.append(fetch(wg_hbm.at[:, cols], wgu.at[n, :, pl.ds(0, 128)], wsem.at[2 * n]))
        loads.append(fetch(wu_hbm.at[:, cols], wgu.at[n, :, pl.ds(128, 128)], wsem.at[2 * n + 1]))
    loads.append(fetch(wd_hbm, wdx.at[pl.ds(0, HID)], wsem.at[6]))

    head8 = lax.broadcasted_iota(jnp.int32, (HEADS, HEAD_DIM), 0)
    lane8 = lax.broadcasted_iota(jnp.int32, (HEADS, HEAD_DIM), 1)
    low_head, low_lane = head8 < HEADS // KV_HEADS, lane8 < HEAD_DIM // 2
    head1 = lax.broadcasted_iota(jnp.int32, (HEADS, 1), 0)
    lam = jnp.zeros((HEADS, 1), f32)
    for h in range(HEADS):
        lam = jnp.where(head1 == h, lam_ref[h], lam)
    slot = lax.broadcasted_iota(jnp.int32, (HEADS, 2 * CACHE), 1)
    kv_of = lax.broadcasted_iota(jnp.int32, (HEADS, 2 * CACHE), 0) // (HEADS // KV_HEADS)
    mine_kv = (slot & 1) == kv_of
    scale = (HEAD_DIM // 2) ** (-0.5)

    def probabilities(scores, own, valid):
        largest = jnp.maximum(jnp.max(jnp.where(valid, scores, -jnp.inf), axis=1, keepdims=True), own)
        raised = jnp.where(valid, jnp.exp(scores - largest), 0.0)
        own_raised = jnp.exp(own - largest)
        total = jnp.sum(raised, axis=1, keepdims=True) + own_raised
        return raised, own_raised, 1.0 / total

    base = HEADS * HEAD_DIM
    for s in range(SEQ_DEV):
        q = qs[s]
        q_one, q_two = jnp.where(low_lane, q, 0.0), jnp.where(low_lane, 0.0, q)
        rows = [qf[s : s + 1, base + 128 * k : base + 128 * (k + 1)] for k in range(4)]
        own_key = jnp.where(low_head, rows[0], rows[1])
        own_value = jnp.where(low_head, rows[2], rows[3])
        own_one = jnp.sum(q_one * own_key, axis=1, keepdims=True) * scale
        own_two = jnp.sum(q_two * own_key, axis=1, keepdims=True) * scale
        keys_in[s].wait()
        both = jnp.concatenate([q_one, q_two], axis=0).astype(bf)
        scores = lax.dot_general(both, keys[s], NT, preferred_element_type=f32) * scale
        valid = mine_kv & (slot < 2 * len_ref[s])
        raised_one, own_one, inv_one = probabilities(scores[:HEADS], own_one, valid)
        raised_two, own_two, inv_two = probabilities(scores[HEADS:], own_two, valid)
        inv_two = inv_two * lam
        weights = (raised_one * inv_one - raised_two * inv_two).astype(bf)
        own_weight = (own_one * inv_one - own_two * inv_two).astype(bf).astype(f32)
        values_in[s].wait()
        mixed = jnp.dot(weights, values[s], preferred_element_type=f32) + own_weight * own_value
        mixed = rms_norm(mixed, hgain_ref[...], 1e-05)
        for h in range(HEADS):
            hf[s : s + 1, HEAD_DIM * h : HEAD_DIM * (h + 1)] = mixed[h : h + 1]
    heads = hf[...].astype(bf)
    for n in range(4):
        out_in[n].wait()
        cols = slice(512 * n, 512 * (n + 1))
        hid_ref[:, cols] = tok_ref[:, cols].astype(f32) + jnp.dot(heads, ow[:, cols], preferred_element_type=f32)
    ffn_in = rms_norm(hid_ref[...], fgain_ref[...], 1e-06).astype(bf)
    gate_row = bgate_ref[...].astype(f32)
    terms = jnp.zeros((SEQ_DEV, 128), f32)
    for k in range(16):
        terms = terms + ffn_in[:, 128 * k : 128 * (k + 1)].astype(f32) * gate_row[k : k + 1]
    gate = jax.nn.sigmoid(jnp.sum(terms, axis=1, keepdims=True))
    place = lax.broadcasted_iota(jnp.int32, (SEQ_DEV, SIDE), 1)
    row = lax.broadcasted_iota(jnp.int32, (SEQ_DEV, SIDE), 0)
    full = jnp.where((place == 16) | (place == 17), gate, 0.0)
    for t in range(SEQ_DEV):
        for k in range(2):
            chosen = (row == t) & (place < 16) & ((place & 7) == routes_ref[k, t])
            full = full + jnp.where(chosen, rweights_ref[k, t], 0.0)
    high = full.astype(bf).astype(f32)
    side = jnp.where((place < 8) | (place == 16), high, full - high)
    x_ref[:, :D] = ffn_in
    x_ref[:, D:] = side.astype(bf)

    arrive_a = [start(x_ref, own4.at[a], as_s.at[d], as_r.at[d], ring(a, sa, d + 1)[1]) for d in range(3)]
    own4[a] = x_ref[...]
    for copy in arrive_a:
        copy.wait_recv()
    for j in range(4):
        pack[4 * j : 4 * j + 4] = own4[j].astype(jnp.float32)
    mine = 4 * c + b
    xown[rows16(mine)] = pack[...].astype(jnp.bfloat16)

    arrive_b = [
        start(xown.at[rows16(mine)], xown.at[rows16(mine)], bs_s.at[d], bs_r.at[d], ring(b, sb, d + 1)[1])
        for d in range(3)
    ]
    arrive_c, arrive_d = {}, []

    def spread(db):
        block = 4 * c + lax.rem(b + 4 - db, 4)
        for dc in (1, 3, 2):
            arrive_c[db, dc] = start(
                xown.at[rows16(block)], xown.at[rows16(block)],
                cs_s.at[3 * db + dc - 1], cs_r.at[3 * db + dc - 1], ring(c, sc, dc)[1],
            )
        across(block)

    def across(block):
        k = len(arrive_d)
        arrive_d.append(start(xown.at[rows16(block)], xpart.at[rows16(block)], ds_s.at[k], ds_r.at[k], partner))

    spread(0)
    for db in (1, 3, 2):
        arrive_b[db - 1].wait_recv()
        spread(db)
    for db in (0, 1, 3, 2):
        for dc in (1, 3, 2):
            arrive_c[db, dc].wait_recv()
            across(4 * lax.rem(c + 4 - dc, 4) + lax.rem(b + 4 - db, 4))

    for load in loads:
        load.wait()
    for copy in arrive_w:
        copy.wait_recv()
    wdx[HID + PART :] = jnp.zeros((128 - PART, D), jnp.bfloat16)
    for r in range(8):
        wdx[HID : HID + PART, 256 * r : 256 * (r + 1)] = wrecv[r, 2 * PART :]

    lane = lax.broadcasted_iota(jnp.int32, (256, SIDE), 1)

    def hidden(rows, k):
        side = rows[:, D:].astype(jnp.float32)
        expert = lax.div(me, SPLIT)
        weight = jnp.sum(jnp.where((lane == expert) | (lane == expert + 8), side, 0.0), axis=1, keepdims=True)
        gate = jnp.sum(jnp.where((lane == 16) | (lane == 17), side, 0.0), axis=1, keepdims=True)
        for n in range(3):
            both = jnp.dot(rows[:, :D], wgu[n], preferred_element_type=jnp.float32)
            first, second = both[:, :128], both[:, 128:]
            act[k, :, 128 * n : 128 * (n + 1)] = (first * jax.nn.sigmoid(first) * second * weight).astype(jnp.bfloat16)
        both = jnp.zeros((256, 128), jnp.float32)
        for r in range(8):
            both += lax.dot_general(
                rows[:, 256 * r : 256 * (r + 1)], wrecv[r, 0:128], NT, preferred_element_type=jnp.float32
            )
        second = pltpu.roll(both, 128 - PART, 1)
        value = both * jax.nn.sigmoid(both) * second * gate
        act[k, :, HID:] = jnp.where(lane < PART, value, 0.0).astype(jnp.bfloat16)

    hidden(xown, 0)
    for copy in arrive_d:
        copy.wait_recv()
    hidden(xpart, 1)

    arrive_2 = []
    for n in range(CHUNKS):
        cols = slice(COLS * n, COLS * (n + 1))
        psend[n] = jnp.dot(act[1], wdx[:, cols], preferred_element_type=jnp.float32).astype(jnp.bfloat16)
        arrive_2.append(start(psend.at[n], drecv.at[n], d2s.at[n], d2r.at[n], partner))
        acc[n] = jnp.dot(act[0], wdx[:, cols], preferred_element_type=jnp.float32)

    def ahead(n, coord, stride, src, dst, send_sem, recv_sem, height):
        copies = []
        for d in (1, 3, 2):
            to, device = ring(coord, stride, d)
            k = 3 * n + d - 1
            copies.append(
                start(
                    src.at[n, pl.ds(pl.multiple_of(to * height, height), height)], dst.at[n, d - 1],
                    send_sem.at[k], recv_sem.at[k], device,
                )
            )
        return copies

    arrive_c2 = []
    for n in range(CHUNKS):
        arrive_2[n].wait_recv()
        total = acc[n] + drecv[n].astype(jnp.float32)
        acc[n] = total
        csend[n] = total.astype(jnp.bfloat16)
        arrive_c2.append(ahead(n, c, sc, csend, crecv, c2s, c2r, 64))
    arrive_b2 = []
    for n in range(CHUNKS):
        for copy in arrive_c2[n]:
            copy.wait_recv()
        total = acc[n, pl.ds(pl.multiple_of(64 * c, 64), 64)]
        for d in range(3):
            total = total + crecv[n, d].astype(jnp.float32)
        bsum[n] = total
        bsend[n] = total.astype(jnp.bfloat16)
        arrive_b2.append(ahead(n, b, sb, bsend, brecv, b2s, b2r, 16))
    arrive_a2 = []
    for n in range(CHUNKS):
        for copy in arrive_b2[n]:
            copy.wait_recv()
        total = bsum[n, rows16(b)]
        for d in range(3):
            total = total + brecv[n, d].astype(jnp.float32)
        fa[n] = total
        for j in range(4):
            piece = fa[n, 4 * j : 4 * j + 4]
            aown[n, j] = piece
            asend[n, j] = piece.astype(jnp.bfloat16)
        copies = []
        for d in (1, 3, 2):
            to, device = ring(a, sa, d)
            k = 3 * n + d - 1
            copies.append(start(asend.at[n, to], arecv.at[n, d - 1], a2s.at[k], a2r.at[k], device))
        arrive_a2.append(copies)
    for n in range(CHUNKS):
        cols = slice(COLS * n, COLS * (n + 1))
        for copy in arrive_a2[n]:
            copy.wait_recv()
        total = hid_ref[:, cols] + aown[n, a]
        for d in range(3):
            total = total + arecv[n, d].astype(jnp.float32)
        out_ref[:, cols] = total.astype(jnp.bfloat16)
    for copy in sends:
        copy.wait_send()


def per_device(
    tokens, lengths, cache_keys, cache_values, query_w, key_w, value_w, out_w, mix_lambda, head_gain,
    attn_gain, ffn_gain, routes, route_weights, exp_gate, exp_up, exp_down, dense_gate, dense_up,
    dense_down, branch_gate,
):
    bf, f32 = jnp.bfloat16, jnp.float32
    dma = pltpu.SemaphoreType.DMA
    vmem = pl.BlockSpec(memory_space=pltpu.VMEM)
    smem = pl.BlockSpec(memory_space=pltpu.SMEM)
    anywhere = pl.BlockSpec(memory_space=pl.ANY)
    kv = KV_HEADS * HEAD_DIM
    return pl.pallas_call(
        layer_kernel,
        out_shape=(
            jax.ShapeDtypeStruct((SEQ_DEV, D), bf),
            jax.ShapeDtypeStruct((SEQ_DEV, kv), bf),
            jax.ShapeDtypeStruct((SEQ_DEV, kv), bf),
        ),
        in_specs=[smem] * 4 + [vmem] * 5 + [anywhere] * 12,
        out_specs=(vmem, vmem, vmem),
        scratch_shapes=[
            pltpu.VMEM((SEQ_DEV, 2 * CACHE, HEAD_DIM), bf),
            pltpu.VMEM((SEQ_DEV, 2 * CACHE, HEAD_DIM), bf),
            pltpu.VMEM((D, HEADS * HEAD_DIM), bf),
            pltpu.VMEM((D, 2 * kv), bf),
            pltpu.VMEM((HEADS * HEAD_DIM, D), bf),
            pltpu.VMEM((352, 256), bf),
            pltpu.VMEM((352, 256), bf),
            pltpu.VMEM((352, 256), bf),
            pltpu.VMEM((SEQ_DEV, HEADS * HEAD_DIM + 2 * kv), f32),
            pltpu.VMEM((SEQ_DEV, HEADS, HEAD_DIM), f32),
            pltpu.VMEM((SEQ_DEV, HEADS * HEAD_DIM), f32),
            pltpu.VMEM((SEQ_DEV, D), f32),
            pltpu.VMEM((SEQ_DEV, WIDE), bf),
            pltpu.VMEM((3, D, 256), bf),
            pltpu.VMEM((512, D), bf),
            pltpu.VMEM((8, 3 * PART, 256), bf),
            pltpu.VMEM((8, 3 * PART, 256), bf),
            pltpu.VMEM((4, 4, WIDE), bf),
            pltpu.VMEM((16, WIDE), f32),
            pltpu.VMEM((256, WIDE), bf),
            pltpu.VMEM((256, WIDE), bf),
            pltpu.VMEM((2, 256, 512), bf),
            pltpu.VMEM((CHUNKS, 256, COLS), f32),
            pltpu.VMEM((CHUNKS, 256, COLS), bf),
            pltpu.VMEM((CHUNKS, 256, COLS), bf),
            pltpu.VMEM((CHUNKS, 256, COLS), bf),
            pltpu.VMEM((CHUNKS, 3, 64, COLS), bf),
            pltpu.VMEM((CHUNKS, 64, COLS), f32),
            pltpu.VMEM((CHUNKS, 64, COLS), bf),
            pltpu.VMEM((CHUNKS, 3, 16, COLS), bf),
            pltpu.VMEM((CHUNKS, 16, COLS), f32),
            pltpu.VMEM((CHUNKS, 4, 4, COLS), f32),
            pltpu.VMEM((CHUNKS, 4, 4, COLS), bf),
            pltpu.VMEM((CHUNKS, 3, 4, COLS), bf),
            dma((3,)), dma((6,)), dma((4,)), dma((4,)), dma((4,)),
            dma((7,)), dma((7,)), dma((7,)), dma((3,)), dma((3,)), dma((3,)), dma((3,)),
            dma((12,)), dma((12,)), dma((16,)), dma((16,)),
            dma((CHUNKS,)), dma((CHUNKS,)),
            dma((3 * CHUNKS,)), dma((3 * CHUNKS,)), dma((3 * CHUNKS,)), dma((3 * CHUNKS,)),
            dma((3 * CHUNKS,)), dma((3 * CHUNKS,)),
        ],
        compiler_params=pltpu.CompilerParams(
            collective_id=0, has_side_effects=True, vmem_limit_bytes=VMEM_LIMIT
        ),
    )(
        lengths, mix_lambda, routes.T, route_weights.T, tokens, attn_gain.reshape(1, D), ffn_gain.reshape(1, D), head_gain.reshape(1, HEAD_DIM),
        branch_gate.reshape(16, 128),
        cache_keys.reshape(-1, HEAD_DIM), cache_values.reshape(-1, HEAD_DIM), query_w, key_w, value_w, out_w,
        exp_gate, exp_up, exp_down, dense_gate[0].T, dense_up[0].T, dense_down[0],
    )


def solution(mesh):
    placed = (
        P("ep", None), P("ep"), P("ep", None, None, None), P("ep", None, None, None),
        P(), P(), P(), P(), P(), P(), P(), P(),
        P("ep", None), P("ep", None), P(None, "ep"), P(None, "ep"), P("ep", None),
        P("ep", None, None), P("ep", None, None), P("ep", None, None), P(),
    )
    return jax.shard_map(
        per_device,
        mesh=mesh,
        in_specs=placed,
        out_specs=(P("ep", None), P("ep", None), P("ep", None)),
        check_vma=False,
    )
```

```python
import jax
import jax.numpy as jnp
from jax import lax
from jax.experimental import pallas as pl
from jax.experimental.pallas import tpu as pltpu
from jax.sharding import PartitionSpec as P

HEADS = 8
KV_HEADS = 2
HEAD_DIM = 128
SEQ_DEV = 4
CACHE = 1024
SPLIT = 16
D = 2048
SIDE = 128
WIDE = D + SIDE
HID = 384
PART = 48
CHUNKS = 4
VMEM_LIMIT = 67043328 - 131072
COLS = D // CHUNKS
MESH = pl.DeviceIdType.MESH
NT = (((1,), (1,)), ((), ()))


def rms_norm(values, gain, epsilon):
    scale = lax.rsqrt(jnp.mean(values * values, axis=-1, keepdims=True) + epsilon)
    return values * scale * gain


def remote(src, dst, send, recv, device):
    return pltpu.make_async_remote_copy(
        src_ref=src, dst_ref=dst, send_sem=send, recv_sem=recv,
        device_id=(device,), device_id_type=MESH,
    )


def rows16(block, count=16):
    return pl.ds(pl.multiple_of(block * 16, 16), count)


def layer_kernel(
    len_hbm, lam_hbm, routes_hbm, rweights_hbm, tok_hbm, again_hbm, fgain_hbm, hgain_hbm, bgate_hbm,
    keys_hbm, values_hbm, qw_hbm, kw_hbm, vw_hbm, ow_hbm,
    wg_hbm, wu_hbm, wd_hbm, dg_hbm, du_hbm, dd_hbm,
    out_ref, newk_ref, newv_ref,
    len_ref, lam_ref, routes_ref, rweights_ref, tok_ref, again_ref, fgain_ref, hgain_ref, bgate_ref,
    keys, values, qw, kvw, ow, dg_ref, du_ref, dd_ref, qf, qs, sc, hf, hid_ref, x_ref,
    wgu, wdx, wsend, wrecv, own4, pack, xown, xpart, act, acc, psend, drecv, csend, crecv,
    bsum, bsend, brecv, fa, aown, asend, arecv,
    isem, dsem, qsem, ksem, vsem, osem,
    wsem, rs_w, rr_w, as_s, as_r, bs_s, bs_r, cs_s, cs_r, ds_s, ds_r,
    d2s, d2r, c2s, c2r, b2s, b2r, a2s, a2r,
):
    me = lax.axis_index("ep")
    core = lax.rem(me, 2)
    x = lax.rem(lax.div(me, 2), 4)
    y = lax.rem(lax.div(me, 8), 4)
    z = lax.div(me, 32)
    other = 1 - core
    a, sa = x * other + y * core, 2 * other + 8 * core
    b, sb = y * other + z * core, 8 * other + 32 * core
    c, sc_ = z * other + x * core, 32 * other + 2 * core
    row_block = lax.div(me, SPLIT)
    partner = me + other - core

    def ring(coord, stride, d):
        new = lax.rem(coord + d, 4)
        return new, me + (new - coord) * stride

    def group(d):
        new = lax.rem(row_block + d, 8)
        return new, me + (new - row_block) * SPLIT

    bf, f32 = jnp.bfloat16, jnp.float32

    def fetch(src, dst, sem):
        copy = pltpu.make_async_copy(src, dst, sem)
        copy.start()
        return copy

    small = (
        (tok_hbm, tok_ref), (again_hbm, again_ref), (len_hbm, len_ref), (lam_hbm, lam_ref),
        (routes_hbm, routes_ref), (rweights_hbm, rweights_ref), (fgain_hbm, fgain_ref),
        (hgain_hbm, hgain_ref), (bgate_hbm, bgate_ref),
    )
    small_in = [fetch(src, dst, isem.at[k]) for k, (src, dst) in enumerate(small)]
    dense_in = [
        fetch(src, dst, dsem.at[k])
        for k, (src, dst) in enumerate(((dg_hbm, dg_ref), (du_hbm, du_ref), (dd_hbm, dd_ref)))
    ]
    proj_in = []
    for n in range(4):
        cols = pl.ds(256 * n, 256)
        proj_in.append(fetch(qw_hbm.at[:, cols], qw.at[:, cols], qsem.at[n]))
    proj_in.append(fetch(kw_hbm, kvw.at[:, pl.ds(0, 256)], qsem.at[4]))
    proj_in.append(fetch(vw_hbm, kvw.at[:, pl.ds(256, 256)], qsem.at[5]))

    barrier = pltpu.get_barrier_semaphore()
    for coord, stride in ((a, sa), (b, sb), (c, sc_)):
        for d in (1, 2, 3):
            pl.semaphore_signal(barrier, inc=1, device_id=(ring(coord, stride, d)[1],), device_id_type=MESH)
    for d in range(1, 8):
        pl.semaphore_signal(barrier, inc=1, device_id=(group(d)[1],), device_id_type=MESH)
    pl.semaphore_signal(barrier, inc=1, device_id=(partner,), device_id_type=MESH)

    sends = []

    def start(*args):
        copy = remote(*args)
        copy.start()
        sends.append(copy)
        return copy

    span = [pl.ds(2 * CACHE * s, 2 * CACHE) for s in range(SEQ_DEV)]
    for copy in small_in:
        copy.wait()
    normed = rms_norm(tok_ref[...].astype(f32), again_ref[...], 1e-06).astype(bf)
    for n in range(4):
        proj_in[n].wait()
        cols = slice(256 * n, 256 * (n + 1))
        if n == 0:
            keys_in = [fetch(keys_hbm.at[span[s]], keys.at[s], ksem.at[s]) for s in range(SEQ_DEV)]
        if n == 2:
            values_in = [fetch(values_hbm.at[span[s]], values.at[s], vsem.at[s]) for s in range(SEQ_DEV)]
        qf[:, cols] = jnp.dot(normed, qw[:, cols], preferred_element_type=f32).astype(bf).astype(f32)
        if n == 1:
            for copy in dense_in:
                copy.wait()
            for k, tile in enumerate((dg_ref, du_ref, dd_ref)):
                for r in range(7):
                    wsend[r, PART * k : PART * (k + 1)] = tile[PART * r : PART * (r + 1)]
                wsend[7, PART * k : PART * k + 16] = tile[336:352]
                wsend[7, PART * k + 16 : PART * (k + 1)] = jnp.zeros((32, 256), bf)
            pl.semaphore_wait(barrier, 17)
            arrive_w = []
            for d in range(7):
                to, device = group(d + 1)
                arrive_w.append(start(wsend.at[to], wrecv.at[row_block], rs_w.at[d], rr_w.at[d], device))
            wrecv[row_block] = wsend[row_block]
    proj_in[4].wait()
    proj_in[5].wait()
    out_in = [
        fetch(ow_hbm.at[:, pl.ds(512 * n, 512)], ow.at[:, pl.ds(512 * n, 512)], osem.at[n]) for n in range(4)
    ]
    new = jnp.dot(normed, kvw[...], preferred_element_type=f32).astype(bf)
    newk_ref[...] = new[:, :256]
    newv_ref[...] = new[:, 256:]
    qf[:, HEADS * HEAD_DIM :] = new.astype(f32)
    for s in range(SEQ_DEV):
        for h in range(HEADS):
            qs[s, h : h + 1] = qf[s : s + 1, HEAD_DIM * h : HEAD_DIM * (h + 1)]

    head8 = lax.broadcasted_iota(jnp.int32, (HEADS, HEAD_DIM), 0)
    lane8 = lax.broadcasted_iota(jnp.int32, (HEADS, HEAD_DIM), 1)
    low_head, low_lane = head8 < HEADS // KV_HEADS, lane8 < HEAD_DIM // 2
    head1 = lax.broadcasted_iota(jnp.int32, (HEADS, 1), 0)
    lam = jnp.zeros((HEADS, 1), f32)
    for h in range(HEADS):
        lam = jnp.where(head1 == h, lam_ref[h], lam)
    slot = lax.broadcasted_iota(jnp.int32, (HEADS, 2 * CACHE), 1)
    kv_of = lax.broadcasted_iota(jnp.int32, (HEADS, 2 * CACHE), 0) // (HEADS // KV_HEADS)
    mine_kv = (slot & 1) == kv_of
    scale = (HEAD_DIM // 2) ** (-0.5)

    def probabilities(scores, own, valid):
        largest = jnp.maximum(jnp.max(jnp.where(valid, scores, -jnp.inf), axis=1, keepdims=True), own)
        raised = jnp.where(valid, jnp.exp(scores - largest), 0.0)
        own_raised = jnp.exp(own - largest)
        total = jnp.sum(raised, axis=1, keepdims=True) + own_raised
        return raised, own_raised, 1.0 / total

    base = HEADS * HEAD_DIM
    for s in range(SEQ_DEV):
        keys_in[s].wait()
    for s in range(SEQ_DEV):
        q = qs[s]
        both = jnp.concatenate([jnp.where(low_lane, q, 0.0), jnp.where(low_lane, 0.0, q)], axis=0).astype(bf)
        sc[s] = lax.dot_general(both, keys[s], NT, preferred_element_type=f32) * scale
    loads = []
    for n in range(3):
        cols = pl.ds(128 * n, 128)
        loads.append(fetch(wg_hbm.at[:, cols], wgu.at[n, :, pl.ds(0, 128)], wsem.at[2 * n]))
        loads.append(fetch(wu_hbm.at[:, cols], wgu.at[n, :, pl.ds(128, 128)], wsem.at[2 * n + 1]))
    loads.append(fetch(wd_hbm, wdx.at[pl.ds(0, HID)], wsem.at[6]))

    for s in range(SEQ_DEV):
        values_in[s].wait()
    for s in range(SEQ_DEV):
        q = qs[s]
        rows = [qf[s : s + 1, base + 128 * k : base + 128 * (k + 1)] for k in range(4)]
        own_score = q * jnp.where(low_head, rows[0], rows[1])
        own_value = jnp.where(low_head, rows[2], rows[3])
        own_one = jnp.sum(jnp.where(low_lane, own_score, 0.0), axis=1, keepdims=True) * scale
        own_two = jnp.sum(jnp.where(low_lane, 0.0, own_score), axis=1, keepdims=True) * scale
        valid = mine_kv & (slot < 2 * len_ref[s])
        raised_one, own_one, inv_one = probabilities(sc[s, :HEADS], own_one, valid)
        raised_two, own_two, inv_two = probabilities(sc[s, HEADS:], own_two, valid)
        inv_two = inv_two * lam
        weights = (raised_one * inv_one - raised_two * inv_two).astype(bf)
        own_weight = (own_one * inv_one - own_two * inv_two).astype(bf).astype(f32)
        mixed = jnp.dot(weights, values[s], preferred_element_type=f32) + own_weight * own_value
        mixed = rms_norm(mixed, hgain_ref[...], 1e-05)
        for h in range(HEADS):
            hf[s : s + 1, HEAD_DIM * h : HEAD_DIM * (h + 1)] = mixed[h : h + 1]
    heads = hf[...].astype(bf)
    for n in range(4):
        out_in[n].wait()
        cols = slice(512 * n, 512 * (n + 1))
        hid_ref[:, cols] = tok_ref[:, cols].astype(f32) + jnp.dot(heads, ow[:, cols], preferred_element_type=f32)
    ffn_in = rms_norm(hid_ref[...], fgain_ref[...], 1e-06).astype(bf)
    gate_row = bgate_ref[...].astype(f32)
    terms = jnp.zeros((SEQ_DEV, 128), f32)
    for k in range(16):
        terms = terms + ffn_in[:, 128 * k : 128 * (k + 1)].astype(f32) * gate_row[k : k + 1]
    gate = jax.nn.sigmoid(jnp.sum(terms, axis=1, keepdims=True))
    place = lax.broadcasted_iota(jnp.int32, (SEQ_DEV, SIDE), 1)
    row = lax.broadcasted_iota(jnp.int32, (SEQ_DEV, SIDE), 0)
    full = jnp.where((place == 16) | (place == 17), gate, 0.0)
    for t in range(SEQ_DEV):
        for k in range(2):
            chosen = (row == t) & (place < 16) & ((place & 7) == routes_ref[k, t])
            full = full + jnp.where(chosen, rweights_ref[k, t], 0.0)
    high = full.astype(bf).astype(f32)
    side = jnp.where((place < 8) | (place == 16), high, full - high)
    x_ref[:, :D] = ffn_in
    x_ref[:, D:] = side.astype(bf)

    arrive_a = [start(x_ref, own4.at[a], as_s.at[d], as_r.at[d], ring(a, sa, d + 1)[1]) for d in range(3)]
    own4[a] = x_ref[...]
    for copy in arrive_a:
        copy.wait_recv()
    for j in range(4):
        pack[4 * j : 4 * j + 4] = own4[j].astype(jnp.float32)
    mine = 4 * c + b
    xown[rows16(mine)] = pack[...].astype(jnp.bfloat16)

    arrive_b = [
        start(xown.at[rows16(mine)], xown.at[rows16(mine)], bs_s.at[d], bs_r.at[d], ring(b, sb, d + 1)[1])
        for d in range(3)
    ]
    arrive_c, arrive_d = {}, []

    def spread(db):
        block = 4 * c + lax.rem(b + 4 - db, 4)
        for dc in (1, 3, 2):
            arrive_c[db, dc] = start(
                xown.at[rows16(block)], xown.at[rows16(block)],
                cs_s.at[3 * db + dc - 1], cs_r.at[3 * db + dc - 1], ring(c, sc_, dc)[1],
            )
        across(block)

    def across(block):
        k = len(arrive_d)
        arrive_d.append(start(xown.at[rows16(block)], xpart.at[rows16(block)], ds_s.at[k], ds_r.at[k], partner))

    spread(0)
    for db in (1, 3, 2):
        arrive_b[db - 1].wait_recv()
        spread(db)
    for db in (0, 1, 3, 2):
        for dc in (1, 3, 2):
            arrive_c[db, dc].wait_recv()
            across(4 * lax.rem(c + 4 - dc, 4) + lax.rem(b + 4 - db, 4))

    for load in loads:
        load.wait()
    for copy in arrive_w:
        copy.wait_recv()
    wdx[HID + PART :] = jnp.zeros((128 - PART, D), jnp.bfloat16)
    for r in range(8):
        wdx[HID : HID + PART, 256 * r : 256 * (r + 1)] = wrecv[r, 2 * PART :]

    lane = lax.broadcasted_iota(jnp.int32, (256, SIDE), 1)

    def hidden(rows, k):
        side = rows[:, D:].astype(jnp.float32)
        expert = lax.div(me, SPLIT)
        weight = jnp.sum(jnp.where((lane == expert) | (lane == expert + 8), side, 0.0), axis=1, keepdims=True)
        gate = jnp.sum(jnp.where((lane == 16) | (lane == 17), side, 0.0), axis=1, keepdims=True)
        for n in range(3):
            both = jnp.dot(rows[:, :D], wgu[n], preferred_element_type=jnp.float32)
            first, second = both[:, :128], both[:, 128:]
            act[k, :, 128 * n : 128 * (n + 1)] = (first * jax.nn.sigmoid(first) * second * weight).astype(jnp.bfloat16)
        both = jnp.zeros((256, 128), jnp.float32)
        for r in range(8):
            both += lax.dot_general(
                rows[:, 256 * r : 256 * (r + 1)], wrecv[r, 0:128], NT, preferred_element_type=jnp.float32
            )
        second = pltpu.roll(both, 128 - PART, 1)
        value = both * jax.nn.sigmoid(both) * second * gate
        act[k, :, HID:] = jnp.where(lane < PART, value, 0.0).astype(jnp.bfloat16)

    hidden(xown, 0)
    for copy in arrive_d:
        copy.wait_recv()
    hidden(xpart, 1)

    def ahead(n, coord, stride, src, dst, send_sem, recv_sem, height):
        copies = []
        for d in (1, 3, 2):
            to, device = ring(coord, stride, d)
            k = 3 * n + d - 1
            copies.append(
                start(
                    src.at[n, pl.ds(pl.multiple_of(to * height, height), height)], dst.at[n, d - 1],
                    send_sem.at[k], recv_sem.at[k], device,
                )
            )
        return copies

    arrive_2, arrive_c2 = [], []

    def merge(n):
        arrive_2[n].wait_recv()
        total = acc[n] + drecv[n].astype(jnp.float32)
        acc[n] = total
        csend[n] = total.astype(jnp.bfloat16)
        arrive_c2.append(ahead(n, c, sc_, csend, crecv, c2s, c2r, 64))

    for n in range(CHUNKS):
        cols = slice(COLS * n, COLS * (n + 1))
        psend[n] = jnp.dot(act[1], wdx[:, cols], preferred_element_type=jnp.float32).astype(jnp.bfloat16)
        arrive_2.append(start(psend.at[n], drecv.at[n], d2s.at[n], d2r.at[n], partner))
        acc[n] = jnp.dot(act[0], wdx[:, cols], preferred_element_type=jnp.float32)
        if n >= 2:
            merge(n - 2)
    merge(CHUNKS - 2)
    merge(CHUNKS - 1)
    arrive_b2 = []
    for n in range(CHUNKS):
        for copy in arrive_c2[n]:
            copy.wait_recv()
        total = acc[n, pl.ds(pl.multiple_of(64 * c, 64), 64)]
        for d in range(3):
            total = total + crecv[n, d].astype(jnp.float32)
        bsum[n] = total
        bsend[n] = total.astype(jnp.bfloat16)
        arrive_b2.append(ahead(n, b, sb, bsend, brecv, b2s, b2r, 16))
    arrive_a2 = []
    for n in range(CHUNKS):
        for copy in arrive_b2[n]:
            copy.wait_recv()
        total = bsum[n, rows16(b)]
        for d in range(3):
            total = total + brecv[n, d].astype(jnp.float32)
        fa[n] = total
        for j in range(4):
            piece = fa[n, 4 * j : 4 * j + 4]
            aown[n, j] = piece
            asend[n, j] = piece.astype(jnp.bfloat16)
        copies = []
        for d in (1, 3, 2):
            to, device = ring(a, sa, d)
            k = 3 * n + d - 1
            copies.append(start(asend.at[n, to], arecv.at[n, d - 1], a2s.at[k], a2r.at[k], device))
        arrive_a2.append(copies)
    for n in range(CHUNKS):
        cols = slice(COLS * n, COLS * (n + 1))
        for copy in arrive_a2[n]:
            copy.wait_recv()
        total = hid_ref[:, cols] + aown[n, a]
        for d in range(3):
            total = total + arecv[n, d].astype(jnp.float32)
        out_ref[:, cols] = total.astype(jnp.bfloat16)
    for copy in sends:
        copy.wait_send()


def hand_over(out_in, newk_in, newv_in, out_ref, newk_ref, newv_ref, sem):
    pairs = ((out_in, out_ref), (newk_in, newk_ref), (newv_in, newv_ref))
    copies = [pltpu.make_async_copy(src, dst, sem.at[k]) for k, (src, dst) in enumerate(pairs)]
    for copy in copies:
        copy.start()
    for copy in copies:
        copy.wait()


def per_device(
    tokens, lengths, cache_keys, cache_values, query_w, key_w, value_w, out_w, mix_lambda, head_gain,
    attn_gain, ffn_gain, routes, route_weights, exp_gate, exp_up, exp_down, dense_gate, dense_up,
    dense_down, branch_gate,
):
    bf, f32 = jnp.bfloat16, jnp.float32
    dma = pltpu.SemaphoreType.DMA
    vmem = pl.BlockSpec(memory_space=pltpu.VMEM)
    anywhere = pl.BlockSpec(memory_space=pl.ANY)
    kv = KV_HEADS * HEAD_DIM
    shapes = tuple(jax.ShapeDtypeStruct((SEQ_DEV, width), bf) for width in (D, kv, kv))
    made = pl.pallas_call(
        layer_kernel,
        out_shape=tuple(pltpu.VMEM(shape.shape, bf) for shape in shapes),
        in_specs=[anywhere] * 21,
        out_specs=(vmem, vmem, vmem),
        scratch_shapes=[
            pltpu.SMEM((SEQ_DEV,), jnp.int32),
            pltpu.SMEM((HEADS,), f32),
            pltpu.SMEM((2, SEQ_DEV), jnp.int32),
            pltpu.SMEM((2, SEQ_DEV), f32),
            pltpu.VMEM((SEQ_DEV, D), bf),
            pltpu.VMEM((1, D), f32),
            pltpu.VMEM((1, D), f32),
            pltpu.VMEM((1, HEAD_DIM), f32),
            pltpu.VMEM((16, 128), bf),
            pltpu.VMEM((SEQ_DEV, 2 * CACHE, HEAD_DIM), bf),
            pltpu.VMEM((SEQ_DEV, 2 * CACHE, HEAD_DIM), bf),
            pltpu.VMEM((D, HEADS * HEAD_DIM), bf),
            pltpu.VMEM((D, 2 * kv), bf),
            pltpu.VMEM((HEADS * HEAD_DIM, D), bf),
            pltpu.VMEM((352, 256), bf),
            pltpu.VMEM((352, 256), bf),
            pltpu.VMEM((352, 256), bf),
            pltpu.VMEM((SEQ_DEV, HEADS * HEAD_DIM + 2 * kv), f32),
            pltpu.VMEM((SEQ_DEV, HEADS, HEAD_DIM), f32),
            pltpu.VMEM((SEQ_DEV, 2 * HEADS, 2 * CACHE), f32),
            pltpu.VMEM((SEQ_DEV, HEADS * HEAD_DIM), f32),
            pltpu.VMEM((SEQ_DEV, D), f32),
            pltpu.VMEM((SEQ_DEV, WIDE), bf),
            pltpu.VMEM((3, D, 256), bf),
            pltpu.VMEM((512, D), bf),
            pltpu.VMEM((8, 3 * PART, 256), bf),
            pltpu.VMEM((8, 3 * PART, 256), bf),
            pltpu.VMEM((4, 4, WIDE), bf),
            pltpu.VMEM((16, WIDE), f32),
            pltpu.VMEM((256, WIDE), bf),
            pltpu.VMEM((256, WIDE), bf),
            pltpu.VMEM((2, 256, 512), bf),
            pltpu.VMEM((CHUNKS, 256, COLS), f32),
            pltpu.VMEM((CHUNKS, 256, COLS), bf),
            pltpu.VMEM((CHUNKS, 256, COLS), bf),
            pltpu.VMEM((CHUNKS, 256, COLS), bf),
            pltpu.VMEM((CHUNKS, 3, 64, COLS), bf),
            pltpu.VMEM((CHUNKS, 64, COLS), f32),
            pltpu.VMEM((CHUNKS, 64, COLS), bf),
            pltpu.VMEM((CHUNKS, 3, 16, COLS), bf),
            pltpu.VMEM((CHUNKS, 16, COLS), f32),
            pltpu.VMEM((CHUNKS, 4, 4, COLS), f32),
            pltpu.VMEM((CHUNKS, 4, 4, COLS), bf),
            pltpu.VMEM((CHUNKS, 3, 4, COLS), bf),
            dma((9,)), dma((3,)), dma((6,)), dma((4,)), dma((4,)), dma((4,)),
            dma((7,)), dma((7,)), dma((7,)), dma((3,)), dma((3,)), dma((3,)), dma((3,)),
            dma((12,)), dma((12,)), dma((16,)), dma((16,)),
            dma((CHUNKS,)), dma((CHUNKS,)),
            dma((3 * CHUNKS,)), dma((3 * CHUNKS,)), dma((3 * CHUNKS,)), dma((3 * CHUNKS,)),
            dma((3 * CHUNKS,)), dma((3 * CHUNKS,)),
        ],
        compiler_params=pltpu.CompilerParams(
            collective_id=0, has_side_effects=True, vmem_limit_bytes=VMEM_LIMIT
        ),
    )(
        lengths, mix_lambda, routes.T, route_weights.T, tokens, attn_gain.reshape(1, D), ffn_gain.reshape(1, D), head_gain.reshape(1, HEAD_DIM),
        branch_gate.reshape(16, 128),
        cache_keys.reshape(-1, HEAD_DIM), cache_values.reshape(-1, HEAD_DIM), query_w, key_w, value_w, out_w,
        exp_gate, exp_up, exp_down, dense_gate[0].T, dense_up[0].T, dense_down[0],
    )
    return pl.pallas_call(
        hand_over, out_shape=shapes, in_specs=[vmem] * 3, out_specs=(anywhere,) * 3, scratch_shapes=[dma((3,))]
    )(*[pltpu.with_memory_space_constraint(piece, pltpu.VMEM) for piece in made])


def solution(mesh):
    placed = (
        P("ep", None), P("ep"), P("ep", None, None, None), P("ep", None, None, None),
        P(), P(), P(), P(), P(), P(), P(), P(),
        P("ep", None), P("ep", None), P(None, "ep"), P(None, "ep"), P("ep", None),
        P("ep", None, None), P("ep", None, None), P("ep", None, None), P(),
    )
    return jax.shard_map(
        per_device,
        mesh=mesh,
        in_specs=placed,
        out_specs=(P("ep", None), P("ep", None), P("ep", None)),
        check_vma=False,
    )
```

```python
import jax
import jax.numpy as jnp
from jax import lax
from jax.experimental import pallas as pl
from jax.experimental.pallas import tpu as pltpu
from jax.sharding import PartitionSpec as P

HEADS = 8
KV_HEADS = 2
HEAD_DIM = 128
SEQ_DEV = 4
CACHE = 1024
SPLIT = 16
D = 2048
SIDE = 128
WIDE = D + SIDE
HID = 384
PART = 48
CHUNKS = 4
EDGE = 5 * 128
VMEM_LIMIT = 67043328 - 131072
COLS = D // CHUNKS
MESH = pl.DeviceIdType.MESH
NT = (((1,), (1,)), ((), ()))


def rms_norm(values, gain, epsilon):
    scale = lax.rsqrt(jnp.mean(values * values, axis=-1, keepdims=True) + epsilon)
    return values * scale * gain


def remote(src, dst, send, recv, device):
    return pltpu.make_async_remote_copy(
        src_ref=src, dst_ref=dst, send_sem=send, recv_sem=recv,
        device_id=(device,), device_id_type=MESH,
    )


def layer_kernel(
    len_hbm, lam_hbm, routes_hbm, rweights_hbm, tok_hbm, again_hbm, fgain_hbm, hgain_hbm, bgate_hbm,
    keys_hbm, values_hbm, qw_hbm, kw_hbm, vw_hbm, ow_hbm,
    wg_hbm, wu_hbm, wd_hbm, dg_hbm, du_hbm, dd_hbm,
    out_ref, newk_ref, newv_ref,
    len_ref, lam_ref, routes_ref, rweights_ref, tok_ref, again_ref, fgain_ref, hgain_ref, bgate_ref,
    keys, values, qw, kvw, ow, tiles, qf, qs, sc, hf, hid_ref, x_ref,
    wgu, wdx, wsend, wrecv, land0, land1, pack, xown, xpart, act, acc, psend, drecv, csend, crecv,
    bsum, aown, asend, arecv,
    isem, dsem, qsem, ksem, vsem, osem,
    wsem, rs_w, rr_w, as_s, as_r, cs_s, cs_r, ds_s, ds_r, d2s, d2r, c2s, c2r, a2s, a2r,
):
    me = lax.axis_index("ep")
    core = lax.rem(me, 2)
    x = lax.rem(lax.div(me, 2), 4)
    y = lax.rem(lax.div(me, 8), 4)
    z = lax.div(me, 32)
    other = 1 - core
    a, sa = x * other + y * core, 2 * other + 8 * core
    p, sp = y * other + x * core, 8 * other + 2 * core
    colours = ((p, sp, z, 32), (z, 32, p, sp))
    row_block = lax.div(me, SPLIT)
    partner = me + other - core

    def ring(coord, stride, d):
        new = lax.rem(coord + d, 4)
        return new, me + (new - coord) * stride

    def plane(coord, stride, db, da):
        new_b, new_a = lax.rem(coord + db, 4), lax.rem(a + da, 4)
        return new_b, new_a, me + (new_b - coord) * stride + (new_a - a) * sa

    def group(d):
        new = lax.rem(row_block + d, 8)
        return new, me + (new - row_block) * SPLIT

    bf, f32 = jnp.bfloat16, jnp.float32

    def fetch(src, dst, sem):
        copy = pltpu.make_async_copy(src, dst, sem)
        copy.start()
        return copy

    for k, tile in enumerate((dg_hbm, du_hbm, dd_hbm)):
        fetch(tile, tiles.at[k], dsem)
    small = (
        (tok_hbm, tok_ref), (again_hbm, again_ref), (len_hbm, len_ref), (lam_hbm, lam_ref),
        (routes_hbm, routes_ref), (rweights_hbm, rweights_ref), (fgain_hbm, fgain_ref),
        (hgain_hbm, hgain_ref), (bgate_hbm, bgate_ref),
    )
    small_in = [fetch(src, dst, isem.at[k]) for k, (src, dst) in enumerate(small)]
    quarter = [pl.ds(256 * n, 256) for n in range(4)]
    proj_in = [fetch(qw_hbm.at[:, part], qw.at[:, part], qsem.at[k]) for k, part in enumerate(quarter[:2])]
    barrier = pltpu.get_barrier_semaphore()
    for coord, stride, _, _ in colours:
        for k in range(1, 16):
            device = plane(coord, stride, k // 4, k % 4)[2]
            pl.semaphore_signal(barrier, inc=1, device_id=(device,), device_id_type=MESH)
    for d in range(1, 8):
        pl.semaphore_signal(barrier, inc=1, device_id=(group(d)[1],), device_id_type=MESH)
    pl.semaphore_signal(barrier, inc=1, device_id=(partner,), device_id_type=MESH)

    def start(*args):
        remote(*args).start()

    for copy in small_in:
        copy.wait()
    proj_in += [fetch(qw_hbm.at[:, part], qw.at[:, part], qsem.at[2 + k]) for k, part in enumerate(quarter[2:])]
    fetch(kw_hbm, kvw.at[:, pl.ds(0, 256)], qsem.at[4])
    fetch(vw_hbm, kvw.at[:, pl.ds(256, 256)], qsem.at[4])
    landed(tiles, dsem)
    for k in range(3):
        for r in range(7):
            wsend[r, PART * k : PART * (k + 1)] = tiles[k, PART * r : PART * (r + 1)]
        wsend[7, PART * k : PART * k + 16] = tiles[k, 336:352]
        wsend[7, PART * k + 16 : PART * (k + 1)] = jnp.zeros((32, 256), bf)
    pl.semaphore_wait(barrier, 38)
    for d in range(1, 8):
        to, device = group(d)
        start(wsend.at[to], wrecv.at[row_block], rs_w, rr_w, device)
    wrecv[row_block] = wsend[row_block]
    normed = rms_norm(tok_ref[...].astype(f32), again_ref[...], 1e-06).astype(bf)
    for n in range(4):
        proj_in[n].wait()
        cols = slice(256 * n, 256 * (n + 1))
        if n == 0:
            fetch(keys_hbm, keys, ksem)
        if n == 2:
            fetch(values_hbm, values, vsem)
        qf[:, cols] = jnp.dot(normed, qw[:, cols], preferred_element_type=f32).astype(bf).astype(f32)
    landed(kvw, qsem.at[4])
    out_in = [
        fetch(ow_hbm.at[:, pl.ds(512 * n, 512)], ow.at[:, pl.ds(512 * n, 512)], osem.at[n]) for n in range(4)
    ]
    new = jnp.dot(normed, kvw[...], preferred_element_type=f32).astype(bf)
    newk_ref[...] = new[:, :256]
    newv_ref[...] = new[:, 256:]
    qf[:, HEADS * HEAD_DIM :] = new.astype(f32)
    for s in range(SEQ_DEV):
        for h in range(HEADS):
            qs[s, h : h + 1] = qf[s : s + 1, HEAD_DIM * h : HEAD_DIM * (h + 1)]

    head8 = lax.broadcasted_iota(jnp.int32, (HEADS, HEAD_DIM), 0)
    lane8 = lax.broadcasted_iota(jnp.int32, (HEADS, HEAD_DIM), 1)
    low_head, low_lane = head8 < HEADS // KV_HEADS, lane8 < HEAD_DIM // 2
    head1 = lax.broadcasted_iota(jnp.int32, (HEADS, 1), 0)
    lam = jnp.zeros((HEADS, 1), f32)
    for h in range(HEADS):
        lam = jnp.where(head1 == h, lam_ref[h], lam)
    slot = lax.broadcasted_iota(jnp.int32, (HEADS, 2 * CACHE), 1)
    kv_of = lax.broadcasted_iota(jnp.int32, (HEADS, 2 * CACHE), 0) // (HEADS // KV_HEADS)
    mine_kv = (slot & 1) == kv_of
    scale = (HEAD_DIM // 2) ** (-0.5)

    def probabilities(scores, own, valid):
        largest = jnp.maximum(jnp.max(jnp.where(valid, scores, -jnp.inf), axis=1, keepdims=True), own)
        raised = jnp.where(valid, jnp.exp(scores - largest), 0.0)
        own_raised = jnp.exp(own - largest)
        total = jnp.sum(raised, axis=1, keepdims=True) + own_raised
        return raised, own_raised, 1.0 / total

    base = HEADS * HEAD_DIM
    landed(keys, ksem)
    for s in range(SEQ_DEV):
        q = qs[s]
        both = jnp.concatenate([jnp.where(low_lane, q, 0.0), jnp.where(low_lane, 0.0, q)], axis=0).astype(bf)
        sc[s] = lax.dot_general(both, keys[s], NT, preferred_element_type=f32) * scale
    for n in range(3):
        cols = pl.ds(128 * n, 128)
        fetch(wg_hbm.at[:, cols], wgu.at[n, :, pl.ds(0, 128)], wsem.at[0])
        fetch(wu_hbm.at[:, cols], wgu.at[n, :, pl.ds(128, 128)], wsem.at[0])
    fetch(wd_hbm, wdx.at[pl.ds(0, HID)], wsem.at[1])
    landed(values, vsem)
    for s in range(SEQ_DEV):
        q = qs[s]
        rows = [qf[s : s + 1, base + 128 * k : base + 128 * (k + 1)] for k in range(4)]
        own_score = q * jnp.where(low_head, rows[0], rows[1])
        own_value = jnp.where(low_head, rows[2], rows[3])
        own_one = jnp.sum(jnp.where(low_lane, own_score, 0.0), axis=1, keepdims=True) * scale
        own_two = jnp.sum(jnp.where(low_lane, 0.0, own_score), axis=1, keepdims=True) * scale
        valid = mine_kv & (slot < 2 * len_ref[s])
        raised_one, own_one, inv_one = probabilities(sc[s, :HEADS], own_one, valid)
        raised_two, own_two, inv_two = probabilities(sc[s, HEADS:], own_two, valid)
        inv_two = inv_two * lam
        weights = (raised_one * inv_one - raised_two * inv_two).astype(bf)
        own_weight = (own_one * inv_one - own_two * inv_two).astype(bf).astype(f32)
        mixed = jnp.dot(weights, values[s], preferred_element_type=f32) + own_weight * own_value
        mixed = rms_norm(mixed, hgain_ref[...], 1e-05)
        for h in range(HEADS):
            hf[s : s + 1, HEAD_DIM * h : HEAD_DIM * (h + 1)] = mixed[h : h + 1]
    heads = hf[...].astype(bf)
    for n in range(4):
        out_in[n].wait()
        cols = slice(512 * n, 512 * (n + 1))
        hid_ref[:, cols] = tok_ref[:, cols].astype(f32) + jnp.dot(heads, ow[:, cols], preferred_element_type=f32)
    ffn_in = rms_norm(hid_ref[...], fgain_ref[...], 1e-06).astype(bf)
    gate_row = bgate_ref[...].astype(f32)
    terms = jnp.zeros((SEQ_DEV, 128), f32)
    for k in range(16):
        terms = terms + ffn_in[:, 128 * k : 128 * (k + 1)].astype(f32) * gate_row[k : k + 1]
    gate = jax.nn.sigmoid(jnp.sum(terms, axis=1, keepdims=True))
    place = lax.broadcasted_iota(jnp.int32, (SEQ_DEV, SIDE), 1)
    row = lax.broadcasted_iota(jnp.int32, (SEQ_DEV, SIDE), 0)
    full = jnp.where((place == 16) | (place == 17), gate, 0.0)
    for t in range(SEQ_DEV):
        for k in range(2):
            chosen = (row == t) & (place < 16) & ((place & 7) == routes_ref[k, t])
            full = full + jnp.where(chosen, rweights_ref[k, t], 0.0)
    high = full.astype(bf).astype(f32)
    side = jnp.where((place < 8) | (place == 16), high, full - high)
    x_ref[:, :D] = ffn_in
    x_ref[:, D:] = side.astype(bf)

    lanes = (slice(0, EDGE), slice(EDGE, WIDE))
    spans = (pl.ds(0, EDGE), pl.ds(EDGE, WIDE - EDGE))
    lands = (land0, land1)
    for k in (1, 2, 3, 4, 5, 6, 7, 12, 13, 14, 15, 8, 9, 10, 11):
        for s, (coord, stride, _, _) in enumerate(colours):
            device = plane(coord, stride, k // 4, k % 4)[2]
            start(x_ref.at[:, spans[s]], lands[s].at[4 * coord + a], as_s.at[s], as_r.at[s, k // 4], device)
    for s, (coord, _, _, _) in enumerate(colours):
        lands[s][4 * coord + a] = x_ref[:, lanes[s]]

    def place_of(s, along_c, along_b):
        return (along_c, along_b) if s == 0 else (along_b, along_c)

    def across(s, place):
        at = (*place, slice(None), spans[s])
        start(xown.at[at], xpart.at[at], ds_s, ds_r, partner)

    order = (0, 1, 3, 2)
    for db in order:
        for s, (b, _, c, sc_) in enumerate(colours):
            landed(lands[s].at[pl.ds(0, 4 if db else 3)], as_r.at[s, db])
            row = lax.rem(b + 4 - db, 4)
            for j in range(4):
                pack[4 * j : 4 * j + 4, lanes[s]] = lands[s][4 * row + j].astype(f32)
            place = place_of(s, c, row)
            xown[(*place, slice(None), lanes[s])] = pack[:, lanes[s]].astype(bf)
            at = (*place, slice(None), spans[s])
            for dc in (1, 3, 2):
                start(xown.at[at], xown.at[at], cs_s.at[s], cs_r.at[s, db], ring(c, sc_, dc)[1])
            across(s, place)
    for db in order:
        for s, (b, _, c, _) in enumerate(colours):
            landed(xown.at[0, pl.ds(0, 3), :, spans[s]], cs_r.at[s, db])
            for dc in (1, 3, 2):
                across(s, place_of(s, lax.rem(c + 4 - dc, 4), lax.rem(b + 4 - db, 4)))

    landed(wgu, wsem.at[0])
    landed(wdx.at[pl.ds(0, HID)], wsem.at[1])
    landed(wrecv.at[pl.ds(0, 7)], rr_w)
    wdx[HID + PART :] = jnp.zeros((128 - PART, D), jnp.bfloat16)
    for r in range(8):
        wdx[HID : HID + PART, 256 * r : 256 * (r + 1)] = wrecv[r, 2 * PART :]

    lane = lax.broadcasted_iota(jnp.int32, (256, SIDE), 1)

    def hidden(rows, k):
        side = rows[:, D:].astype(jnp.float32)
        expert = lax.div(me, SPLIT)
        weight = jnp.sum(jnp.where((lane == expert) | (lane == expert + 8), side, 0.0), axis=1, keepdims=True)
        gate = jnp.sum(jnp.where((lane == 16) | (lane == 17), side, 0.0), axis=1, keepdims=True)
        for n in range(3):
            both = jnp.dot(rows[:, :D], wgu[n], preferred_element_type=jnp.float32)
            first, second = both[:, :128], both[:, 128:]
            act[k, :, 128 * n : 128 * (n + 1)] = (first * jax.nn.sigmoid(first) * second * weight).astype(jnp.bfloat16)
        both = jnp.zeros((256, 128), jnp.float32)
        for r in range(8):
            both += lax.dot_general(
                rows[:, 256 * r : 256 * (r + 1)], wrecv[r, 0:128], NT, preferred_element_type=jnp.float32
            )
        second = pltpu.roll(both, 128 - PART, 1)
        value = both * jax.nn.sigmoid(both) * second * gate
        act[k, :, HID:] = jnp.where(lane < PART, value, 0.0).astype(jnp.bfloat16)

    def merge(n):
        landed(drecv.at[n], d2r.at[n])
        total = acc[n] + drecv[n].astype(f32)
        acc[n] = total
        csend[n] = total.astype(bf)
        s = min(n, 1)
        c, sc_ = colours[s][2:]
        for d in (1, 3, 2):
            to, device = ring(c, sc_, d)
            start(csend.at[n, to] if s == 0 else csend.at[n, :, to], crecv.at[n, d - 1], c2s, c2r.at[n], device)

    hidden(xown[...].reshape(256, WIDE), 0)
    landed(xpart, ds_r)
    hidden(xpart[...].reshape(256, WIDE), 1)
    for n in range(CHUNKS):
        cols = slice(COLS * n, COLS * (n + 1))
        psend[n] = jnp.dot(act[1], wdx[:, cols], preferred_element_type=f32).astype(bf).reshape(4, 4, 16, COLS)
        start(psend.at[n], drecv.at[n], d2s, d2r.at[n], partner)
    for n in range(CHUNKS):
        cols = slice(COLS * n, COLS * (n + 1))
        acc[n] = jnp.dot(act[0], wdx[:, cols], preferred_element_type=f32).reshape(4, 4, 16, COLS)
        merge(n)
    for n in range(CHUNKS):
        s = min(n, 1)
        b, sb, c, _ = colours[s]
        landed(crecv.at[n], c2r.at[n])
        total = acc[n, c] if s == 0 else acc[n, :, c]
        for d in range(3):
            total = total + crecv[n, d].astype(f32)
        bsum[n] = total
        for k in range(4):
            for j in range(4):
                piece = bsum[n, k, 4 * j : 4 * j + 4]
                aown[n, k, j] = piece
                asend[n, k, j] = piece.astype(bf)
        for k in (1, 2, 3, 4, 5, 6, 7, 12, 13, 14, 15, 8, 9, 10, 11):
            to_b, to_a, device = plane(b, sb, k // 4, k % 4)
            start(asend.at[n, to_b, to_a], arecv.at[n, k - 1], a2s, a2r.at[n], device)
    for n in range(CHUNKS):
        cols = slice(COLS * n, COLS * (n + 1))
        total = hid_ref[:, cols] + aown[n, colours[min(n, 1)][0], a]
        landed(arecv.at[n], a2r.at[n])
        for k in range(15):
            total = total + arecv[n, k].astype(f32)
        out_ref[:, cols] = total.astype(bf)
    landed(wsend.at[pl.ds(0, 7)], rs_w)
    for s in range(2):
        landed(lands[s].at[pl.ds(0, 15)], as_s.at[s])
        landed(xown.at[pl.ds(0, 3), :, :, spans[s]], cs_s.at[s])
    landed(xown, ds_s)
    landed(psend, d2s)
    landed(crecv, c2s)
    landed(arecv, a2s)


def landed(ref, sem):
    pltpu.make_async_copy(ref, ref, sem).wait()


def hand_over(out_in, newk_in, newv_in, out_ref, newk_ref, newv_ref, sem):
    pairs = ((out_in, out_ref), (newk_in, newk_ref), (newv_in, newv_ref))
    copies = [pltpu.make_async_copy(src, dst, sem.at[k]) for k, (src, dst) in enumerate(pairs)]
    for copy in copies:
        copy.start()
    for copy in copies:
        copy.wait()


def per_device(
    tokens, lengths, cache_keys, cache_values, query_w, key_w, value_w, out_w, mix_lambda, head_gain,
    attn_gain, ffn_gain, routes, route_weights, exp_gate, exp_up, exp_down, dense_gate, dense_up,
    dense_down, branch_gate,
):
    bf, f32 = jnp.bfloat16, jnp.float32
    dma = pltpu.SemaphoreType.DMA
    vmem = pl.BlockSpec(memory_space=pltpu.VMEM)
    anywhere = pl.BlockSpec(memory_space=pl.ANY)
    kv = KV_HEADS * HEAD_DIM
    shapes = tuple(jax.ShapeDtypeStruct((SEQ_DEV, width), bf) for width in (D, kv, kv))
    made = pl.pallas_call(
        layer_kernel,
        out_shape=tuple(pltpu.VMEM(shape.shape, bf) for shape in shapes),
        in_specs=[anywhere] * 21,
        out_specs=(vmem, vmem, vmem),
        scratch_shapes=[
            pltpu.SMEM((SEQ_DEV,), jnp.int32),
            pltpu.SMEM((HEADS,), f32),
            pltpu.SMEM((2, SEQ_DEV), jnp.int32),
            pltpu.SMEM((2, SEQ_DEV), f32),
            pltpu.VMEM((SEQ_DEV, D), bf),
            pltpu.VMEM((1, D), f32),
            pltpu.VMEM((1, D), f32),
            pltpu.VMEM((1, HEAD_DIM), f32),
            pltpu.VMEM((16, 128), bf),
            pltpu.VMEM((SEQ_DEV, 2 * CACHE, HEAD_DIM), bf),
            pltpu.VMEM((SEQ_DEV, 2 * CACHE, HEAD_DIM), bf),
            pltpu.VMEM((D, HEADS * HEAD_DIM), bf),
            pltpu.VMEM((D, 2 * kv), bf),
            pltpu.VMEM((HEADS * HEAD_DIM, D), bf),
            pltpu.VMEM((3, 352, 256), bf),
            pltpu.VMEM((SEQ_DEV, HEADS * HEAD_DIM + 2 * kv), f32),
            pltpu.VMEM((SEQ_DEV, HEADS, HEAD_DIM), f32),
            pltpu.VMEM((SEQ_DEV, 2 * HEADS, 2 * CACHE), f32),
            pltpu.VMEM((SEQ_DEV, HEADS * HEAD_DIM), f32),
            pltpu.VMEM((SEQ_DEV, D), f32),
            pltpu.VMEM((SEQ_DEV, WIDE), bf),
            pltpu.VMEM((3, D, 256), bf),
            pltpu.VMEM((512, D), bf),
            pltpu.VMEM((8, 3 * PART, 256), bf),
            pltpu.VMEM((8, 3 * PART, 256), bf),
            pltpu.VMEM((16, SEQ_DEV, EDGE), bf),
            pltpu.VMEM((16, SEQ_DEV, WIDE - EDGE), bf),
            pltpu.VMEM((16, WIDE), f32),
            pltpu.VMEM((4, 4, 16, WIDE), bf),
            pltpu.VMEM((4, 4, 16, WIDE), bf),
            pltpu.VMEM((2, 256, 512), bf),
            pltpu.VMEM((CHUNKS, 4, 4, 16, COLS), f32),
            pltpu.VMEM((CHUNKS, 4, 4, 16, COLS), bf),
            pltpu.VMEM((CHUNKS, 4, 4, 16, COLS), bf),
            pltpu.VMEM((CHUNKS, 4, 4, 16, COLS), bf),
            pltpu.VMEM((CHUNKS, 3, 4, 16, COLS), bf),
            pltpu.VMEM((CHUNKS, 4, 16, COLS), f32),
            pltpu.VMEM((CHUNKS, 4, 4, SEQ_DEV, COLS), f32),
            pltpu.VMEM((CHUNKS, 4, 4, SEQ_DEV, COLS), bf),
            pltpu.VMEM((CHUNKS, 15, SEQ_DEV, COLS), bf),
            dma((9,)), dma, dma((5,)), dma, dma, dma((4,)),
            dma((2,)), dma, dma, dma((2,)), dma((2, 4)), dma((2,)), dma((2, 4)), dma, dma,
            dma, dma((CHUNKS,)), dma, dma((CHUNKS,)), dma, dma((CHUNKS,)),
        ],
        compiler_params=pltpu.CompilerParams(
            collective_id=0, has_side_effects=True, vmem_limit_bytes=VMEM_LIMIT
        ),
    )(
        lengths, mix_lambda, routes.T, route_weights.T, tokens, attn_gain.reshape(1, D), ffn_gain.reshape(1, D), head_gain.reshape(1, HEAD_DIM),
        branch_gate.reshape(16, 128),
        cache_keys.reshape(SEQ_DEV, -1, HEAD_DIM), cache_values.reshape(SEQ_DEV, -1, HEAD_DIM), query_w, key_w, value_w, out_w,
        exp_gate, exp_up, exp_down, dense_gate[0].T, dense_up[0].T, dense_down[0],
    )
    return pl.pallas_call(
        hand_over, out_shape=shapes, in_specs=[vmem] * 3, out_specs=(anywhere,) * 3, scratch_shapes=[dma((3,))]
    )(*[pltpu.with_memory_space_constraint(piece, pltpu.VMEM) for piece in made])


def solution(mesh):
    placed = (
        P("ep", None), P("ep"), P("ep", None, None, None), P("ep", None, None, None),
        P(), P(), P(), P(), P(), P(), P(), P(),
        P("ep", None), P("ep", None), P(None, "ep"), P(None, "ep"), P("ep", None),
        P("ep", None, None), P("ep", None, None), P("ep", None, None), P(),
    )
    return jax.shard_map(
        per_device,
        mesh=mesh,
        in_specs=placed,
        out_specs=(P("ep", None), P("ep", None), P("ep", None)),
        check_vma=False,
    )
```

```python
import jax
import jax.numpy as jnp
from jax import lax
from jax.experimental import pallas as pl
from jax.experimental.pallas import tpu as pltpu
from jax.sharding import PartitionSpec as P

HEADS = 8
KV_HEADS = 2
HEAD_DIM = 128
SEQ_DEV = 4
CACHE = 1024
SPLIT = 16
D = 2048
SIDE = 128
WIDE = D + SIDE
HID = 384
PART = 48
CHUNKS = ((0, 512, 1), (512, 512, 1), (1024, 640, 0), (1664, 384, 1))
HALVES = ((0, 1024, (0, 1)), (1024, 1024, (2, 3)))
EDGE = 6 * 128
VMEM_LIMIT = 67043328 - 131072
MESH = pl.DeviceIdType.MESH
FAR_FIRST = (10, 6, 14, 9, 11, 2, 8, 5, 7, 13, 15, 1, 3, 4, 12)
NEAR_FIRST = (1, 2, 3, 4, 5, 6, 7, 12, 13, 14, 15, 8, 9, 10, 11)
NT = (((1,), (1,)), ((), ()))


def rms_norm(values, gain, epsilon):
    scale = lax.rsqrt(jnp.mean(values * values, axis=-1, keepdims=True) + epsilon)
    return values * scale * gain


def remote(src, dst, send, recv, device):
    return pltpu.make_async_remote_copy(
        src_ref=src, dst_ref=dst, send_sem=send, recv_sem=recv,
        device_id=(device,), device_id_type=MESH,
    )


def layer_kernel(
    len_hbm, lam_hbm, routes_hbm, rweights_hbm, tok_hbm, again_hbm, fgain_hbm, hgain_hbm, bgate_hbm,
    keys_hbm, values_hbm, qw_hbm, kw_hbm, vw_hbm, ow_hbm,
    wg_hbm, wu_hbm, wd_hbm, dg_hbm, du_hbm, dd_hbm,
    out_ref, newk_ref, newv_ref,
    len_ref, lam_ref, routes_ref, rweights_ref, tok_ref, again_ref, fgain_ref, hgain_ref, bgate_ref,
    keys, values, qw, kvw, ow, tiles, qf, qs, sc, hf, hid_ref, x_ref,
    wgu, wdx, wsend, wrecv, land0, land1, pack, xown, xpart, act, acc, psend, drecv, csend, crecv,
    bsum, aown, asend, arecv,
    isem, dsem, qsem, ksem, vsem, osem,
    wsem, rs_w, rr_w, as_s, as_r, cs_s, cs_r, ds_s, ds_r, d2s, d2r, c2s, c2r, a2s, a2r,
):
    me = lax.axis_index("ep")
    core = lax.rem(me, 2)
    x = lax.rem(lax.div(me, 2), 4)
    y = lax.rem(lax.div(me, 8), 4)
    z = lax.div(me, 32)
    other = 1 - core
    a, sa = x * other + y * core, 2 * other + 8 * core
    p, sp = y * other + x * core, 8 * other + 2 * core
    colours = ((p, sp, z, 32), (z, 32, p, sp))
    row_block = lax.div(me, SPLIT)
    partner = me + other - core

    def ring(coord, stride, d):
        new = lax.rem(coord + d, 4)
        return new, me + (new - coord) * stride

    def plane(coord, stride, db, da):
        new_b, new_a = lax.rem(coord + db, 4), lax.rem(a + da, 4)
        return new_b, new_a, me + (new_b - coord) * stride + (new_a - a) * sa

    def group(d):
        new = lax.rem(row_block + d, 8)
        return new, me + (new - row_block) * SPLIT

    bf, f32 = jnp.bfloat16, jnp.float32

    def fetch(src, dst, sem, priority=0):
        copy = pltpu.make_async_copy(src, dst, sem)
        copy.start(priority=priority)
        return copy

    for k, tile in enumerate((dg_hbm, du_hbm, dd_hbm)):
        fetch(tile, tiles.at[k], dsem)
    small = (
        (tok_hbm, tok_ref), (again_hbm, again_ref), (len_hbm, len_ref), (lam_hbm, lam_ref),
        (routes_hbm, routes_ref), (rweights_hbm, rweights_ref), (fgain_hbm, fgain_ref),
        (hgain_hbm, hgain_ref), (bgate_hbm, bgate_ref),
    )
    small_in = [fetch(src, dst, isem.at[k]) for k, (src, dst) in enumerate(small)]
    quarter = [pl.ds(256 * n, 256) for n in range(4)]
    proj_in = [fetch(qw_hbm.at[:, part], qw.at[:, part], qsem.at[k], 1) for k, part in enumerate(quarter)]
    fetch(kw_hbm, kvw.at[:, pl.ds(0, 256)], qsem.at[4], 1)
    fetch(vw_hbm, kvw.at[:, pl.ds(256, 256)], qsem.at[4], 1)
    barrier = pltpu.get_barrier_semaphore()
    for coord, stride, _, _ in colours:
        for k in range(1, 16):
            device = plane(coord, stride, k // 4, k % 4)[2]
            pl.semaphore_signal(barrier, inc=1, device_id=(device,), device_id_type=MESH)
    for d in range(1, 8):
        pl.semaphore_signal(barrier, inc=1, device_id=(group(d)[1],), device_id_type=MESH)
    pl.semaphore_signal(barrier, inc=1, device_id=(partner,), device_id_type=MESH)

    def start(*args):
        remote(*args).start()

    for copy in small_in:
        copy.wait()
    landed(tiles, dsem)
    for k in range(3):
        for r in range(7):
            wsend[r, PART * k : PART * (k + 1)] = tiles[k, PART * r : PART * (r + 1)]
        wsend[7, PART * k : PART * k + 16] = tiles[k, 336:352]
        wsend[7, PART * k + 16 : PART * (k + 1)] = jnp.zeros((32, 256), bf)
    pl.semaphore_wait(barrier, 38)
    for d in range(1, 8):
        to, device = group(d)
        start(wsend.at[to], wrecv.at[row_block], rs_w, rr_w, device)
    wrecv[row_block] = wsend[row_block]
    normed = rms_norm(tok_ref[...].astype(f32), again_ref[...], 1e-06).astype(bf)
    for n in range(4):
        proj_in[n].wait()
        cols = slice(256 * n, 256 * (n + 1))
        if n == 0:
            fetch(keys_hbm, keys, ksem, 1)
        if n == 2:
            fetch(values_hbm, values, vsem, 1)
        qf[:, cols] = jnp.dot(normed, qw[:, cols], preferred_element_type=f32).astype(bf).astype(f32)
    landed(kvw, qsem.at[4])
    out_in = [
        fetch(ow_hbm.at[:, pl.ds(512 * n, 512)], ow.at[:, pl.ds(512 * n, 512)], osem.at[n]) for n in range(4)
    ]
    new = jnp.dot(normed, kvw[...], preferred_element_type=f32).astype(bf)
    newk_ref[...] = new[:, :256]
    newv_ref[...] = new[:, 256:]
    qf[:, HEADS * HEAD_DIM :] = new.astype(f32)
    for s in range(SEQ_DEV):
        for h in range(HEADS):
            qs[s, h : h + 1] = qf[s : s + 1, HEAD_DIM * h : HEAD_DIM * (h + 1)]

    head8 = lax.broadcasted_iota(jnp.int32, (HEADS, HEAD_DIM), 0)
    lane8 = lax.broadcasted_iota(jnp.int32, (HEADS, HEAD_DIM), 1)
    low_head, low_lane = head8 < HEADS // KV_HEADS, lane8 < HEAD_DIM // 2
    head1 = lax.broadcasted_iota(jnp.int32, (HEADS, 1), 0)
    lam = jnp.zeros((HEADS, 1), f32)
    for h in range(HEADS):
        lam = jnp.where(head1 == h, lam_ref[h], lam)
    slot = lax.broadcasted_iota(jnp.int32, (HEADS, 2 * CACHE), 1)
    kv_of = lax.broadcasted_iota(jnp.int32, (HEADS, 2 * CACHE), 0) // (HEADS // KV_HEADS)
    mine_kv = (slot & 1) == kv_of
    scale = (HEAD_DIM // 2) ** (-0.5)

    def probabilities(scores, own, valid):
        largest = jnp.maximum(jnp.max(jnp.where(valid, scores, -jnp.inf), axis=1, keepdims=True), own)
        raised = jnp.where(valid, jnp.exp(scores - largest), 0.0)
        own_raised = jnp.exp(own - largest)
        total = jnp.sum(raised, axis=1, keepdims=True) + own_raised
        return raised, own_raised, 1.0 / total

    base = HEADS * HEAD_DIM
    landed(keys, ksem)
    for s in range(SEQ_DEV):
        q = qs[s]
        both = jnp.concatenate([jnp.where(low_lane, q, 0.0), jnp.where(low_lane, 0.0, q)], axis=0).astype(bf)
        sc[s] = lax.dot_general(both, keys[s], NT, preferred_element_type=f32) * scale
    for n in range(3):
        cols = pl.ds(128 * n, 128)
        fetch(wg_hbm.at[:, cols], wgu.at[n, :, pl.ds(0, 128)], wsem.at[0])
        fetch(wu_hbm.at[:, cols], wgu.at[n, :, pl.ds(128, 128)], wsem.at[0])
    fetch(wd_hbm, wdx.at[pl.ds(0, HID)], wsem.at[1])
    landed(values, vsem)
    for s in range(SEQ_DEV):
        q = qs[s]
        rows = [qf[s : s + 1, base + 128 * k : base + 128 * (k + 1)] for k in range(4)]
        own_score = q * jnp.where(low_head, rows[0], rows[1])
        own_value = jnp.where(low_head, rows[2], rows[3])
        own_one = jnp.sum(jnp.where(low_lane, own_score, 0.0), axis=1, keepdims=True) * scale
        own_two = jnp.sum(jnp.where(low_lane, 0.0, own_score), axis=1, keepdims=True) * scale
        valid = mine_kv & (slot < 2 * len_ref[s])
        raised_one, own_one, inv_one = probabilities(sc[s, :HEADS], own_one, valid)
        raised_two, own_two, inv_two = probabilities(sc[s, HEADS:], own_two, valid)
        inv_two = inv_two * lam
        weights = (raised_one * inv_one - raised_two * inv_two).astype(bf)
        own_weight = (own_one * inv_one - own_two * inv_two).astype(bf).astype(f32)
        mixed = jnp.dot(weights, values[s], preferred_element_type=f32) + own_weight * own_value
        mixed = rms_norm(mixed, hgain_ref[...], 1e-05)
        for h in range(HEADS):
            hf[s : s + 1, HEAD_DIM * h : HEAD_DIM * (h + 1)] = mixed[h : h + 1]
    heads = hf[...].astype(bf)
    for n in range(4):
        out_in[n].wait()
        cols = slice(512 * n, 512 * (n + 1))
        hid_ref[:, cols] = tok_ref[:, cols].astype(f32) + jnp.dot(heads, ow[:, cols], preferred_element_type=f32)
    ffn_in = rms_norm(hid_ref[...], fgain_ref[...], 1e-06).astype(bf)
    gate_row = bgate_ref[...].astype(f32)
    terms = jnp.zeros((SEQ_DEV, 128), f32)
    for k in range(16):
        terms = terms + ffn_in[:, 128 * k : 128 * (k + 1)].astype(f32) * gate_row[k : k + 1]
    gate = jax.nn.sigmoid(jnp.sum(terms, axis=1, keepdims=True))
    place = lax.broadcasted_iota(jnp.int32, (SEQ_DEV, SIDE), 1)
    row = lax.broadcasted_iota(jnp.int32, (SEQ_DEV, SIDE), 0)
    full = jnp.where((place == 16) | (place == 17), gate, 0.0)
    for t in range(SEQ_DEV):
        for k in range(2):
            chosen = (row == t) & (place < 16) & ((place & 7) == routes_ref[k, t])
            full = full + jnp.where(chosen, rweights_ref[k, t], 0.0)
    high = full.astype(bf).astype(f32)
    side = jnp.where((place < 8) | (place == 16), high, full - high)
    x_ref[:, :D] = ffn_in
    x_ref[:, D:] = side.astype(bf)

    lanes = (slice(0, EDGE), slice(EDGE, WIDE))
    spans = (pl.ds(0, EDGE), pl.ds(EDGE, WIDE - EDGE))
    lands = (land0, land1)
    for k in NEAR_FIRST:
        for s, (coord, stride, _, _) in enumerate(colours):
            device = plane(coord, stride, k // 4, k % 4)[2]
            start(x_ref.at[:, spans[s]], lands[s].at[4 * coord + a], as_s.at[s], as_r.at[s, k // 4], device)
    for s, (coord, _, _, _) in enumerate(colours):
        lands[s][4 * coord + a] = x_ref[:, lanes[s]]

    def place_of(s, along_c, along_b):
        return (along_c, along_b) if s == 0 else (along_b, along_c)

    def across(s, place):
        at = (*place, slice(None), spans[s])
        start(xown.at[at], xpart.at[at], ds_s, ds_r, partner)

    order = (0, 1, 3, 2)
    for db in order:
        for s, (b, _, c, sc_) in enumerate(colours):
            landed(lands[s].at[pl.ds(0, 4 if db else 3)], as_r.at[s, db])
            row = lax.rem(b + 4 - db, 4)
            for j in range(4):
                pack[4 * j : 4 * j + 4, lanes[s]] = lands[s][4 * row + j].astype(f32)
            place = place_of(s, c, row)
            xown[(*place, slice(None), lanes[s])] = pack[:, lanes[s]].astype(bf)
            at = (*place, slice(None), spans[s])
            for dc in (1, 3, 2):
                start(xown.at[at], xown.at[at], cs_s.at[s], cs_r.at[s, db], ring(c, sc_, dc)[1])
            across(s, place)
    for db in order:
        for s, (b, _, c, _) in enumerate(colours):
            landed(xown.at[0, pl.ds(0, 3), :, spans[s]], cs_r.at[s, db])
            for dc in (1, 3, 2):
                across(s, place_of(s, lax.rem(c + 4 - dc, 4), lax.rem(b + 4 - db, 4)))

    landed(wgu, wsem.at[0])
    landed(wdx.at[pl.ds(0, HID)], wsem.at[1])
    landed(wrecv.at[pl.ds(0, 7)], rr_w)
    wdx[HID + PART :] = jnp.zeros((128 - PART, D), jnp.bfloat16)
    for r in range(8):
        wdx[HID : HID + PART, 256 * r : 256 * (r + 1)] = wrecv[r, 2 * PART :]

    lane = lax.broadcasted_iota(jnp.int32, (256, SIDE), 1)

    def hidden(source, k, parts):
        rows = source[...].reshape(256, WIDE)
        side = rows[:, D:].astype(f32)
        for n in parts:
            if n < 3:
                expert = lax.div(me, SPLIT)
                weight = jnp.sum(jnp.where((lane == expert) | (lane == expert + 8), side, 0.0), axis=1, keepdims=True)
                both = jnp.dot(rows[:, :D], wgu[n], preferred_element_type=f32)
                first, second = both[:, :128], both[:, 128:]
                value = first * jax.nn.sigmoid(first) * second * weight
            else:
                gate = jnp.sum(jnp.where((lane == 16) | (lane == 17), side, 0.0), axis=1, keepdims=True)
                both = jnp.zeros((256, 128), f32)
                for r in range(8):
                    both += lax.dot_general(
                        rows[:, 256 * r : 256 * (r + 1)], wrecv[r, 0:128], NT, preferred_element_type=f32
                    )
                second = pltpu.roll(both, 128 - PART, 1)
                value = jnp.where(lane < PART, both * jax.nn.sigmoid(both) * second * gate, 0.0)
            act[k, :, 128 * n : 128 * (n + 1)] = value.astype(bf)

    def merge(n):
        low, width, s = CHUNKS[n]
        cols, span = slice(low, low + width), pl.ds(low, width)
        landed(drecv.at[:, :, :, span], d2r.at[n])
        total = acc[:, :, :, cols] + drecv[:, :, :, cols].astype(f32)
        acc[:, :, :, cols] = total
        csend[:, :, :, cols] = total.astype(bf)
        c, sc_ = colours[s][2:]
        for d in (2, 1, 3):
            to, device = ring(c, sc_, d)
            src = csend.at[to, :, :, span] if s == 0 else csend.at[:, to, :, span]
            start(src, crecv.at[d - 1, :, :, span], c2s, c2r.at[n], device)

    hidden(xown, 0, (0, 1))
    landed(xpart, ds_r)
    hidden(xpart, 1, (0, 1, 2, 3))
    for low, width, chunks in HALVES:
        cols = slice(low, low + width)
        part = jnp.dot(act[1], wdx[:, cols], preferred_element_type=f32).astype(bf)
        psend[:, :, :, cols] = part.reshape(4, 4, 16, width)
        for n in chunks:
            span = pl.ds(*CHUNKS[n][:2])
            start(psend.at[:, :, :, span], drecv.at[:, :, :, span], d2s, d2r.at[n], partner)
    hidden(xown, 0, (2, 3))
    for low, width, chunks in HALVES:
        cols = slice(low, low + width)
        part = jnp.dot(act[0], wdx[:, cols], preferred_element_type=f32)
        acc[:, :, :, cols] = part.reshape(4, 4, 16, width)
        for n in chunks:
            merge(n)
    for n, (low, width, s) in enumerate(CHUNKS):
        cols, span = slice(low, low + width), pl.ds(low, width)
        b, sb, c, _ = colours[s]
        landed(crecv.at[:, :, :, span], c2r.at[n])
        total = acc[c, :, :, cols] if s == 0 else acc[:, c, :, cols]
        for d in range(3):
            total = total + crecv[d, :, :, cols].astype(f32)
        bsum[:, :, cols] = total
        for k in range(4):
            for j in range(4):
                piece = bsum[k, 4 * j : 4 * j + 4, cols]
                aown[k, j, :, cols] = piece
                asend[k, j, :, cols] = piece.astype(bf)
        for k in FAR_FIRST:
            to_b, to_a, device = plane(b, sb, k // 4, k % 4)
            start(asend.at[to_b, to_a, :, span], arecv.at[k - 1, :, span], a2s, a2r.at[n], device)
    for n, (low, width, s) in enumerate(CHUNKS):
        cols, span = slice(low, low + width), pl.ds(low, width)
        total = hid_ref[:, cols] + aown[colours[s][0], a, :, cols]
        landed(arecv.at[:, :, span], a2r.at[n])
        for k in range(15):
            total = total + arecv[k, :, cols].astype(f32)
        out_ref[:, cols] = total.astype(bf)
    landed(wsend.at[pl.ds(0, 7)], rs_w)
    for s in range(2):
        landed(lands[s].at[pl.ds(0, 15)], as_s.at[s])
        landed(xown.at[pl.ds(0, 3), :, :, spans[s]], cs_s.at[s])
    landed(xown, ds_s)
    landed(psend, d2s)
    landed(crecv, c2s)
    landed(arecv, a2s)


def landed(ref, sem):
    pltpu.make_async_copy(ref, ref, sem).wait()


def hand_over(out_in, newk_in, newv_in, out_ref, newk_ref, newv_ref, sem):
    pairs = ((out_in, out_ref), (newk_in, newk_ref), (newv_in, newv_ref))
    copies = [pltpu.make_async_copy(src, dst, sem.at[k]) for k, (src, dst) in enumerate(pairs)]
    for copy in copies:
        copy.start()
    for copy in copies:
        copy.wait()


def per_device(
    tokens, lengths, cache_keys, cache_values, query_w, key_w, value_w, out_w, mix_lambda, head_gain,
    attn_gain, ffn_gain, routes, route_weights, exp_gate, exp_up, exp_down, dense_gate, dense_up,
    dense_down, branch_gate,
):
    bf, f32 = jnp.bfloat16, jnp.float32
    dma = pltpu.SemaphoreType.DMA
    vmem = pl.BlockSpec(memory_space=pltpu.VMEM)
    anywhere = pl.BlockSpec(memory_space=pl.ANY)
    kv = KV_HEADS * HEAD_DIM
    shapes = tuple(jax.ShapeDtypeStruct((SEQ_DEV, width), bf) for width in (D, kv, kv))
    made = pl.pallas_call(
        layer_kernel,
        out_shape=tuple(pltpu.VMEM(shape.shape, bf) for shape in shapes),
        in_specs=[anywhere] * 21,
        out_specs=(vmem, vmem, vmem),
        scratch_shapes=[
            pltpu.SMEM((SEQ_DEV,), jnp.int32),
            pltpu.SMEM((HEADS,), f32),
            pltpu.SMEM((2, SEQ_DEV), jnp.int32),
            pltpu.SMEM((2, SEQ_DEV), f32),
            pltpu.VMEM((SEQ_DEV, D), bf),
            pltpu.VMEM((1, D), f32),
            pltpu.VMEM((1, D), f32),
            pltpu.VMEM((1, HEAD_DIM), f32),
            pltpu.VMEM((16, 128), bf),
            pltpu.VMEM((SEQ_DEV, 2 * CACHE, HEAD_DIM), bf),
            pltpu.VMEM((SEQ_DEV, 2 * CACHE, HEAD_DIM), bf),
            pltpu.VMEM((D, HEADS * HEAD_DIM), bf),
            pltpu.VMEM((D, 2 * kv), bf),
            pltpu.VMEM((HEADS * HEAD_DIM, D), bf),
            pltpu.VMEM((3, 352, 256), bf),
            pltpu.VMEM((SEQ_DEV, HEADS * HEAD_DIM + 2 * kv), f32),
            pltpu.VMEM((SEQ_DEV, HEADS, HEAD_DIM), f32),
            pltpu.VMEM((SEQ_DEV, 2 * HEADS, 2 * CACHE), f32),
            pltpu.VMEM((SEQ_DEV, HEADS * HEAD_DIM), f32),
            pltpu.VMEM((SEQ_DEV, D), f32),
            pltpu.VMEM((SEQ_DEV, WIDE), bf),
            pltpu.VMEM((3, D, 256), bf),
            pltpu.VMEM((512, D), bf),
            pltpu.VMEM((8, 3 * PART, 256), bf),
            pltpu.VMEM((8, 3 * PART, 256), bf),
            pltpu.VMEM((16, SEQ_DEV, EDGE), bf),
            pltpu.VMEM((16, SEQ_DEV, WIDE - EDGE), bf),
            pltpu.VMEM((16, WIDE), f32),
            pltpu.VMEM((4, 4, 16, WIDE), bf),
            pltpu.VMEM((4, 4, 16, WIDE), bf),
            pltpu.VMEM((2, 256, 512), bf),
            pltpu.VMEM((4, 4, 16, D), f32),
            pltpu.VMEM((4, 4, 16, D), bf),
            pltpu.VMEM((4, 4, 16, D), bf),
            pltpu.VMEM((4, 4, 16, D), bf),
            pltpu.VMEM((3, 4, 16, D), bf),
            pltpu.VMEM((4, 16, D), f32),
            pltpu.VMEM((4, 4, SEQ_DEV, D), f32),
            pltpu.VMEM((4, 4, SEQ_DEV, D), bf),
            pltpu.VMEM((15, SEQ_DEV, D), bf),
            dma((9,)), dma, dma((5,)), dma, dma, dma((4,)),
            dma((2,)), dma, dma, dma((2,)), dma((2, 4)), dma((2,)), dma((2, 4)), dma, dma,
            dma, dma((4,)), dma, dma((4,)), dma, dma((4,)),
        ],
        compiler_params=pltpu.CompilerParams(
            collective_id=0, has_side_effects=True, vmem_limit_bytes=VMEM_LIMIT
        ),
    )(
        lengths, mix_lambda, routes.T, route_weights.T, tokens, attn_gain.reshape(1, D), ffn_gain.reshape(1, D), head_gain.reshape(1, HEAD_DIM),
        branch_gate.reshape(16, 128),
        cache_keys.reshape(SEQ_DEV, -1, HEAD_DIM), cache_values.reshape(SEQ_DEV, -1, HEAD_DIM), query_w, key_w, value_w, out_w,
        exp_gate, exp_up, exp_down, dense_gate[0].T, dense_up[0].T, dense_down[0],
    )
    return pl.pallas_call(
        hand_over, out_shape=shapes, in_specs=[vmem] * 3, out_specs=(anywhere,) * 3, scratch_shapes=[dma((3,))]
    )(*[pltpu.with_memory_space_constraint(piece, pltpu.VMEM) for piece in made])


def solution(mesh):
    placed = (
        P("ep", None), P("ep"), P("ep", None, None, None), P("ep", None, None, None),
        P(), P(), P(), P(), P(), P(), P(), P(),
        P("ep", None), P("ep", None), P(None, "ep"), P(None, "ep"), P("ep", None),
        P("ep", None, None), P("ep", None, None), P("ep", None, None), P(),
    )
    return jax.shard_map(
        per_device,
        mesh=mesh,
        in_specs=placed,
        out_specs=(P("ep", None), P("ep", None), P("ep", None)),
        check_vma=False,
    )
```

```python
import jax
import jax.numpy as jnp
from jax import lax
from jax.experimental import pallas as pl
from jax.experimental.pallas import tpu as pltpu
from jax.sharding import PartitionSpec as P

HEADS = 8
KV_HEADS = 2
HEAD_DIM = 128
SEQ_DEV = 4
CACHE = 1024
SPLIT = 16
D = 2048
SIDE = 128
WIDE = D + SIDE
HID = 384
PART = 48
CHUNKS = ((0, 512, 1), (512, 512, 1), (1024, 640, 0), (1664, 384, 1))
HALVES = ((0, 1024, (0, 1)), (1024, 1024, (2, 3)))
EDGE = 6 * 128
VMEM_LIMIT = 67043328 - 131072
MESH = pl.DeviceIdType.MESH
FAR_FIRST = (10, 6, 14, 9, 11, 2, 8, 5, 7, 13, 15, 1, 3, 4, 12)
NEAR_FIRST = (1, 2, 3, 4, 5, 6, 7, 12, 13, 14, 15, 8, 9, 10, 11)
NT = (((1,), (1,)), ((), ()))


def rms_norm(values, gain, epsilon):
    scale = lax.rsqrt(jnp.mean(values * values, axis=-1, keepdims=True) + epsilon)
    return values * scale * gain


def remote(src, dst, send, recv, device):
    return pltpu.make_async_remote_copy(
        src_ref=src, dst_ref=dst, send_sem=send, recv_sem=recv,
        device_id=(device,), device_id_type=MESH,
    )


def layer_kernel(
    len_hbm, lam_hbm, routes_hbm, rweights_hbm, tok_hbm, again_hbm, fgain_hbm, hgain_hbm, bgate_hbm,
    keys_hbm, values_hbm, qw_hbm, kw_hbm, vw_hbm, ow_hbm,
    wg_hbm, wu_hbm, wd_hbm, dg_hbm, du_hbm, dd_hbm,
    out_ref, newk_ref, newv_ref,
    len_ref, lam_ref, routes_ref, rweights_ref, tok_ref, again_ref, fgain_ref, hgain_ref, bgate_ref,
    keys, values, qw, kvw, ow, tiles, qf, qs, sc, hf, hid_ref, x_ref,
    wgu, wdx, wsend, wrecv, land0, land1, pack, xown, xpart, act, acc, psend, drecv, csend, crecv,
    bsum, aown, asend, arecv,
    isem, dsem, qsem, ksem, vsem, osem,
    wsem, rs_w, rr_w, as_s, as_r, cs_s, cs_r, ds_s, ds_r, d2s, d2r, c2s, c2r, a2s, a2r,
):
    me = lax.axis_index("ep")
    core = lax.rem(me, 2)
    x = lax.rem(lax.div(me, 2), 4)
    y = lax.rem(lax.div(me, 8), 4)
    z = lax.div(me, 32)
    other = 1 - core
    a, sa = x * other + y * core, 2 * other + 8 * core
    p, sp = y * other + x * core, 8 * other + 2 * core
    colours = ((p, sp, z, 32), (z, 32, p, sp))
    row_block = lax.div(me, SPLIT)
    partner = me + other - core

    def ring(coord, stride, d):
        new = lax.rem(coord + d, 4)
        return new, me + (new - coord) * stride

    def plane(coord, stride, db, da):
        new_b, new_a = lax.rem(coord + db, 4), lax.rem(a + da, 4)
        return new_b, new_a, me + (new_b - coord) * stride + (new_a - a) * sa

    def group(d):
        new = lax.rem(row_block + d, 8)
        return new, me + (new - row_block) * SPLIT

    bf, f32 = jnp.bfloat16, jnp.float32

    def fetch(src, dst, sem, priority=0):
        copy = pltpu.make_async_copy(src, dst, sem)
        copy.start(priority=priority)
        return copy

    for k, tile in enumerate((dg_hbm, du_hbm, dd_hbm)):
        fetch(tile, tiles.at[k], dsem)
    small = (
        (tok_hbm, tok_ref), (again_hbm, again_ref), (len_hbm, len_ref), (lam_hbm, lam_ref),
        (routes_hbm, routes_ref), (rweights_hbm, rweights_ref), (fgain_hbm, fgain_ref),
        (hgain_hbm, hgain_ref), (bgate_hbm, bgate_ref),
    )
    small_in = [fetch(src, dst, isem.at[k]) for k, (src, dst) in enumerate(small)]
    quarter = [pl.ds(512 * n, 512) for n in range(4)]
    proj_in = [fetch(qw_hbm.at[part], qw.at[part], qsem.at[k], 1) for k, part in enumerate(quarter)]
    fetch(kw_hbm, kvw.at[:, pl.ds(0, 256)], qsem.at[4], 1)
    fetch(vw_hbm, kvw.at[:, pl.ds(256, 256)], qsem.at[4], 1)
    barrier = pltpu.get_barrier_semaphore()
    for coord, stride, _, _ in colours:
        for k in range(1, 16):
            device = plane(coord, stride, k // 4, k % 4)[2]
            pl.semaphore_signal(barrier, inc=1, device_id=(device,), device_id_type=MESH)
    for d in range(1, 8):
        pl.semaphore_signal(barrier, inc=1, device_id=(group(d)[1],), device_id_type=MESH)
    pl.semaphore_signal(barrier, inc=1, device_id=(partner,), device_id_type=MESH)

    def start(*args):
        remote(*args).start()

    for copy in small_in:
        copy.wait()
    landed(tiles, dsem)
    for k in range(3):
        for r in range(7):
            wsend[r, PART * k : PART * (k + 1)] = tiles[k, PART * r : PART * (r + 1)]
        wsend[7, PART * k : PART * k + 16] = tiles[k, 336:352]
        wsend[7, PART * k + 16 : PART * (k + 1)] = jnp.zeros((32, 256), bf)
    pl.semaphore_wait(barrier, 38)
    for d in range(1, 8):
        to, device = group(d)
        start(wsend.at[to], wrecv.at[row_block], rs_w, rr_w, device)
    wrecv[row_block] = wsend[row_block]
    normed = rms_norm(tok_ref[...].astype(f32), again_ref[...], 1e-06).astype(bf)
    query = jnp.zeros((SEQ_DEV, HEADS * HEAD_DIM), f32)
    for n in range(4):
        proj_in[n].wait()
        if n == 0:
            fetch(keys_hbm, keys, ksem, 1)
        if n == 2:
            fetch(values_hbm, values, vsem, 1)
        part = slice(512 * n, 512 * (n + 1))
        query = query + jnp.dot(normed[:, part], qw[part], preferred_element_type=f32)
    qf[:, : HEADS * HEAD_DIM] = query.astype(bf).astype(f32)
    landed(kvw, qsem.at[4])
    rows256 = [pl.ds(256 * n, 256) for n in range(4)]
    out_in = [fetch(ow_hbm.at[part], ow.at[part], osem.at[n], 1) for n, part in enumerate(rows256)]
    new = jnp.dot(normed, kvw[...], preferred_element_type=f32).astype(bf)
    newk_ref[...] = new[:, :256]
    newv_ref[...] = new[:, 256:]
    qf[:, HEADS * HEAD_DIM :] = new.astype(f32)
    for s in range(SEQ_DEV):
        for h in range(HEADS):
            qs[s, h : h + 1] = qf[s : s + 1, HEAD_DIM * h : HEAD_DIM * (h + 1)]

    head8 = lax.broadcasted_iota(jnp.int32, (HEADS, HEAD_DIM), 0)
    lane8 = lax.broadcasted_iota(jnp.int32, (HEADS, HEAD_DIM), 1)
    low_head, low_lane = head8 < HEADS // KV_HEADS, lane8 < HEAD_DIM // 2
    head1 = lax.broadcasted_iota(jnp.int32, (HEADS, 1), 0)
    lam = jnp.zeros((HEADS, 1), f32)
    for h in range(HEADS):
        lam = jnp.where(head1 == h, lam_ref[h], lam)
    slot = lax.broadcasted_iota(jnp.int32, (HEADS, 2 * CACHE), 1)
    kv_of = lax.broadcasted_iota(jnp.int32, (HEADS, 2 * CACHE), 0) // (HEADS // KV_HEADS)
    mine_kv = (slot & 1) == kv_of
    scale = (HEAD_DIM // 2) ** (-0.5)

    def probabilities(scores, own, valid):
        largest = jnp.maximum(jnp.max(jnp.where(valid, scores, -jnp.inf), axis=1, keepdims=True), own)
        raised = jnp.where(valid, jnp.exp(scores - largest), 0.0)
        own_raised = jnp.exp(own - largest)
        total = jnp.sum(raised, axis=1, keepdims=True) + own_raised
        return raised, own_raised, 1.0 / total

    base = HEADS * HEAD_DIM
    landed(keys, ksem)
    for s in range(SEQ_DEV):
        q = qs[s]
        both = jnp.concatenate([jnp.where(low_lane, q, 0.0), jnp.where(low_lane, 0.0, q)], axis=0).astype(bf)
        sc[s] = lax.dot_general(both, keys[s], NT, preferred_element_type=f32) * scale
    for n in range(3):
        cols = pl.ds(128 * n, 128)
        fetch(wg_hbm.at[:, cols], wgu.at[n, :, pl.ds(0, 128)], wsem.at[0], 1)
        fetch(wu_hbm.at[:, cols], wgu.at[n, :, pl.ds(128, 128)], wsem.at[0], 1)
    fetch(wd_hbm, wdx.at[pl.ds(0, HID)], wsem.at[1], 1)
    landed(values, vsem)
    for s in range(SEQ_DEV):
        q = qs[s]
        rows = [qf[s : s + 1, base + 128 * k : base + 128 * (k + 1)] for k in range(4)]
        own_score = q * jnp.where(low_head, rows[0], rows[1])
        own_value = jnp.where(low_head, rows[2], rows[3])
        own_one = jnp.sum(jnp.where(low_lane, own_score, 0.0), axis=1, keepdims=True) * scale
        own_two = jnp.sum(jnp.where(low_lane, 0.0, own_score), axis=1, keepdims=True) * scale
        valid = mine_kv & (slot < 2 * len_ref[s])
        raised_one, own_one, inv_one = probabilities(sc[s, :HEADS], own_one, valid)
        raised_two, own_two, inv_two = probabilities(sc[s, HEADS:], own_two, valid)
        inv_two = inv_two * lam
        weights = (raised_one * inv_one - raised_two * inv_two).astype(bf)
        own_weight = (own_one * inv_one - own_two * inv_two).astype(bf).astype(f32)
        mixed = jnp.dot(weights, values[s], preferred_element_type=f32) + own_weight * own_value
        mixed = rms_norm(mixed, hgain_ref[...], 1e-05)
        for h in range(HEADS):
            hf[s : s + 1, HEAD_DIM * h : HEAD_DIM * (h + 1)] = mixed[h : h + 1]
    heads = hf[...].astype(bf)
    state = tok_ref[...].astype(f32)
    for n in range(4):
        out_in[n].wait()
        part = slice(256 * n, 256 * (n + 1))
        state = state + jnp.dot(heads[:, part], ow[part], preferred_element_type=f32)
    hid_ref[...] = state
    ffn_in = rms_norm(state, fgain_ref[...], 1e-06).astype(bf)
    gate_row = bgate_ref[...].astype(f32)
    terms = jnp.zeros((SEQ_DEV, 128), f32)
    for k in range(16):
        terms = terms + ffn_in[:, 128 * k : 128 * (k + 1)].astype(f32) * gate_row[k : k + 1]
    gate = jax.nn.sigmoid(jnp.sum(terms, axis=1, keepdims=True))
    place = lax.broadcasted_iota(jnp.int32, (SEQ_DEV, SIDE), 1)
    row = lax.broadcasted_iota(jnp.int32, (SEQ_DEV, SIDE), 0)
    full = jnp.where((place == 16) | (place == 17), gate, 0.0)
    for t in range(SEQ_DEV):
        for k in range(2):
            chosen = (row == t) & (place < 16) & ((place & 7) == routes_ref[k, t])
            full = full + jnp.where(chosen, rweights_ref[k, t], 0.0)
    high = full.astype(bf).astype(f32)
    side = jnp.where((place < 8) | (place == 16), high, full - high)
    x_ref[:, :D] = ffn_in
    x_ref[:, D:] = side.astype(bf)

    lanes = (slice(0, EDGE), slice(EDGE, WIDE))
    spans = (pl.ds(0, EDGE), pl.ds(EDGE, WIDE - EDGE))
    lands = (land0, land1)
    for k in NEAR_FIRST:
        for s, (coord, stride, _, _) in enumerate(colours):
            device = plane(coord, stride, k // 4, k % 4)[2]
            start(x_ref.at[:, spans[s]], lands[s].at[4 * coord + a], as_s.at[s], as_r.at[s, k // 4], device)
    for s, (coord, _, _, _) in enumerate(colours):
        lands[s][4 * coord + a] = x_ref[:, lanes[s]]

    def place_of(s, along_c, along_b):
        return (along_c, along_b) if s == 0 else (along_b, along_c)

    def across(s, place):
        at = (*place, slice(None), spans[s])
        start(xown.at[at], xpart.at[at], ds_s, ds_r, partner)

    order = (0, 1, 3, 2)
    for db in order:
        for s, (b, _, c, sc_) in enumerate(colours):
            landed(lands[s].at[pl.ds(0, 4 if db else 3)], as_r.at[s, db])
            row = lax.rem(b + 4 - db, 4)
            for j in range(4):
                pack[4 * j : 4 * j + 4, lanes[s]] = lands[s][4 * row + j].astype(f32)
            place = place_of(s, c, row)
            xown[(*place, slice(None), lanes[s])] = pack[:, lanes[s]].astype(bf)
            at = (*place, slice(None), spans[s])
            for dc in (1, 3, 2):
                start(xown.at[at], xown.at[at], cs_s.at[s], cs_r.at[s, db], ring(c, sc_, dc)[1])
            across(s, place)
    for db in order:
        for s, (b, _, c, _) in enumerate(colours):
            landed(xown.at[0, pl.ds(0, 3), :, spans[s]], cs_r.at[s, db])
            for dc in (1, 3, 2):
                across(s, place_of(s, lax.rem(c + 4 - dc, 4), lax.rem(b + 4 - db, 4)))

    landed(wgu, wsem.at[0])
    landed(wdx.at[pl.ds(0, HID)], wsem.at[1])
    landed(wrecv.at[pl.ds(0, 7)], rr_w)
    wdx[HID + PART :] = jnp.zeros((128 - PART, D), jnp.bfloat16)
    for r in range(8):
        wdx[HID : HID + PART, 256 * r : 256 * (r + 1)] = wrecv[r, 2 * PART :]

    lane = lax.broadcasted_iota(jnp.int32, (256, SIDE), 1)

    def hidden(source, k, parts):
        rows = source[...].reshape(256, WIDE)
        side = rows[:, D:].astype(f32)
        for n in parts:
            if n < 3:
                expert = lax.div(me, SPLIT)
                weight = jnp.sum(jnp.where((lane == expert) | (lane == expert + 8), side, 0.0), axis=1, keepdims=True)
                both = jnp.dot(rows[:, :D], wgu[n], preferred_element_type=f32)
                first, second = both[:, :128], both[:, 128:]
                value = first * jax.nn.sigmoid(first) * second * weight
            else:
                gate = jnp.sum(jnp.where((lane == 16) | (lane == 17), side, 0.0), axis=1, keepdims=True)
                both = jnp.zeros((256, 128), f32)
                for r in range(8):
                    both += lax.dot_general(
                        rows[:, 256 * r : 256 * (r + 1)], wrecv[r, 0:128], NT, preferred_element_type=f32
                    )
                second = pltpu.roll(both, 128 - PART, 1)
                value = jnp.where(lane < PART, both * jax.nn.sigmoid(both) * second * gate, 0.0)
            act[k, :, 128 * n : 128 * (n + 1)] = value.astype(bf)

    def merge(n):
        low, width, s = CHUNKS[n]
        cols, span = slice(low, low + width), pl.ds(low, width)
        landed(drecv.at[:, :, :, span], d2r.at[n])
        csend[:, :, :, cols] = (acc[:, :, :, cols] + drecv[:, :, :, cols].astype(f32)).astype(bf)
        c, sc_ = colours[s][2:]
        for d in (2, 1, 3):
            to, device = ring(c, sc_, d)
            src = csend.at[to, :, :, span] if s == 0 else csend.at[:, to, :, span]
            start(src, crecv.at[d - 1, :, :, span], c2s, c2r.at[n], device)

    hidden(xown, 0, (0, 1))
    landed(xpart, ds_r)
    hidden(xpart, 1, (0, 1, 2, 3))
    for low, width, chunks in HALVES:
        cols = slice(low, low + width)
        part = jnp.dot(act[1], wdx[:, cols], preferred_element_type=f32).astype(bf)
        psend[:, :, :, cols] = part.reshape(4, 4, 16, width)
        for n in chunks:
            span = pl.ds(*CHUNKS[n][:2])
            start(psend.at[:, :, :, span], drecv.at[:, :, :, span], d2s, d2r.at[n], partner)
    hidden(xown, 0, (2, 3))
    for low, width, chunks in HALVES:
        cols = slice(low, low + width)
        part = jnp.dot(act[0], wdx[:, cols], preferred_element_type=f32)
        acc[:, :, :, cols] = part.reshape(4, 4, 16, width)
        for n in chunks:
            merge(n)
    for n, (low, width, s) in enumerate(CHUNKS):
        cols, span = slice(low, low + width), pl.ds(low, width)
        b, sb, c, _ = colours[s]
        landed(crecv.at[:, :, :, span], c2r.at[n])
        if s == 0:
            total = acc[c, :, :, cols] + drecv[c, :, :, cols].astype(f32)
        else:
            total = acc[:, c, :, cols] + drecv[:, c, :, cols].astype(f32)
        for d in range(3):
            total = total + crecv[d, :, :, cols].astype(f32)
        bsum[:, :, cols] = total
        for k in range(4):
            for j in range(4):
                piece = bsum[k, 4 * j : 4 * j + 4, cols]
                aown[k, j, :, cols] = piece
                asend[k, j, :, cols] = piece.astype(bf)
        for k in FAR_FIRST:
            to_b, to_a, device = plane(b, sb, k // 4, k % 4)
            start(asend.at[to_b, to_a, :, span], arecv.at[k - 1, :, span], a2s, a2r.at[n], device)
    for n, (low, width, s) in enumerate(CHUNKS):
        cols, span = slice(low, low + width), pl.ds(low, width)
        total = hid_ref[:, cols] + aown[colours[s][0], a, :, cols]
        landed(arecv.at[:, :, span], a2r.at[n])
        for k in range(15):
            total = total + arecv[k, :, cols].astype(f32)
        out_ref[:, cols] = total.astype(bf)
    landed(wsend.at[pl.ds(0, 7)], rs_w)
    for s in range(2):
        landed(lands[s].at[pl.ds(0, 15)], as_s.at[s])
        landed(xown.at[pl.ds(0, 3), :, :, spans[s]], cs_s.at[s])
    landed(xown, ds_s)
    landed(psend, d2s)
    landed(crecv, c2s)
    landed(arecv, a2s)


def landed(ref, sem):
    pltpu.make_async_copy(ref, ref, sem).wait()


def hand_over(out_in, newk_in, newv_in, out_ref, newk_ref, newv_ref, sem):
    pairs = ((out_in, out_ref), (newk_in, newk_ref), (newv_in, newv_ref))
    copies = [pltpu.make_async_copy(src, dst, sem.at[k]) for k, (src, dst) in enumerate(pairs)]
    for copy in copies:
        copy.start()
    for copy in copies:
        copy.wait()


def per_device(
    tokens, lengths, cache_keys, cache_values, query_w, key_w, value_w, out_w, mix_lambda, head_gain,
    attn_gain, ffn_gain, routes, route_weights, exp_gate, exp_up, exp_down, dense_gate, dense_up,
    dense_down, branch_gate,
):
    bf, f32 = jnp.bfloat16, jnp.float32
    dma = pltpu.SemaphoreType.DMA
    vmem = pl.BlockSpec(memory_space=pltpu.VMEM)
    anywhere = pl.BlockSpec(memory_space=pl.ANY)
    kv = KV_HEADS * HEAD_DIM
    shapes = tuple(jax.ShapeDtypeStruct((SEQ_DEV, width), bf) for width in (D, kv, kv))
    made = pl.pallas_call(
        layer_kernel,
        out_shape=tuple(pltpu.VMEM(shape.shape, bf) for shape in shapes),
        in_specs=[anywhere] * 21,
        out_specs=(vmem, vmem, vmem),
        scratch_shapes=[
            pltpu.SMEM((SEQ_DEV,), jnp.int32),
            pltpu.SMEM((HEADS,), f32),
            pltpu.SMEM((2, SEQ_DEV), jnp.int32),
            pltpu.SMEM((2, SEQ_DEV), f32),
            pltpu.VMEM((SEQ_DEV, D), bf),
            pltpu.VMEM((1, D), f32),
            pltpu.VMEM((1, D), f32),
            pltpu.VMEM((1, HEAD_DIM), f32),
            pltpu.VMEM((16, 128), bf),
            pltpu.VMEM((SEQ_DEV, 2 * CACHE, HEAD_DIM), bf),
            pltpu.VMEM((SEQ_DEV, 2 * CACHE, HEAD_DIM), bf),
            pltpu.VMEM((D, HEADS * HEAD_DIM), bf),
            pltpu.VMEM((D, 2 * kv), bf),
            pltpu.VMEM((HEADS * HEAD_DIM, D), bf),
            pltpu.VMEM((3, 352, 256), bf),
            pltpu.VMEM((SEQ_DEV, HEADS * HEAD_DIM + 2 * kv), f32),
            pltpu.VMEM((SEQ_DEV, HEADS, HEAD_DIM), f32),
            pltpu.VMEM((SEQ_DEV, 2 * HEADS, 2 * CACHE), f32),
            pltpu.VMEM((SEQ_DEV, HEADS * HEAD_DIM), f32),
            pltpu.VMEM((SEQ_DEV, D), f32),
            pltpu.VMEM((SEQ_DEV, WIDE), bf),
            pltpu.VMEM((3, D, 256), bf),
            pltpu.VMEM((512, D), bf),
            pltpu.VMEM((8, 3 * PART, 256), bf),
            pltpu.VMEM((8, 3 * PART, 256), bf),
            pltpu.VMEM((16, SEQ_DEV, EDGE), bf),
            pltpu.VMEM((16, SEQ_DEV, WIDE - EDGE), bf),
            pltpu.VMEM((16, WIDE), f32),
            pltpu.VMEM((4, 4, 16, WIDE), bf),
            pltpu.VMEM((4, 4, 16, WIDE), bf),
            pltpu.VMEM((2, 256, 512), bf),
            pltpu.VMEM((4, 4, 16, D), f32),
            pltpu.VMEM((4, 4, 16, D), bf),
            pltpu.VMEM((4, 4, 16, D), bf),
            pltpu.VMEM((4, 4, 16, D), bf),
            pltpu.VMEM((3, 4, 16, D), bf),
            pltpu.VMEM((4, 16, D), f32),
            pltpu.VMEM((4, 4, SEQ_DEV, D), f32),
            pltpu.VMEM((4, 4, SEQ_DEV, D), bf),
            pltpu.VMEM((15, SEQ_DEV, D), bf),
            dma((9,)), dma, dma((5,)), dma, dma, dma((4,)),
            dma((2,)), dma, dma, dma((2,)), dma((2, 4)), dma((2,)), dma((2, 4)), dma, dma,
            dma, dma((4,)), dma, dma((4,)), dma, dma((4,)),
        ],
        compiler_params=pltpu.CompilerParams(
            collective_id=0, has_side_effects=True, vmem_limit_bytes=VMEM_LIMIT
        ),
    )(
        lengths, mix_lambda, routes.T, route_weights.T, tokens, attn_gain.reshape(1, D), ffn_gain.reshape(1, D), head_gain.reshape(1, HEAD_DIM),
        branch_gate.reshape(16, 128),
        cache_keys.reshape(SEQ_DEV, -1, HEAD_DIM), cache_values.reshape(SEQ_DEV, -1, HEAD_DIM), query_w, key_w, value_w, out_w,
        exp_gate, exp_up, exp_down, dense_gate[0].T, dense_up[0].T, dense_down[0],
    )
    return pl.pallas_call(
        hand_over, out_shape=shapes, in_specs=[vmem] * 3, out_specs=(anywhere,) * 3, scratch_shapes=[dma((3,))]
    )(*[pltpu.with_memory_space_constraint(piece, pltpu.VMEM) for piece in made])


def solution(mesh):
    placed = (
        P("ep", None), P("ep"), P("ep", None, None, None), P("ep", None, None, None),
        P(), P(), P(), P(), P(), P(), P(), P(),
        P("ep", None), P("ep", None), P(None, "ep"), P(None, "ep"), P("ep", None),
        P("ep", None, None), P("ep", None, None), P("ep", None, None), P(),
    )
    return jax.shard_map(
        per_device,
        mesh=mesh,
        in_specs=placed,
        out_specs=(P("ep", None), P("ep", None), P("ep", None)),
        check_vma=False,
    )
```

```python
import jax
import jax.numpy as jnp
from jax import lax
from jax.experimental import pallas as pl
from jax.experimental.pallas import tpu as pltpu
from jax.sharding import PartitionSpec as P

HEADS = 8
KV_HEADS = 2
HEAD_DIM = 128
SEQ_DEV = 4
CACHE = 1024
SPLIT = 16
D = 2048
SIDE = 128
WIDE = D + SIDE
HID = 384
PART = 48
CHUNKS = ((0, 512, 1), (512, 512, 1), (1024, 640, 0), (1664, 384, 1))
HALVES = ((0, 1024, (0, 1)), (1024, 1024, (2, 3)))
EDGE = 6 * 128
VMEM_LIMIT = 67043328 - 131072
MESH = pl.DeviceIdType.MESH
FAR_FIRST = (10, 6, 14, 9, 11, 2, 8, 5, 7, 13, 15, 1, 3, 4, 12)
NEAR_FIRST = (1, 2, 3, 4, 5, 6, 7, 12, 13, 14, 15, 8, 9, 10, 11)
NT = (((1,), (1,)), ((), ()))


def rms_norm(values, gain, epsilon):
    scale = lax.rsqrt(jnp.mean(values * values, axis=-1, keepdims=True) + epsilon)
    return values * scale * gain


def remote(src, dst, send, recv, device):
    return pltpu.make_async_remote_copy(
        src_ref=src, dst_ref=dst, send_sem=send, recv_sem=recv,
        device_id=(device,), device_id_type=MESH,
    )


def layer_kernel(
    len_hbm, lam_hbm, routes_hbm, rweights_hbm, tok_hbm, again_hbm, fgain_hbm, hgain_hbm, bgate_hbm,
    keys_hbm, values_hbm, qw_hbm, kw_hbm, vw_hbm, ow_hbm,
    wg_hbm, wu_hbm, wd_hbm, dg_hbm, du_hbm, dd_hbm,
    out_ref, newk_ref, newv_ref,
    len_ref, lam_ref, routes_ref, rweights_ref, tok_ref, again_ref, fgain_ref, hgain_ref, bgate_ref,
    keys, values, qw, kvw, ow, tiles, qf, qs, sc, hf, hid_ref, x_ref,
    wgu, wdx, wsend, wrecv, land0, land1, pack, xown, xpart, act, acc, psend, drecv, csend, crecv,
    bsum, aown, asend, arecv,
    isem, dsem, qsem, ksem, vsem, osem,
    wsem, rs_w, rr_w, as_s, as_r, cs_s, cs_r, ds_s, ds_r, d2s, d2r, c2s, c2r, a2s, a2r,
):
    me = lax.axis_index("ep")
    core = lax.rem(me, 2)
    x = lax.rem(lax.div(me, 2), 4)
    y = lax.rem(lax.div(me, 8), 4)
    z = lax.div(me, 32)
    other = 1 - core
    a, sa = x * other + y * core, 2 * other + 8 * core
    p, sp = y * other + x * core, 8 * other + 2 * core
    colours = ((p, sp, z, 32), (z, 32, p, sp))
    row_block = lax.div(me, SPLIT)
    partner = me + other - core

    def ring(coord, stride, d):
        new = lax.rem(coord + d, 4)
        return new, me + (new - coord) * stride

    def plane(coord, stride, db, da):
        new_b, new_a = lax.rem(coord + db, 4), lax.rem(a + da, 4)
        return new_b, new_a, me + (new_b - coord) * stride + (new_a - a) * sa

    def group(d):
        new = lax.rem(row_block + d, 8)
        return new, me + (new - row_block) * SPLIT

    bf, f32 = jnp.bfloat16, jnp.float32

    def fetch(src, dst, sem, priority=0):
        copy = pltpu.make_async_copy(src, dst, sem)
        copy.start(priority=priority)
        return copy

    for k, tile in enumerate((dg_hbm, du_hbm, dd_hbm)):
        fetch(tile, tiles.at[k], dsem)
    small = (
        (tok_hbm, tok_ref), (again_hbm, again_ref), (len_hbm, len_ref), (lam_hbm, lam_ref),
        (routes_hbm, routes_ref), (rweights_hbm, rweights_ref), (fgain_hbm, fgain_ref),
        (hgain_hbm, hgain_ref), (bgate_hbm, bgate_ref),
    )
    small_in = [fetch(src, dst, isem.at[k]) for k, (src, dst) in enumerate(small)]
    quarter = [pl.ds(512 * n, 512) for n in range(4)]
    proj_in = [fetch(qw_hbm.at[part], qw.at[part], qsem.at[k], 1) for k, part in enumerate(quarter)]
    fetch(kw_hbm, kvw.at[:, pl.ds(0, 256)], qsem.at[4], 1)
    fetch(vw_hbm, kvw.at[:, pl.ds(256, 256)], qsem.at[4], 1)
    barrier = pltpu.get_barrier_semaphore()
    for coord, stride, _, _ in colours:
        for k in range(1, 16):
            device = plane(coord, stride, k // 4, k % 4)[2]
            pl.semaphore_signal(barrier, inc=1, device_id=(device,), device_id_type=MESH)
    for d in range(1, 8):
        pl.semaphore_signal(barrier, inc=1, device_id=(group(d)[1],), device_id_type=MESH)
    pl.semaphore_signal(barrier, inc=1, device_id=(partner,), device_id_type=MESH)

    def start(*args):
        remote(*args).start()

    for copy in small_in:
        copy.wait()
    landed(tiles, dsem)
    for k in range(3):
        for r in range(7):
            wsend[r, PART * k : PART * (k + 1)] = tiles[k, PART * r : PART * (r + 1)]
        wsend[7, PART * k : PART * k + 16] = tiles[k, 336:352]
        wsend[7, PART * k + 16 : PART * (k + 1)] = jnp.zeros((32, 256), bf)
    pl.semaphore_wait(barrier, 38)
    for d in range(1, 8):
        to, device = group(d)
        start(wsend.at[to], wrecv.at[row_block], rs_w, rr_w, device)
    wrecv[row_block] = wsend[row_block]
    normed = rms_norm(tok_ref[...].astype(f32), again_ref[...], 1e-06).astype(bf)
    query = jnp.zeros((SEQ_DEV, HEADS * HEAD_DIM), f32)
    for n in range(4):
        proj_in[n].wait()
        if n == 0:
            fetch(keys_hbm, keys, ksem, 1)
        if n == 2:
            fetch(values_hbm, values, vsem, 1)
        part = slice(512 * n, 512 * (n + 1))
        query = query + jnp.dot(normed[:, part], qw[part], preferred_element_type=f32)
    qf[:, : HEADS * HEAD_DIM] = query.astype(bf).astype(f32)
    landed(kvw, qsem.at[4])
    rows256 = [pl.ds(256 * n, 256) for n in range(4)]
    out_in = [fetch(ow_hbm.at[part], ow.at[part], osem.at[n], 1) for n, part in enumerate(rows256)]
    new = jnp.dot(normed, kvw[...], preferred_element_type=f32).astype(bf)
    newk_ref[...] = new[:, :256]
    newv_ref[...] = new[:, 256:]
    qf[:, HEADS * HEAD_DIM :] = new.astype(f32)
    for s in range(SEQ_DEV):
        for h in range(HEADS):
            qs[s, h : h + 1] = qf[s : s + 1, HEAD_DIM * h : HEAD_DIM * (h + 1)]

    head8 = lax.broadcasted_iota(jnp.int32, (HEADS, HEAD_DIM), 0)
    lane8 = lax.broadcasted_iota(jnp.int32, (HEADS, HEAD_DIM), 1)
    low_head, low_lane = head8 < HEADS // KV_HEADS, lane8 < HEAD_DIM // 2
    head1 = lax.broadcasted_iota(jnp.int32, (HEADS, 1), 0)
    lam = jnp.zeros((HEADS, 1), f32)
    for h in range(HEADS):
        lam = jnp.where(head1 == h, lam_ref[h], lam)
    slot = lax.broadcasted_iota(jnp.int32, (HEADS, 2 * CACHE), 1)
    kv_of = lax.broadcasted_iota(jnp.int32, (HEADS, 2 * CACHE), 0) // (HEADS // KV_HEADS)
    mine_kv = (slot & 1) == kv_of
    scale = (HEAD_DIM // 2) ** (-0.5)

    def probabilities(scores, own, valid):
        largest = jnp.maximum(jnp.max(jnp.where(valid, scores, -jnp.inf), axis=1, keepdims=True), own)
        raised = jnp.where(valid, jnp.exp(scores - largest), 0.0)
        own_raised = jnp.exp(own - largest)
        total = jnp.sum(raised, axis=1, keepdims=True) + own_raised
        return raised, own_raised, 1.0 / total

    base = HEADS * HEAD_DIM
    landed(keys, ksem)
    for s in range(SEQ_DEV):
        q = qs[s]
        both = jnp.concatenate([jnp.where(low_lane, q, 0.0), jnp.where(low_lane, 0.0, q)], axis=0).astype(bf)
        sc[s] = lax.dot_general(both, keys[s], NT, preferred_element_type=f32) * scale
    for n in range(3):
        cols = pl.ds(128 * n, 128)
        fetch(wg_hbm.at[:, cols], wgu.at[n, :, pl.ds(0, 128)], wsem.at[0], 1)
        fetch(wu_hbm.at[:, cols], wgu.at[n, :, pl.ds(128, 128)], wsem.at[0], 1)
    fetch(wd_hbm, wdx.at[pl.ds(0, HID)], wsem.at[1], 1)
    landed(values, vsem)
    for s in range(SEQ_DEV):
        q = qs[s]
        rows = [qf[s : s + 1, base + 128 * k : base + 128 * (k + 1)] for k in range(4)]
        own_score = q * jnp.where(low_head, rows[0], rows[1])
        own_value = jnp.where(low_head, rows[2], rows[3])
        own_one = jnp.sum(jnp.where(low_lane, own_score, 0.0), axis=1, keepdims=True) * scale
        own_two = jnp.sum(jnp.where(low_lane, 0.0, own_score), axis=1, keepdims=True) * scale
        valid = mine_kv & (slot < 2 * len_ref[s])
        raised_one, own_one, inv_one = probabilities(sc[s, :HEADS], own_one, valid)
        raised_two, own_two, inv_two = probabilities(sc[s, HEADS:], own_two, valid)
        inv_two = inv_two * lam
        weights = (raised_one * inv_one - raised_two * inv_two).astype(bf)
        own_weight = (own_one * inv_one - own_two * inv_two).astype(bf).astype(f32)
        mixed = jnp.dot(weights, values[s], preferred_element_type=f32) + own_weight * own_value
        mixed = rms_norm(mixed, hgain_ref[...], 1e-05)
        for h in range(HEADS):
            hf[s : s + 1, HEAD_DIM * h : HEAD_DIM * (h + 1)] = mixed[h : h + 1]
    heads = hf[...].astype(bf)
    state = tok_ref[...].astype(f32)
    for n in range(4):
        out_in[n].wait()
        part = slice(256 * n, 256 * (n + 1))
        state = state + jnp.dot(heads[:, part], ow[part], preferred_element_type=f32)
    hid_ref[...] = state
    ffn_in = rms_norm(state, fgain_ref[...], 1e-06).astype(bf)
    gate_row = bgate_ref[...].astype(f32)
    terms = jnp.zeros((SEQ_DEV, 128), f32)
    for k in range(16):
        terms = terms + ffn_in[:, 128 * k : 128 * (k + 1)].astype(f32) * gate_row[k : k + 1]
    gate = jax.nn.sigmoid(jnp.sum(terms, axis=1, keepdims=True))
    place = lax.broadcasted_iota(jnp.int32, (SEQ_DEV, SIDE), 1)
    row = lax.broadcasted_iota(jnp.int32, (SEQ_DEV, SIDE), 0)
    full = jnp.where((place == 16) | (place == 17), gate, 0.0)
    for t in range(SEQ_DEV):
        for k in range(2):
            chosen = (row == t) & (place < 16) & ((place & 7) == routes_ref[k, t])
            full = full + jnp.where(chosen, rweights_ref[k, t], 0.0)
    high = full.astype(bf).astype(f32)
    side = jnp.where((place < 8) | (place == 16), high, full - high)
    x_ref[:, :D] = ffn_in
    x_ref[:, D:] = side.astype(bf)

    lanes = (slice(0, EDGE), slice(EDGE, WIDE))
    spans = (pl.ds(0, EDGE), pl.ds(EDGE, WIDE - EDGE))
    lands = (land0, land1)
    for k in NEAR_FIRST:
        for s, (coord, stride, _, _) in enumerate(colours):
            device = plane(coord, stride, k // 4, k % 4)[2]
            start(x_ref.at[:, spans[s]], lands[s].at[4 * coord + a], as_s.at[s], as_r.at[s, k // 4], device)
    for s, (coord, _, _, _) in enumerate(colours):
        lands[s][4 * coord + a] = x_ref[:, lanes[s]]

    def place_of(s, along_c, along_b):
        return (along_c, along_b) if s == 0 else (along_b, along_c)

    def across(s, place):
        at = (*place, slice(None), spans[s])
        start(xown.at[at], xpart.at[at], ds_s, ds_r, partner)

    order = (0, 1, 3, 2)
    for db in order:
        for s, (b, _, c, sc_) in enumerate(colours):
            landed(lands[s].at[pl.ds(0, 4 if db else 3)], as_r.at[s, db])
            row = lax.rem(b + 4 - db, 4)
            for j in range(4):
                pack[4 * j : 4 * j + 4, lanes[s]] = lands[s][4 * row + j].astype(f32)
            place = place_of(s, c, row)
            xown[(*place, slice(None), lanes[s])] = pack[:, lanes[s]].astype(bf)
            at = (*place, slice(None), spans[s])
            for dc in (2, 1, 3):
                start(xown.at[at], xown.at[at], cs_s.at[s], cs_r.at[s, db], ring(c, sc_, dc)[1])
            across(s, place)
    for db in order:
        for s, (b, _, c, _) in enumerate(colours):
            landed(xown.at[0, pl.ds(0, 3), :, spans[s]], cs_r.at[s, db])
            for dc in (1, 3, 2):
                across(s, place_of(s, lax.rem(c + 4 - dc, 4), lax.rem(b + 4 - db, 4)))

    landed(wgu, wsem.at[0])
    landed(wdx.at[pl.ds(0, HID)], wsem.at[1])
    landed(wrecv.at[pl.ds(0, 7)], rr_w)
    wdx[HID + PART :] = jnp.zeros((128 - PART, D), jnp.bfloat16)
    for r in range(8):
        wdx[HID : HID + PART, 256 * r : 256 * (r + 1)] = wrecv[r, 2 * PART :]

    lane = lax.broadcasted_iota(jnp.int32, (256, SIDE), 1)

    def hidden(source, k, parts):
        rows = source[...].reshape(256, WIDE)
        side = rows[:, D:].astype(f32)
        for n in parts:
            if n < 3:
                expert = lax.div(me, SPLIT)
                weight = jnp.sum(jnp.where((lane == expert) | (lane == expert + 8), side, 0.0), axis=1, keepdims=True)
                both = jnp.dot(rows[:, :D], wgu[n], preferred_element_type=f32)
                first, second = both[:, :128], both[:, 128:]
                value = first * jax.nn.sigmoid(first) * second * weight
            else:
                gate = jnp.sum(jnp.where((lane == 16) | (lane == 17), side, 0.0), axis=1, keepdims=True)
                both = jnp.zeros((256, 128), f32)
                for r in range(8):
                    both += lax.dot_general(
                        rows[:, 256 * r : 256 * (r + 1)], wrecv[r, 0:128], NT, preferred_element_type=f32
                    )
                second = pltpu.roll(both, 128 - PART, 1)
                value = jnp.where(lane < PART, both * jax.nn.sigmoid(both) * second * gate, 0.0)
            act[k, :, 128 * n : 128 * (n + 1)] = value.astype(bf)

    def merge(n):
        low, width, s = CHUNKS[n]
        cols, span = slice(low, low + width), pl.ds(low, width)
        landed(drecv.at[:, :, :, span], d2r.at[n])
        csend[:, :, :, cols] = (acc[:, :, :, cols] + drecv[:, :, :, cols].astype(f32)).astype(bf)
        c, sc_ = colours[s][2:]
        for d in (2, 1, 3):
            to, device = ring(c, sc_, d)
            src = csend.at[to, :, :, span] if s == 0 else csend.at[:, to, :, span]
            start(src, crecv.at[d - 1, :, :, span], c2s, c2r.at[n], device)

    hidden(xown, 0, (0, 1))
    landed(xpart, ds_r)
    hidden(xpart, 1, (0, 1, 2, 3))
    for low, width, chunks in HALVES:
        cols = slice(low, low + width)
        part = jnp.dot(act[1], wdx[:, cols], preferred_element_type=f32).astype(bf)
        psend[:, :, :, cols] = part.reshape(4, 4, 16, width)
        for n in chunks:
            span = pl.ds(*CHUNKS[n][:2])
            start(psend.at[:, :, :, span], drecv.at[:, :, :, span], d2s, d2r.at[n], partner)
    hidden(xown, 0, (2, 3))
    for low, width, chunks in HALVES:
        cols = slice(low, low + width)
        part = jnp.dot(act[0], wdx[:, cols], preferred_element_type=f32)
        acc[:, :, :, cols] = part.reshape(4, 4, 16, width)
        for n in chunks:
            merge(n)
    for n, (low, width, s) in enumerate(CHUNKS):
        cols, span = slice(low, low + width), pl.ds(low, width)
        b, sb, c, _ = colours[s]
        landed(crecv.at[:, :, :, span], c2r.at[n])
        if s == 0:
            total = acc[c, :, :, cols] + drecv[c, :, :, cols].astype(f32)
        else:
            total = acc[:, c, :, cols] + drecv[:, c, :, cols].astype(f32)
        for d in range(3):
            total = total + crecv[d, :, :, cols].astype(f32)
        bsum[:, :, cols] = total
        for k in range(4):
            for j in range(4):
                piece = bsum[k, 4 * j : 4 * j + 4, cols]
                aown[k, j, :, cols] = piece
                asend[k, j, :, cols] = piece.astype(bf)
        for k in FAR_FIRST:
            to_b, to_a, device = plane(b, sb, k // 4, k % 4)
            start(asend.at[to_b, to_a, :, span], arecv.at[k - 1, :, span], a2s, a2r.at[n], device)
    for n, (low, width, s) in enumerate(CHUNKS):
        cols, span = slice(low, low + width), pl.ds(low, width)
        total = hid_ref[:, cols] + aown[colours[s][0], a, :, cols]
        landed(arecv.at[:, :, span], a2r.at[n])
        for k in range(15):
            total = total + arecv[k, :, cols].astype(f32)
        out_ref[:, cols] = total.astype(bf)
    landed(wsend.at[pl.ds(0, 7)], rs_w)
    for s in range(2):
        landed(lands[s].at[pl.ds(0, 15)], as_s.at[s])
        landed(xown.at[pl.ds(0, 3), :, :, spans[s]], cs_s.at[s])
    landed(xown, ds_s)
    landed(psend, d2s)
    landed(crecv, c2s)
    landed(arecv, a2s)


def landed(ref, sem):
    pltpu.make_async_copy(ref, ref, sem).wait()


def hand_over(out_in, newk_in, newv_in, out_ref, newk_ref, newv_ref, sem):
    pairs = ((out_in, out_ref), (newk_in, newk_ref), (newv_in, newv_ref))
    copies = [pltpu.make_async_copy(src, dst, sem.at[k]) for k, (src, dst) in enumerate(pairs)]
    for copy in copies:
        copy.start()
    for copy in copies:
        copy.wait()


def per_device(
    tokens, lengths, cache_keys, cache_values, query_w, key_w, value_w, out_w, mix_lambda, head_gain,
    attn_gain, ffn_gain, routes, route_weights, exp_gate, exp_up, exp_down, dense_gate, dense_up,
    dense_down, branch_gate,
):
    bf, f32 = jnp.bfloat16, jnp.float32
    dma = pltpu.SemaphoreType.DMA
    vmem = pl.BlockSpec(memory_space=pltpu.VMEM)
    anywhere = pl.BlockSpec(memory_space=pl.ANY)
    kv = KV_HEADS * HEAD_DIM
    shapes = tuple(jax.ShapeDtypeStruct((SEQ_DEV, width), bf) for width in (D, kv, kv))
    made = pl.pallas_call(
        layer_kernel,
        out_shape=tuple(pltpu.VMEM(shape.shape, bf) for shape in shapes),
        in_specs=[anywhere] * 21,
        out_specs=(vmem, vmem, vmem),
        scratch_shapes=[
            pltpu.SMEM((SEQ_DEV,), jnp.int32),
            pltpu.SMEM((HEADS,), f32),
            pltpu.SMEM((2, SEQ_DEV), jnp.int32),
            pltpu.SMEM((2, SEQ_DEV), f32),
            pltpu.VMEM((SEQ_DEV, D), bf),
            pltpu.VMEM((1, D), f32),
            pltpu.VMEM((1, D), f32),
            pltpu.VMEM((1, HEAD_DIM), f32),
            pltpu.VMEM((16, 128), bf),
            pltpu.VMEM((SEQ_DEV, 2 * CACHE, HEAD_DIM), bf),
            pltpu.VMEM((SEQ_DEV, 2 * CACHE, HEAD_DIM), bf),
            pltpu.VMEM((D, HEADS * HEAD_DIM), bf),
            pltpu.VMEM((D, 2 * kv), bf),
            pltpu.VMEM((HEADS * HEAD_DIM, D), bf),
            pltpu.VMEM((3, 352, 256), bf),
            pltpu.VMEM((SEQ_DEV, HEADS * HEAD_DIM + 2 * kv), f32),
            pltpu.VMEM((SEQ_DEV, HEADS, HEAD_DIM), f32),
            pltpu.VMEM((SEQ_DEV, 2 * HEADS, 2 * CACHE), f32),
            pltpu.VMEM((SEQ_DEV, HEADS * HEAD_DIM), f32),
            pltpu.VMEM((SEQ_DEV, D), f32),
            pltpu.VMEM((SEQ_DEV, WIDE), bf),
            pltpu.VMEM((3, D, 256), bf),
            pltpu.VMEM((512, D), bf),
            pltpu.VMEM((8, 3 * PART, 256), bf),
            pltpu.VMEM((8, 3 * PART, 256), bf),
            pltpu.VMEM((16, SEQ_DEV, EDGE), bf),
            pltpu.VMEM((16, SEQ_DEV, WIDE - EDGE), bf),
            pltpu.VMEM((16, WIDE), f32),
            pltpu.VMEM((4, 4, 16, WIDE), bf),
            pltpu.VMEM((4, 4, 16, WIDE), bf),
            pltpu.VMEM((2, 256, 512), bf),
            pltpu.VMEM((4, 4, 16, D), f32),
            pltpu.VMEM((4, 4, 16, D), bf),
            pltpu.VMEM((4, 4, 16, D), bf),
            pltpu.VMEM((4, 4, 16, D), bf),
            pltpu.VMEM((3, 4, 16, D), bf),
            pltpu.VMEM((4, 16, D), f32),
            pltpu.VMEM((4, 4, SEQ_DEV, D), f32),
            pltpu.VMEM((4, 4, SEQ_DEV, D), bf),
            pltpu.VMEM((15, SEQ_DEV, D), bf),
            dma((9,)), dma, dma((5,)), dma, dma, dma((4,)),
            dma((2,)), dma, dma, dma((2,)), dma((2, 4)), dma((2,)), dma((2, 4)), dma, dma,
            dma, dma((4,)), dma, dma((4,)), dma, dma((4,)),
        ],
        compiler_params=pltpu.CompilerParams(
            collective_id=0, has_side_effects=True, vmem_limit_bytes=VMEM_LIMIT
        ),
    )(
        lengths, mix_lambda, routes.T, route_weights.T, tokens, attn_gain.reshape(1, D), ffn_gain.reshape(1, D), head_gain.reshape(1, HEAD_DIM),
        branch_gate.reshape(16, 128),
        cache_keys.reshape(SEQ_DEV, -1, HEAD_DIM), cache_values.reshape(SEQ_DEV, -1, HEAD_DIM), query_w, key_w, value_w, out_w,
        exp_gate, exp_up, exp_down, dense_gate[0].T, dense_up[0].T, dense_down[0],
    )
    return pl.pallas_call(
        hand_over, out_shape=shapes, in_specs=[vmem] * 3, out_specs=(anywhere,) * 3, scratch_shapes=[dma((3,))]
    )(*[pltpu.with_memory_space_constraint(piece, pltpu.VMEM) for piece in made])


def solution(mesh):
    placed = (
        P("ep", None), P("ep"), P("ep", None, None, None), P("ep", None, None, None),
        P(), P(), P(), P(), P(), P(), P(), P(),
        P("ep", None), P("ep", None), P(None, "ep"), P(None, "ep"), P("ep", None),
        P("ep", None, None), P("ep", None, None), P("ep", None, None), P(),
    )
    return jax.shard_map(
        per_device,
        mesh=mesh,
        in_specs=placed,
        out_specs=(P("ep", None), P("ep", None), P("ep", None)),
        check_vma=False,
    )
```

```python
import jax
import jax.numpy as jnp
from jax import lax
from jax.experimental import pallas as pl
from jax.experimental.pallas import tpu as pltpu
from jax.sharding import PartitionSpec as P

HEADS = 8
KV_HEADS = 2
HEAD_DIM = 128
SEQ_DEV = 4
CACHE = 1024
SPLIT = 16
D = 2048
SIDE = 128
WIDE = D + SIDE
HID = 384
PART = 48
CHUNKS = ((0, 512, 1), (512, 512, 1), (1024, 640, 0), (1664, 384, 1))
HALVES = ((0, 1024, (0, 1)), (1024, 1024, (2, 3)))
EDGE = 6 * 128
VMEM_LIMIT = 67043328 - 131072
MESH = pl.DeviceIdType.MESH
FAR_FIRST = (10, 6, 14, 9, 11, 2, 8, 5, 7, 13, 15, 1, 3, 4, 12)
NEAR_FIRST = (1, 2, 3, 4, 5, 6, 7, 12, 13, 14, 15, 8, 9, 10, 11)
NT = (((1,), (1,)), ((), ()))


def rms_norm(values, gain, epsilon):
    scale = lax.rsqrt(jnp.mean(values * values, axis=-1, keepdims=True) + epsilon)
    return values * scale * gain


def remote(src, dst, send, recv, device):
    return pltpu.make_async_remote_copy(
        src_ref=src, dst_ref=dst, send_sem=send, recv_sem=recv,
        device_id=(device,), device_id_type=MESH,
    )


def layer_kernel(
    len_hbm, lam_hbm, routes_hbm, rweights_hbm, tok_hbm, again_hbm, fgain_hbm, hgain_hbm, bgate_hbm,
    keys_hbm, values_hbm, qw_hbm, kw_hbm, vw_hbm, ow_hbm,
    wg_hbm, wu_hbm, wd_hbm, dg_hbm, du_hbm, dd_hbm,
    out_ref, newk_ref, newv_ref,
    len_ref, lam_ref, routes_ref, rweights_ref, tok_ref, again_ref, fgain_ref, hgain_ref, bgate_ref,
    keys, values, qw, kvw, ow, tiles, qf, qs, sc, hf, hid_ref, x_ref,
    wgu, wdx, wsend, wrecv, land0, land1, pack, xown, xpart, act, acc, psend, drecv, csend, crecv,
    bsum, aown, asend, arecv,
    isem, dsem, qsem, ksem, vsem, osem,
    wsem, rs_w, rr_w, as_s, as_r, cs_s, cs_r, ds_s, ds_r, d2s, d2r, c2s, c2r, a2s, a2r,
):
    me = lax.axis_index("ep")
    core = lax.rem(me, 2)
    x = lax.rem(lax.div(me, 2), 4)
    y = lax.rem(lax.div(me, 8), 4)
    z = lax.div(me, 32)
    other = 1 - core
    a, sa = x * other + y * core, 2 * other + 8 * core
    p, sp = y * other + x * core, 8 * other + 2 * core
    colours = ((p, sp, z, 32), (z, 32, p, sp))
    row_block = lax.div(me, SPLIT)
    partner = me + other - core

    def ring(coord, stride, d):
        new = lax.rem(coord + d, 4)
        return new, me + (new - coord) * stride

    def plane(coord, stride, db, da):
        new_b, new_a = lax.rem(coord + db, 4), lax.rem(a + da, 4)
        return new_b, new_a, me + (new_b - coord) * stride + (new_a - a) * sa

    def group(d):
        new = lax.rem(row_block + d, 8)
        return new, me + (new - row_block) * SPLIT

    bf, f32 = jnp.bfloat16, jnp.float32

    def fetch(src, dst, sem, priority=0):
        copy = pltpu.make_async_copy(src, dst, sem)
        copy.start(priority=priority)
        return copy

    for k, tile in enumerate((dg_hbm, du_hbm, dd_hbm)):
        fetch(tile, tiles.at[k], dsem)
    small = (
        (tok_hbm, tok_ref), (again_hbm, again_ref), (len_hbm, len_ref), (lam_hbm, lam_ref),
        (routes_hbm, routes_ref), (rweights_hbm, rweights_ref), (fgain_hbm, fgain_ref),
        (hgain_hbm, hgain_ref), (bgate_hbm, bgate_ref),
    )
    small_in = [fetch(src, dst, isem.at[k]) for k, (src, dst) in enumerate(small)]
    quarter = [pl.ds(512 * n, 512) for n in range(4)]
    proj_in = [fetch(qw_hbm.at[part], qw.at[part], qsem.at[k], 1) for k, part in enumerate(quarter)]
    fetch(kw_hbm, kvw.at[:, pl.ds(0, 256)], qsem.at[4], 1)
    fetch(vw_hbm, kvw.at[:, pl.ds(256, 256)], qsem.at[4], 1)
    barrier = pltpu.get_barrier_semaphore()
    for coord, stride, _, _ in colours:
        for k in range(1, 16):
            device = plane(coord, stride, k // 4, k % 4)[2]
            pl.semaphore_signal(barrier, inc=1, device_id=(device,), device_id_type=MESH)
    for d in range(1, 8):
        pl.semaphore_signal(barrier, inc=1, device_id=(group(d)[1],), device_id_type=MESH)
    pl.semaphore_signal(barrier, inc=1, device_id=(partner,), device_id_type=MESH)

    def start(*args):
        remote(*args).start()

    for copy in small_in:
        copy.wait()
    landed(tiles, dsem)
    for k in range(3):
        for r in range(7):
            wsend[r, PART * k : PART * (k + 1)] = tiles[k, PART * r : PART * (r + 1)]
        wsend[7, PART * k : PART * k + 16] = tiles[k, 336:352]
        wsend[7, PART * k + 16 : PART * (k + 1)] = jnp.zeros((32, 256), bf)
    fetch(keys_hbm, keys, ksem, 1)
    pl.semaphore_wait(barrier, 38)
    for d in range(1, 8):
        to, device = group(d)
        start(wsend.at[to], wrecv.at[row_block], rs_w, rr_w, device)
    wrecv[row_block] = wsend[row_block]
    normed = rms_norm(tok_ref[...].astype(f32), again_ref[...], 1e-06).astype(bf)
    query = jnp.zeros((SEQ_DEV, HEADS * HEAD_DIM), f32)
    for n in range(4):
        proj_in[n].wait()
        if n == 2:
            fetch(values_hbm, values, vsem, 1)
        part = slice(512 * n, 512 * (n + 1))
        query = query + jnp.dot(normed[:, part], qw[part], preferred_element_type=f32)
    qf[:, : HEADS * HEAD_DIM] = query.astype(bf).astype(f32)
    landed(kvw, qsem.at[4])
    rows256 = [pl.ds(256 * n, 256) for n in range(4)]
    out_in = [fetch(ow_hbm.at[part], ow.at[part], osem.at[n], 1) for n, part in enumerate(rows256)]
    new = jnp.dot(normed, kvw[...], preferred_element_type=f32).astype(bf)
    newk_ref[...] = new[:, :256]
    newv_ref[...] = new[:, 256:]
    qf[:, HEADS * HEAD_DIM :] = new.astype(f32)
    for s in range(SEQ_DEV):
        for h in range(HEADS):
            qs[s, h : h + 1] = qf[s : s + 1, HEAD_DIM * h : HEAD_DIM * (h + 1)]

    head8 = lax.broadcasted_iota(jnp.int32, (HEADS, HEAD_DIM), 0)
    lane8 = lax.broadcasted_iota(jnp.int32, (HEADS, HEAD_DIM), 1)
    low_head, low_lane = head8 < HEADS // KV_HEADS, lane8 < HEAD_DIM // 2
    head1 = lax.broadcasted_iota(jnp.int32, (HEADS, 1), 0)
    lam = jnp.zeros((HEADS, 1), f32)
    for h in range(HEADS):
        lam = jnp.where(head1 == h, lam_ref[h], lam)
    slot = lax.broadcasted_iota(jnp.int32, (HEADS, 2 * CACHE), 1)
    kv_of = lax.broadcasted_iota(jnp.int32, (HEADS, 2 * CACHE), 0) // (HEADS // KV_HEADS)
    mine_kv = (slot & 1) == kv_of
    scale = (HEAD_DIM // 2) ** (-0.5)

    def probabilities(scores, own, valid):
        largest = jnp.maximum(jnp.max(jnp.where(valid, scores, -jnp.inf), axis=1, keepdims=True), own)
        raised = jnp.where(valid, jnp.exp(scores - largest), 0.0)
        own_raised = jnp.exp(own - largest)
        total = jnp.sum(raised, axis=1, keepdims=True) + own_raised
        return raised, own_raised, 1.0 / total

    base = HEADS * HEAD_DIM
    landed(keys, ksem)
    for s in range(SEQ_DEV):
        q = qs[s]
        both = jnp.concatenate([jnp.where(low_lane, q, 0.0), jnp.where(low_lane, 0.0, q)], axis=0).astype(bf)
        sc[s] = lax.dot_general(both, keys[s], NT, preferred_element_type=f32) * scale
    for n in range(3):
        cols = pl.ds(128 * n, 128)
        fetch(wg_hbm.at[:, cols], wgu.at[n, :, pl.ds(0, 128)], wsem.at[0], 1)
        fetch(wu_hbm.at[:, cols], wgu.at[n, :, pl.ds(128, 128)], wsem.at[0], 1)
    fetch(wd_hbm, wdx.at[pl.ds(0, HID)], wsem.at[1], 1)
    landed(values, vsem)
    for s in range(SEQ_DEV):
        q = qs[s]
        rows = [qf[s : s + 1, base + 128 * k : base + 128 * (k + 1)] for k in range(4)]
        own_score = q * jnp.where(low_head, rows[0], rows[1])
        own_value = jnp.where(low_head, rows[2], rows[3])
        own_one = jnp.sum(jnp.where(low_lane, own_score, 0.0), axis=1, keepdims=True) * scale
        own_two = jnp.sum(jnp.where(low_lane, 0.0, own_score), axis=1, keepdims=True) * scale
        valid = mine_kv & (slot < 2 * len_ref[s])
        raised_one, own_one, inv_one = probabilities(sc[s, :HEADS], own_one, valid)
        raised_two, own_two, inv_two = probabilities(sc[s, HEADS:], own_two, valid)
        inv_two = inv_two * lam
        weights = (raised_one * inv_one - raised_two * inv_two).astype(bf)
        own_weight = (own_one * inv_one - own_two * inv_two).astype(bf).astype(f32)
        mixed = jnp.dot(weights, values[s], preferred_element_type=f32) + own_weight * own_value
        mixed = rms_norm(mixed, hgain_ref[...], 1e-05)
        for h in range(HEADS):
            hf[s : s + 1, HEAD_DIM * h : HEAD_DIM * (h + 1)] = mixed[h : h + 1]
    heads = hf[...].astype(bf)
    state = tok_ref[...].astype(f32)
    for n in range(4):
        out_in[n].wait()
        part = slice(256 * n, 256 * (n + 1))
        state = state + jnp.dot(heads[:, part], ow[part], preferred_element_type=f32)
    hid_ref[...] = state
    ffn_in = rms_norm(state, fgain_ref[...], 1e-06).astype(bf)
    gate_row = bgate_ref[...].astype(f32)
    terms = jnp.zeros((SEQ_DEV, 128), f32)
    for k in range(16):
        terms = terms + ffn_in[:, 128 * k : 128 * (k + 1)].astype(f32) * gate_row[k : k + 1]
    gate = jax.nn.sigmoid(jnp.sum(terms, axis=1, keepdims=True))
    place = lax.broadcasted_iota(jnp.int32, (SEQ_DEV, SIDE), 1)
    row = lax.broadcasted_iota(jnp.int32, (SEQ_DEV, SIDE), 0)
    full = jnp.where((place == 16) | (place == 17), gate, 0.0)
    for t in range(SEQ_DEV):
        for k in range(2):
            chosen = (row == t) & (place < 16) & ((place & 7) == routes_ref[k, t])
            full = full + jnp.where(chosen, rweights_ref[k, t], 0.0)
    high = full.astype(bf).astype(f32)
    side = jnp.where((place < 8) | (place == 16), high, full - high)
    x_ref[:, :D] = ffn_in
    x_ref[:, D:] = side.astype(bf)

    lanes = (slice(0, EDGE), slice(EDGE, WIDE))
    spans = (pl.ds(0, EDGE), pl.ds(EDGE, WIDE - EDGE))
    lands = (land0, land1)
    for k in NEAR_FIRST:
        for s, (coord, stride, _, _) in enumerate(colours):
            device = plane(coord, stride, k // 4, k % 4)[2]
            start(x_ref.at[:, spans[s]], lands[s].at[4 * coord + a], as_s.at[s], as_r.at[s, k // 4], device)
    for s, (coord, _, _, _) in enumerate(colours):
        lands[s][4 * coord + a] = x_ref[:, lanes[s]]

    def place_of(s, along_c, along_b):
        return (along_c, along_b) if s == 0 else (along_b, along_c)

    def across(s, place):
        at = (*place, slice(None), spans[s])
        start(xown.at[at], xpart.at[at], ds_s, ds_r, partner)

    order = (0, 1, 3, 2)
    for db in order:
        for s, (b, _, c, sc_) in enumerate(colours):
            landed(lands[s].at[pl.ds(0, 4 if db else 3)], as_r.at[s, db])
            row = lax.rem(b + 4 - db, 4)
            for j in range(4):
                pack[4 * j : 4 * j + 4, lanes[s]] = lands[s][4 * row + j].astype(f32)
            place = place_of(s, c, row)
            xown[(*place, slice(None), lanes[s])] = pack[:, lanes[s]].astype(bf)
            at = (*place, slice(None), spans[s])
            for dc in (2, 1, 3):
                start(xown.at[at], xown.at[at], cs_s.at[s], cs_r.at[s, db], ring(c, sc_, dc)[1])
            across(s, place)
    for db in order:
        for s, (b, _, c, _) in enumerate(colours):
            landed(xown.at[0, pl.ds(0, 3), :, spans[s]], cs_r.at[s, db])
            for dc in (1, 3, 2):
                across(s, place_of(s, lax.rem(c + 4 - dc, 4), lax.rem(b + 4 - db, 4)))

    landed(wgu, wsem.at[0])
    landed(wdx.at[pl.ds(0, HID)], wsem.at[1])
    landed(wrecv.at[pl.ds(0, 7)], rr_w)
    wdx[HID + PART :] = jnp.zeros((128 - PART, D), jnp.bfloat16)
    for r in range(8):
        wdx[HID : HID + PART, 256 * r : 256 * (r + 1)] = wrecv[r, 2 * PART :]

    lane = lax.broadcasted_iota(jnp.int32, (256, SIDE), 1)

    def hidden(source, k, parts):
        rows = source[...].reshape(256, WIDE)
        side = rows[:, D:].astype(f32)
        for n in parts:
            if n < 3:
                expert = lax.div(me, SPLIT)
                weight = jnp.sum(jnp.where((lane == expert) | (lane == expert + 8), side, 0.0), axis=1, keepdims=True)
                both = jnp.dot(rows[:, :D], wgu[n], preferred_element_type=f32)
                first, second = both[:, :128], both[:, 128:]
                value = first * jax.nn.sigmoid(first) * second * weight
            else:
                gate = jnp.sum(jnp.where((lane == 16) | (lane == 17), side, 0.0), axis=1, keepdims=True)
                both = jnp.zeros((256, 128), f32)
                for r in range(8):
                    both += lax.dot_general(
                        rows[:, 256 * r : 256 * (r + 1)], wrecv[r, 0:128], NT, preferred_element_type=f32
                    )
                second = pltpu.roll(both, 128 - PART, 1)
                value = jnp.where(lane < PART, both * jax.nn.sigmoid(both) * second * gate, 0.0)
            act[k, :, 128 * n : 128 * (n + 1)] = value.astype(bf)

    def merge(n):
        low, width, s = CHUNKS[n]
        cols, span = slice(low, low + width), pl.ds(low, width)
        landed(drecv.at[:, :, :, span], d2r.at[n])
        csend[:, :, :, cols] = (acc[:, :, :, cols] + drecv[:, :, :, cols].astype(f32)).astype(bf)
        c, sc_ = colours[s][2:]
        for d in (2, 1, 3):
            to, device = ring(c, sc_, d)
            src = csend.at[to, :, :, span] if s == 0 else csend.at[:, to, :, span]
            start(src, crecv.at[d - 1, :, :, span], c2s, c2r.at[n], device)

    hidden(xown, 0, (0, 1))
    landed(xpart, ds_r)
    hidden(xpart, 1, (0, 1, 2, 3))
    for low, width, chunks in HALVES:
        cols = slice(low, low + width)
        part = jnp.dot(act[1], wdx[:, cols], preferred_element_type=f32).astype(bf)
        psend[:, :, :, cols] = part.reshape(4, 4, 16, width)
        for n in chunks:
            span = pl.ds(*CHUNKS[n][:2])
            start(psend.at[:, :, :, span], drecv.at[:, :, :, span], d2s, d2r.at[n], partner)
    hidden(xown, 0, (2, 3))
    for low, width, chunks in HALVES:
        cols = slice(low, low + width)
        part = jnp.dot(act[0], wdx[:, cols], preferred_element_type=f32)
        acc[:, :, :, cols] = part.reshape(4, 4, 16, width)
        for n in chunks:
            merge(n)
    for n, (low, width, s) in enumerate(CHUNKS):
        cols, span = slice(low, low + width), pl.ds(low, width)
        b, sb, c, _ = colours[s]
        landed(crecv.at[:, :, :, span], c2r.at[n])
        if s == 0:
            total = acc[c, :, :, cols] + drecv[c, :, :, cols].astype(f32)
        else:
            total = acc[:, c, :, cols] + drecv[:, c, :, cols].astype(f32)
        for d in range(3):
            total = total + crecv[d, :, :, cols].astype(f32)
        bsum[:, :, cols] = total
        for k in range(4):
            for j in range(4):
                piece = bsum[k, 4 * j : 4 * j + 4, cols]
                aown[k, j, :, cols] = piece
                asend[k, j, :, cols] = piece.astype(bf)
        for k in FAR_FIRST:
            to_b, to_a, device = plane(b, sb, k // 4, k % 4)
            start(asend.at[to_b, to_a, :, span], arecv.at[k - 1, :, span], a2s, a2r.at[n], device)
    for n, (low, width, s) in enumerate(CHUNKS):
        cols, span = slice(low, low + width), pl.ds(low, width)
        total = hid_ref[:, cols] + aown[colours[s][0], a, :, cols]
        landed(arecv.at[:, :, span], a2r.at[n])
        for k in range(15):
            total = total + arecv[k, :, cols].astype(f32)
        out_ref[:, cols] = total.astype(bf)
    landed(wsend.at[pl.ds(0, 7)], rs_w)
    for s in range(2):
        landed(lands[s].at[pl.ds(0, 15)], as_s.at[s])
        landed(xown.at[pl.ds(0, 3), :, :, spans[s]], cs_s.at[s])
    landed(xown, ds_s)
    landed(psend, d2s)
    landed(crecv, c2s)
    landed(arecv, a2s)


def landed(ref, sem):
    pltpu.make_async_copy(ref, ref, sem).wait()


def hand_over(out_in, newk_in, newv_in, out_ref, newk_ref, newv_ref, sem):
    pairs = ((out_in, out_ref), (newk_in, newk_ref), (newv_in, newv_ref))
    copies = [pltpu.make_async_copy(src, dst, sem.at[k]) for k, (src, dst) in enumerate(pairs)]
    for copy in copies:
        copy.start()
    for copy in copies:
        copy.wait()


def per_device(
    tokens, lengths, cache_keys, cache_values, query_w, key_w, value_w, out_w, mix_lambda, head_gain,
    attn_gain, ffn_gain, routes, route_weights, exp_gate, exp_up, exp_down, dense_gate, dense_up,
    dense_down, branch_gate,
):
    bf, f32 = jnp.bfloat16, jnp.float32
    dma = pltpu.SemaphoreType.DMA
    vmem = pl.BlockSpec(memory_space=pltpu.VMEM)
    anywhere = pl.BlockSpec(memory_space=pl.ANY)
    kv = KV_HEADS * HEAD_DIM
    shapes = tuple(jax.ShapeDtypeStruct((SEQ_DEV, width), bf) for width in (D, kv, kv))
    made = pl.pallas_call(
        layer_kernel,
        out_shape=tuple(pltpu.VMEM(shape.shape, bf) for shape in shapes),
        in_specs=[anywhere] * 21,
        out_specs=(vmem, vmem, vmem),
        scratch_shapes=[
            pltpu.SMEM((SEQ_DEV,), jnp.int32),
            pltpu.SMEM((HEADS,), f32),
            pltpu.SMEM((2, SEQ_DEV), jnp.int32),
            pltpu.SMEM((2, SEQ_DEV), f32),
            pltpu.VMEM((SEQ_DEV, D), bf),
            pltpu.VMEM((1, D), f32),
            pltpu.VMEM((1, D), f32),
            pltpu.VMEM((1, HEAD_DIM), f32),
            pltpu.VMEM((16, 128), bf),
            pltpu.VMEM((SEQ_DEV, 2 * CACHE, HEAD_DIM), bf),
            pltpu.VMEM((SEQ_DEV, 2 * CACHE, HEAD_DIM), bf),
            pltpu.VMEM((D, HEADS * HEAD_DIM), bf),
            pltpu.VMEM((D, 2 * kv), bf),
            pltpu.VMEM((HEADS * HEAD_DIM, D), bf),
            pltpu.VMEM((3, 352, 256), bf),
            pltpu.VMEM((SEQ_DEV, HEADS * HEAD_DIM + 2 * kv), f32),
            pltpu.VMEM((SEQ_DEV, HEADS, HEAD_DIM), f32),
            pltpu.VMEM((SEQ_DEV, 2 * HEADS, 2 * CACHE), f32),
            pltpu.VMEM((SEQ_DEV, HEADS * HEAD_DIM), f32),
            pltpu.VMEM((SEQ_DEV, D), f32),
            pltpu.VMEM((SEQ_DEV, WIDE), bf),
            pltpu.VMEM((3, D, 256), bf),
            pltpu.VMEM((512, D), bf),
            pltpu.VMEM((8, 3 * PART, 256), bf),
            pltpu.VMEM((8, 3 * PART, 256), bf),
            pltpu.VMEM((16, SEQ_DEV, EDGE), bf),
            pltpu.VMEM((16, SEQ_DEV, WIDE - EDGE), bf),
            pltpu.VMEM((16, WIDE), f32),
            pltpu.VMEM((4, 4, 16, WIDE), bf),
            pltpu.VMEM((4, 4, 16, WIDE), bf),
            pltpu.VMEM((2, 256, 512), bf),
            pltpu.VMEM((4, 4, 16, D), f32),
            pltpu.VMEM((4, 4, 16, D), bf),
            pltpu.VMEM((4, 4, 16, D), bf),
            pltpu.VMEM((4, 4, 16, D), bf),
            pltpu.VMEM((3, 4, 16, D), bf),
            pltpu.VMEM((4, 16, D), f32),
            pltpu.VMEM((4, 4, SEQ_DEV, D), f32),
            pltpu.VMEM((4, 4, SEQ_DEV, D), bf),
            pltpu.VMEM((15, SEQ_DEV, D), bf),
            dma((9,)), dma, dma((5,)), dma, dma, dma((4,)),
            dma((2,)), dma, dma, dma((2,)), dma((2, 4)), dma((2,)), dma((2, 4)), dma, dma,
            dma, dma((4,)), dma, dma((4,)), dma, dma((4,)),
        ],
        compiler_params=pltpu.CompilerParams(
            collective_id=0, has_side_effects=True, vmem_limit_bytes=VMEM_LIMIT
        ),
    )(
        lengths, mix_lambda, routes.T, route_weights.T, tokens, attn_gain.reshape(1, D), ffn_gain.reshape(1, D), head_gain.reshape(1, HEAD_DIM),
        branch_gate.reshape(16, 128),
        cache_keys.reshape(SEQ_DEV, -1, HEAD_DIM), cache_values.reshape(SEQ_DEV, -1, HEAD_DIM), query_w, key_w, value_w, out_w,
        exp_gate, exp_up, exp_down, dense_gate[0].T, dense_up[0].T, dense_down[0],
    )
    return pl.pallas_call(
        hand_over, out_shape=shapes, in_specs=[vmem] * 3, out_specs=(anywhere,) * 3, scratch_shapes=[dma((3,))]
    )(*[pltpu.with_memory_space_constraint(piece, pltpu.VMEM) for piece in made])


def solution(mesh):
    placed = (
        P("ep", None), P("ep"), P("ep", None, None, None), P("ep", None, None, None),
        P(), P(), P(), P(), P(), P(), P(), P(),
        P("ep", None), P("ep", None), P(None, "ep"), P(None, "ep"), P("ep", None),
        P("ep", None, None), P("ep", None, None), P("ep", None, None), P(),
    )
    return jax.shard_map(
        per_device,
        mesh=mesh,
        in_specs=placed,
        out_specs=(P("ep", None), P("ep", None), P("ep", None)),
        check_vma=False,
    )
```
